256 devices in a mesh: grp: 2 (over y), sp: 16 (over z), tp: 8 (over x, core).
Axes of the slice: x: 4, y: 2, z: 16, core: 2. Of those that a mesh axis runs over, the one named last changes fastest.
The devices are a block of a 4x16x16 slice.
Arguments:
- tokens: bfloat16 [16384, 4096], P(('grp', 'sp', 'tp')), parts along dimension 0, may hold values from -6 to 6
- norm_gain: float32 [4096], replicated, may hold values from 0.1 to 1.9
- query_diff: bfloat16 [4096, 2048], P('sp', 'tp'), may hold values from -1.25 to 1.25
- key_diff: bfloat16 [4096, 2048], P('sp', 'tp'), may hold values from -1.25 to 1.25
- value_diff: bfloat16 [4096, 2048], P('sp', 'tp'), may hold values from -0.09375 to 0.09375
- lam: float32 [8], P('tp'), may hold values from 0.3 to 0.8
- output_norm_gain: float32 [256], replicated, may hold values from 0.1 to 1.9
- query_win: bfloat16 [4096, 2048], P('sp', 'tp'), may hold values from -1.25 to 1.25
- keyval_win: bfloat16 [4, 4096, 256], P(None, 'sp'), may hold values from -1.25 to 1.25
- sink: float32 [16], P('tp'), may hold values from 4 to 7
- proj_diff: bfloat16 [2048, 4096], P('tp'), may hold values from -0.125 to 0.125
- proj_win: bfloat16 [2048, 4096], P('tp'), may hold values from -0.79296875 to 0.79296875
Outputs:
- mixed: bfloat16 [16384, 4096], P(('grp', 'sp', 'tp')), parts along dimension 0
The draws below stay inside these ranges and needn't reach their ends.
There are 2 independent parts, one for each index of `grp`. The reference program is written for one: setup_inputs(seed, part) draws one part's arguments, and reference() takes and returns one part's arrays. A program takes and returns all parts, laid end to end along the dimension named above; an argument that names none is the same for every part. Nothing has to cross between parts.
All inputs are finite; a program needn't handle non-finite values.
Results may differ from the reference program's by a relative error of at most 0.015.
Values may be sent and summed in bfloat16 or wider, within the bound.
A program may use at most 128 MiB of HBM per device.

```python
import math
import jax
import jax.numpy as jnp
from jax import lax

D = 4096
HEAD = 128
DIFF_HEADS = 8
WIN_HEADS = 16
KV_HEADS = 4
WINDOW = 128
VDIM = 256
SEQ = 8192


def draw_tokens(key, part):
    base = jnp.clip(jax.random.normal(key, (SEQ, D), jnp.float32), -6.0, 6.0)
    return base.astype(jnp.bfloat16)


def diff_pair(key):
    scale = 1.3 * D ** (-0.5)
    width = DIFF_HEADS * 2 * HEAD
    first = jnp.clip(jax.random.normal(jax.random.fold_in(key, 11), (D, width), jnp.float32), -4.0, 4.0) * scale
    second = jnp.clip(jax.random.normal(jax.random.fold_in(key, 12), (D, width), jnp.float32), -4.0, 4.0) * scale
    return (first, second)


def draw_query_diff(key, part):
    return diff_pair(key)[0].astype(jnp.bfloat16)


def draw_key_diff(key, part):
    return diff_pair(key)[1].astype(jnp.bfloat16)


def window_pair(key):
    scale = 1.3 * D ** (-0.5)
    keys = jnp.clip(jax.random.normal(jax.random.fold_in(key, 21), (KV_HEADS, D, HEAD), jnp.float32), -4.0, 4.0) * scale
    values = jnp.clip(jax.random.normal(jax.random.fold_in(key, 22), (KV_HEADS, D, HEAD), jnp.float32), -4.0, 4.0) * D ** (-0.5)
    queries = jnp.clip(jax.random.normal(jax.random.fold_in(key, 23), (D, WIN_HEADS * HEAD), jnp.float32), -4.0, 4.0) * scale
    return (queries, jnp.concatenate([keys, values], axis=2))


def draw_query_win(key, part):
    return window_pair(key)[0].astype(jnp.bfloat16)


def draw_keyval_win(key, part):
    return window_pair(key)[1].astype(jnp.bfloat16)


def shard_levels(rng, dims, split, least, top_value):
    level = 1.0
    for position, parts in split:
        steps = jax.random.uniform(jax.random.fold_in(jax.random.fold_in(rng, 6), position), (parts,), jnp.float32, least / len(split), top_value / len(split))
        level = level * jnp.repeat(jnp.exp(steps), dims[position] // parts).reshape((-1,) + (1,) * (len(dims) - 1 - position))
    return level


def scatter_about(rng, dims, scale, limit, shards=(), kind=jnp.bfloat16):
    values = scale * jax.random.normal(rng, dims, jnp.float32)
    if shards:
        values = values * shard_levels(rng, dims, shards, -0.22, 0.18)
    return jnp.clip(values, -limit, limit).astype(kind)


def setup_inputs(seed: int = 0, part: int = 0) -> dict:
    key_of = jax.random.split(jax.random.key(seed), 13)
    part_splits = jax.random.split(jax.random.fold_in(key_of[12], part), 13)
    return {
        "tokens": draw_tokens(jax.random.fold_in(jax.random.fold_in(key_of[12], part), 71), part),
        "norm_gain": jnp.clip(1.0 + 0.18 * jax.random.normal(key_of[1], (D,), jnp.float32), 0.1, 1.9),
        "query_diff": draw_query_diff(jax.random.fold_in(key_of[12], 71), part),
        "key_diff": draw_key_diff(jax.random.fold_in(key_of[12], 71), part),
        "value_diff": scatter_about(key_of[4], (D, DIFF_HEADS * VDIM), D ** -0.5, 0.09375, ((0, 16), (1, 8))),
        "lam": jnp.clip(0.3 + 0.5 * jax.random.uniform(key_of[5], (DIFF_HEADS,), jnp.float32) ** shard_levels(key_of[5], (DIFF_HEADS,), ((0, 8),), -0.2, 0.2), 0.3, 0.8),
        "output_norm_gain": jnp.clip(1.0 + 0.18 * jax.random.normal(key_of[6], (VDIM,), jnp.float32), 0.1, 1.9),
        "query_win": draw_query_win(jax.random.fold_in(key_of[12], 71), part),
        "keyval_win": draw_keyval_win(jax.random.fold_in(key_of[12], 71), part),
        "sink": jnp.clip(4.0 + 3.0 * jax.random.uniform(key_of[9], (WIN_HEADS,), jnp.float32) ** shard_levels(key_of[9], (WIN_HEADS,), ((0, 8),), -0.2, 0.2), 4.0, 7.0),
        "proj_diff": scatter_about(key_of[10], (DIFF_HEADS * VDIM, D), (DIFF_HEADS * VDIM) ** -0.5, 0.125, ((0, 8),)),
        "proj_win": scatter_about(key_of[11], (WIN_HEADS * HEAD, D), (6 * (WIN_HEADS * HEAD) ** -0.5), 0.79296875, ((0, 8),)),
    }


EPS = 1e-06

def root_mean_square_rows(values, gain):
    return values * lax.rsqrt(lax.optimization_barrier(jnp.mean(values * values, axis=-1, keepdims=True)) + EPS) * gain

def reference(tokens, norm_gain, query_diff, key_diff, value_diff, lam, output_norm_gain, query_win, keyval_win, sink, proj_diff, proj_win):
    seq = tokens.shape[0]
    normed = root_mean_square_rows(tokens.astype(jnp.float32), norm_gain).astype(jnp.bfloat16)

    def project(weight):
        return jnp.dot(normed, weight, preferred_element_type=jnp.float32).astype(jnp.bfloat16)
    q_diff = project(query_diff).reshape(seq, DIFF_HEADS, 2, HEAD)
    k_diff = project(key_diff).reshape(seq, DIFF_HEADS, 2, HEAD)
    v_diff = project(value_diff).reshape(seq, DIFF_HEADS, VDIM)
    q_win = project(query_win).reshape(seq, WIN_HEADS, HEAD)
    kv_win = jnp.stack([project(keyval_win[g]) for g in range(KV_HEADS)], axis=1)
    scale = HEAD ** (-0.5)
    qblock = math.gcd(seq, 512)

    def diff_head(args):
        q_head, k_head, v_head, lambda_head = args

        def one_block(q_rows):
            output_list = []
            for m in range(2):
                scores = jnp.dot(q_rows[:, m], k_head[:, m].T, preferred_element_type=jnp.float32) * scale
                top = lax.optimization_barrier(jnp.max(scores, axis=-1, keepdims=True))
                expo = jnp.exp(scores - top)
                total = lax.optimization_barrier(jnp.sum(expo, axis=-1, keepdims=True))
                output_list.append(jnp.dot(expo.astype(jnp.bfloat16), v_head, preferred_element_type=jnp.float32) / total)
            difference_output = output_list[0] - lambda_head * output_list[1]
            return root_mean_square_rows(difference_output, output_norm_gain).astype(jnp.bfloat16)
        result = lax.map(one_block, q_head.reshape(seq // qblock, qblock, 2, HEAD))
        return result.reshape(seq, VDIM)
    differential_output = lax.map(diff_head, (jnp.transpose(q_diff, (1, 0, 2, 3)), jnp.transpose(k_diff, (1, 0, 2, 3)), jnp.transpose(v_diff, (1, 0, 2)), lam))
    differential_output = jnp.transpose(differential_output, (1, 0, 2)).reshape(seq, DIFF_HEADS * VDIM)
    group = WIN_HEADS // KV_HEADS
    nblocks = seq // WINDOW
    q_blocks = q_win.reshape(nblocks, WINDOW, KV_HEADS, group, HEAD).astype(jnp.float32)
    padded = jnp.pad(kv_win, ((WINDOW, WINDOW), (0, 0), (0, 0))).reshape(nblocks + 2, WINDOW, KV_HEADS, 2 * HEAD)
    band = jnp.concatenate([padded[:-2], padded[1:-1], padded[2:]], axis=1).astype(jnp.float32)
    scores = jnp.einsum('nqgrd,nkgd->ngrqk', q_blocks, band[..., :HEAD]) * scale
    q_index = jnp.arange(WINDOW, dtype=jnp.int32)
    k_index = jnp.arange(3 * WINDOW, dtype=jnp.int32)
    offset = k_index[None, :] - WINDOW - q_index[:, None]
    key_pos = jnp.arange(nblocks, dtype=jnp.int32)[:, None] * WINDOW - WINDOW + k_index[None, :]
    valid = (jnp.abs(offset) <= WINDOW)[None] & ((key_pos >= 0) & (key_pos < seq))[:, None, :]
    scores = jnp.where(valid[:, None, None], scores, -jnp.inf)
    sink_logit = sink.reshape(KV_HEADS, group)[:, :, None, None]
    top = jnp.maximum(lax.optimization_barrier(jnp.max(scores, axis=-1, keepdims=True)), sink_logit)
    expo = jnp.exp(scores - top)
    weights = expo / (lax.optimization_barrier(jnp.sum(expo, axis=-1, keepdims=True)) + jnp.exp(sink_logit - top))
    weights = weights.astype(jnp.bfloat16).astype(jnp.float32)
    y_win = jnp.einsum('ngrqk,nkgd->nqgrd', weights, band[..., HEAD:]).astype(jnp.bfloat16)
    y_win = y_win.reshape(seq, WIN_HEADS * HEAD)
    total = jnp.dot(differential_output, proj_diff, preferred_element_type=jnp.float32)
    total = total + jnp.dot(y_win, proj_win, preferred_element_type=jnp.float32)
    return total.astype(jnp.bfloat16)
```

```python
import functools

import jax
import jax.numpy as jnp
from jax import lax
from jax.experimental import pallas as pl
from jax.experimental.pallas import tpu as pltpu
from jax.sharding import Mesh
from jax.sharding import PartitionSpec as P

HEAD = 128
WIN_HEADS = 16
KV_HEADS = 4
WINDOW = 128
VDIM = 256
NX = 4
TP = ("tp_0", "tp_1")
GRP_SP_TP = ("grp", "sp", "tp_0", "tp_1")
EPS = 1e-06
LOG2E = 1.4426950408889634
BF16 = jnp.bfloat16
F32 = jnp.float32
MESH = pl.DeviceIdType.MESH
DMA = pltpu.SemaphoreType.DMA
VMEM = pltpu.VMEM
ANY = pl.ANY


def remote(src, dst, send_sem, recv_sem, where):
    return pltpu.make_async_remote_copy(
        src_ref=src,
        dst_ref=dst,
        send_sem=send_sem,
        recv_sem=recv_sem,
        device_id=where,
        device_id_type=MESH,
    )


def greet(peers):
    barrier = pltpu.get_barrier_semaphore()
    for peer in peers:
        pl.semaphore_signal(barrier, inc=1, device_id=peer, device_id_type=MESH)
    pl.semaphore_wait(barrier, len(peers))


class Ring:
    def __init__(self, n, buf, half, send, recv):
        self.n, self.buf, self.half, self.send, self.recv = n, buf, half, send, recv
        self.me = lax.axis_index("sp")
        self.to = (
            {"sp": lax.rem(self.me + 1, n)},
            {"sp": lax.rem(self.me + n - 1, n)},
        )

    def origin(self, d, s):
        return lax.rem(self.me + (self.n - s if d == 0 else s), self.n)

    def piece(self, d, s, k, hops):
        b = k if d == 0 else 1 - k
        ref = self.buf.at[self.origin(d, hops), pl.ds(b * self.half, self.half)]
        return remote(ref, ref, self.send.at[d, s, k], self.recv.at[d, s, k], self.to[d])

    def start(self, s, k):
        for d in (0, 1):
            self.piece(d, s, k, s).start()

    def land(self, s, k):
        for d in (0, 1):
            self.piece(d, s, k, s + 1).wait_recv()

    def drain(self):
        last = self.n // 2 - 1

        def one(s, carry):
            for k in (0, 1):
                for d in (0, 1):
                    self.piece(d, s, k, s).wait_send()
            return carry

        lax.fori_loop(0, last, one, 0)
        for d in (0, 1):
            self.piece(d, last, 0, last).wait_send()


class Side:
    def __init__(self, own, slots, half, xs, xr, cs, cr):
        self.own, self.slots, self.half = own, slots, half
        self.xs, self.xr, self.cs, self.cr = xs, xr, cs, cr
        self.x = lax.axis_index("tp_0")
        self.c = lax.axis_index("tp_1")
        self.to = (
            {"tp_0": lax.rem(self.x + 1, NX)},
            {"tp_0": lax.rem(self.x + NX - 1, NX)},
        )
        self.other = {"tp_1": 1 - self.c}

    def spot(self, rel, h, core):
        slot = 2 * lax.rem(self.x + rel, NX) + core
        return self.slots.at[slot, pl.ds(h * self.half, self.half)]

    def source(self, rel, h):
        if rel == 0 and self.own is not None:
            return self.own.at[pl.ds(h * self.half, self.half)]
        return self.spot(rel, h, self.c)

    def half_of(self, d, k):
        return (0, 1, 0)[k] if d == 0 else (1, 0, 1)[k]

    def out(self, d, k):
        rel = 0 if k < 2 else (3 if d == 0 else 1)
        h = self.half_of(d, k)
        return remote(
            self.source(rel, h), self.spot(rel, h, self.c), self.xs.at[d, k], self.xr.at[d, k], self.to[d]
        )

    def inward(self, d, k):
        rel = (3 if d == 0 else 1) if k < 2 else 2
        h = self.half_of(d, k)
        ref = self.spot(rel, h, self.c)
        return rel, h, remote(ref, ref, self.xs.at[d, k], self.xr.at[d, k], self.to[d])

    def across(self, rel, h):
        return remote(
            self.source(rel, h), self.spot(rel, h, self.c), self.cs.at[rel, h], self.cr.at[rel, h], self.other
        )

    def start(self):
        for k in (0, 1):
            for d in (0, 1):
                self.out(d, k).start()
        for h in (0, 1):
            self.across(0, h).start()

    def step(self, k):
        for d in (0, 1):
            rel, h, copy = self.inward(d, k)
            copy.wait_recv()
            if k == 0:
                self.out(d, 2).start()
            self.across(rel, h).start()

    def finish(self):
        for rel in range(NX):
            for h in (0, 1):
                ref = self.spot(rel, h, 1 - self.c)
                remote(ref, ref, self.cs.at[rel, h], self.cr.at[rel, h], self.other).wait_recv()

    def drain(self):
        for k in (0, 1, 2):
            for d in (0, 1):
                self.out(d, k).wait_send()
        for rel in range(NX):
            for h in (0, 1):
                self.across(rel, h).wait_send()


def side_sems():
    return [DMA((2, 3)), DMA((2, 3)), DMA((NX, 2)), DMA((NX, 2))]


def project_kernel(
    n, heads_win, tok, gain, kd, vd, qd, qw, kvw, pw,
    kv_out, q_out, qw_out, kvw_out, pw_out,
    wbuf, raw, nbuf, acc, hold, lsem, zs, zr, *sems,
):
    me, x, c = (lax.axis_index(a) for a in ("sp", "tp_0", "tp_1"))
    t = 2 * x + c
    group = WIN_HEADS // KV_HEADS
    local = []
    at = 0
    for w in (kd, vd, qd, qw):
        width = w.shape[1]
        local.append((w, wbuf.at[me, :, pl.ds(at, width)]))
        at += width
    part = kvw.shape[2] // 2
    local.append(
        (
            kvw.at[t * heads_win // group, :, pl.ds(pl.multiple_of(c * part, part), part)],
            wbuf.at[me, :, pl.ds(at, part)],
        )
    )
    local.append((tok, raw.at[t]))
    local.append((pw, hold))
    local = [pltpu.make_async_copy(a, b, lsem.at[i]) for i, (a, b) in enumerate(local)]
    for copy in local:
        copy.start()
    keep = pltpu.make_async_copy(hold, pw_out.at[t], lsem.at[len(local)])

    ring = Ring(n, wbuf, wbuf.shape[1] // 2, zs, zr)
    rows = raw.shape[1]
    side = Side(None, raw, rows // 2, *sems[:4])
    late = Side(pw, pw_out, pw.shape[0] // 2, *sems[4:])
    greet([ring.to[0], ring.to[1], side.to[0], side.to[1], side.other])
    for copy in local[:5]:
        copy.wait()
    for k in (0, 1):
        ring.start(0, k)
    local[5].wait()
    side.start()
    acc[...] = jnp.zeros_like(acc)
    local[6].wait()
    keep.start()

    def normalise():
        tile = 16

        def one(i, carry):
            slot, r = i // (rows // tile), lax.rem(i, rows // tile)
            v = raw[slot, pl.ds(pl.multiple_of(r * tile, tile), tile), :].astype(F32)
            v = v * lax.rsqrt(jnp.mean(v * v, axis=-1, keepdims=True) + EPS) * gain[...]
            v = v.astype(BF16)
            depth = nbuf.shape[2]
            for o in range(n):
                nbuf[o, pl.ds(pl.multiple_of(i * tile, tile), tile), :] = v[:, o * depth : (o + 1) * depth]
            return carry

        lax.fori_loop(0, raw.shape[0] * rows // tile, one, 0)

    def accumulate(o):
        tile = 256

        def one(i, carry):
            r = pl.ds(pl.multiple_of(i * tile, tile), tile)
            acc[r, :] += jnp.dot(nbuf[o, r, :], wbuf[o], preferred_element_type=F32)
            return carry

        lax.fori_loop(0, acc.shape[0] // tile, one, 0)

    last = n // 2 - 1
    ready = 2

    def spread(count):
        def one(i, carry):
            accumulate(lax.rem(me + n - count + i, n))
            return carry

        lax.fori_loop(0, 2 * count + 1, one, 0)

    def step(s, carry):
        ring.land(s, 0)
        ring.start(s + 1, 0)

        @pl.when(s == 0)
        def _():
            side.step(0)

        @pl.when(s == 1)
        def _():
            side.step(1)

        ring.land(s, 1)
        ring.start(s + 1, 1)

        @pl.when(s == 1)
        def _():
            side.step(2)
            late.start()

        @pl.when(s == ready)
        def _():
            side.finish()
            normalise()
            spread(ready + 1)

        @pl.when(s == 3)
        def _():
            late.step(0)

        @pl.when(s == 5)
        def _():
            late.step(1)

        @pl.when(s > ready)
        def _():
            accumulate(lax.rem(me + n - s - 1, n))
            accumulate(lax.rem(me + s + 1, n))

        return carry

    lax.fori_loop(0, last - 1, step, 0)
    ring.land(last - 1, 0)
    ring.start(last, 0)
    ring.land(last - 1, 1)
    late.step(2)
    accumulate(lax.rem(me + n - last, n))
    accumulate(lax.rem(me + last, n))
    ring.land(last, 0)
    accumulate(lax.rem(me + last + 1, n))
    at = 0
    for out in (kv_out, q_out, qw_out, kvw_out):
        out[...] = acc[:, at : at + out.shape[1]].astype(out.dtype)
        at += out.shape[1]
    late.finish()
    keep.wait()
    ring.drain()
    side.drain()
    late.drain()


def attend_kernel(
    n, q, kv, qw, kvw, lam, ogain, sink, pd, pwg, out,
    kbuf, kw, pdb, pwb, top, tot, acc, y, yd, yv, yw, facc,
    lsem, zs, zr, hs, hr, us, ur, ws, wr, *sems,
):
    me, x, c = (lax.axis_index(a) for a in ("sp", "tp_0", "tp_1"))
    t = 2 * x + c
    rows = q.shape[0]
    block = rows // (2 * NX)
    local = [
        pltpu.make_async_copy(kv, kbuf.at[me], lsem.at[0]),
        pltpu.make_async_copy(kvw, kw.at[c, pl.ds(WINDOW, rows)], lsem.at[1]),
        pltpu.make_async_copy(pd, pdb.at[t], lsem.at[2]),
        pltpu.make_async_copy(pwg, pwb, lsem.at[3]),
    ]
    for copy in local:
        copy.start()
    ring = Ring(n, kbuf, kbuf.shape[1] // 2, zs, zr)
    side = Side(None, pdb, pd.shape[0] // 2, *sems)

    def peer(k):
        return {"tp_0": lax.rem(x + k // 2, NX), "tp_1": lax.rem(c + k % 2, 2)}

    def slot(px, pc):
        return 2 * lax.rem(px, NX) + lax.rem(pc, 2)

    others = range(1, 2 * NX)
    greet([ring.to[0], ring.to[1]] + [peer(k) for k in others])

    def edge(d, inward):
        src = pl.ds(rows, WINDOW) if d == 0 else pl.ds(WINDOW, WINDOW)
        dst = pl.ds(0, WINDOW) if d == 0 else pl.ds(rows + WINDOW, WINDOW)
        target = kw.at[c, dst]
        return remote(target if inward else kw.at[c, src], target, hs.at[d], hr.at[d], ring.to[d])

    spans = (pl.ds(WINDOW, rows), pl.ds(0, WINDOW), pl.ds(rows + WINDOW, WINDOW))

    def twin(i, inward):
        ref = kw.at[1 - c if inward else c, spans[i]]
        return remote(ref, ref, us.at[i], ur.at[i], side.other)

    def trade(src, dst, send, recv, k, inward):
        if inward:
            ref = dst.at[slot(x + NX - k // 2, c + k % 2)]
            return remote(ref, ref, send.at[k], recv.at[k], peer(k))
        return remote(src.at[slot(x + k // 2, c + k % 2)], dst.at[t], send.at[k], recv.at[k], peer(k))

    local[0].wait()
    for k in (0, 1):
        ring.start(0, k)
    local[1].wait()
    for d in (0, 1):
        edge(d, False).start()
    twin(0, False).start()
    local[2].wait()
    side.start()

    top[...] = jnp.full_like(top, -jnp.inf)
    tot[...] = jnp.zeros_like(tot)
    acc[...] = jnp.zeros_like(acc)
    scale = HEAD**-0.5
    tile = 256
    lanes = HEAD
    contract_last = (((1,), (1,)), ((), ()))

    def attend(o):
        def one(i, carry):
            r = pl.ds(pl.multiple_of(i * tile, tile), tile)
            values = kbuf[o, :, 2 * HEAD :]
            for m in range(2):
                cols = pl.ds(m * HEAD, HEAD)
                s = lax.dot_general(q[r, cols], kbuf[o, :, cols], contract_last, preferred_element_type=F32)
                s = s * (scale * LOG2E)
                reps = s.shape[1] // lanes
                was = top[m, r, :]
                now = jnp.maximum(was, jnp.max(s, axis=1, keepdims=True))
                fade = jnp.exp2(was - now)
                e = jnp.exp2(s - jnp.concatenate([now] * reps, axis=1))
                part = e[:, :lanes]
                for j in range(1, reps):
                    part = part + e[:, j * lanes : (j + 1) * lanes]
                tot[m, r, :] = tot[m, r, :] * fade + part
                top[m, r, :] = now
                acc[m, r, :] = acc[m, r, :] * jnp.concatenate([fade] * (VDIM // lanes), axis=1) + jnp.dot(
                    e.astype(BF16), values, preferred_element_type=F32
                )
            return carry

        lax.fori_loop(0, rows // tile, one, 0)

    def window():
        span = 3 * WINDOW
        heads = qw.shape[1] // HEAD
        i_q = lax.broadcasted_iota(jnp.int32, (WINDOW, span), 0)
        i_k = lax.broadcasted_iota(jnp.int32, (WINDOW, span), 1)
        near = jnp.abs(i_k - WINDOW - i_q) <= WINDOW

        def one(b, carry):
            r = pl.ds(pl.multiple_of(b * WINDOW, WINDOW), WINDOW)
            band = pl.ds(pl.multiple_of(b * WINDOW, WINDOW), span)
            where = i_k + (me * rows + b * WINDOW - WINDOW)
            valid = near & (where >= 0) & (where < n * rows)
            for h in range(heads):
                cols = pl.ds(h * HEAD, HEAD)
                s = lax.dot_general(qw[r, cols], kw[0, band, :], contract_last, preferred_element_type=F32)
                s = jnp.where(valid, s * scale, -jnp.inf)
                sunk = jnp.broadcast_to(sink[h : h + 1, :], (WINDOW, lanes))
                peak = jnp.maximum(jnp.max(s, axis=1, keepdims=True), sunk)
                e = jnp.exp(s - jnp.concatenate([peak] * 3, axis=1))
                whole = jnp.sum(e, axis=1, keepdims=True) + jnp.exp(sunk - peak)
                w = (e / jnp.concatenate([whole] * 3, axis=1)).astype(BF16)
                res = jnp.dot(w, kw[1, band, :], preferred_element_type=F32).astype(BF16)
                for j in range(WINDOW // block):
                    yv[b * (WINDOW // block) + j, :, cols] = res[j * block : (j + 1) * block]
            return carry

        lax.fori_loop(0, rows // WINDOW, one, 0)

    width = 512

    def project(ys, weights, first):
        def one(j, carry):
            cols = pl.ds(pl.multiple_of(j * width, width), width)
            total = None if first else facc[:, cols]
            for i in range(2 * NX):
                p = jnp.dot(ys[i], weights[i, :, cols], preferred_element_type=F32)
                total = p if total is None else total + p
            if first:
                facc[:, cols] = total
            else:
                out[:, cols] = total.astype(out.dtype)
            return carry

        lax.fori_loop(0, out.shape[1] // width, one, 0)

    attend(me)
    last = n // 2 - 1

    def step(s, carry):
        ring.land(s, 0)
        ring.start(s + 1, 0)

        @pl.when(s == 0)
        def _():
            for d in (0, 1):
                edge(d, True).wait_recv()
                twin(d + 1, False).start()

        @pl.when(s > 0)
        def _():
            attend(ring.origin(0, s))

        ring.land(s, 1)
        ring.start(s + 1, 1)

        @pl.when(s > 0)
        def _():
            attend(ring.origin(1, s))

        @pl.when(s == 1)
        def _():
            for i in range(3):
                twin(i, True).wait_recv()
            window()
            yw[t] = yv[t]

        @pl.when(s == 2)
        def _():
            for k in others:
                trade(yv, yw, ws, wr, k, False).start()
            side.step(0)

        @pl.when(s == 4)
        def _():
            local[3].wait()
            for k in others:
                trade(yv, yw, ws, wr, k, True).wait_recv()
            project(yw, pwb, True)
            side.step(1)

        return carry

    lax.fori_loop(0, last - 1, step, 0)
    ring.land(last - 1, 0)
    ring.start(last, 0)
    attend(ring.origin(0, last - 1))
    ring.land(last - 1, 1)
    attend(ring.origin(1, last - 1))
    side.step(2)

    def both(i, carry):
        attend(lax.rem(me + n - last + 2 * last * i, n))
        return carry

    lax.fori_loop(0, 2, both, 0)
    side.finish()
    ring.land(last, 0)
    attend(lax.rem(me + last + 1, n))

    def close(j, carry):
        r = pl.ds(pl.multiple_of(j * block, block), block)
        maps = [acc[m, r, :] / jnp.sum(tot[m, r, :], axis=1, keepdims=True) for m in range(2)]
        d = maps[0] - lam[...] * maps[1]
        d = d * lax.rsqrt(jnp.mean(d * d, axis=-1, keepdims=True) + EPS) * ogain[...]
        y[j] = d.astype(BF16)
        return carry

    lax.fori_loop(0, 2 * NX, close, 0)
    for k in others:
        trade(y, yd, us.at[pl.ds(3, 2 * NX)], ur.at[pl.ds(3, 2 * NX)], k, False).start()
    yd[t] = y[t]
    for k in others:
        trade(y, yd, us.at[pl.ds(3, 2 * NX)], ur.at[pl.ds(3, 2 * NX)], k, True).wait_recv()
    project(yd, pdb, False)
    for k in others:
        trade(y, yd, us.at[pl.ds(3, 2 * NX)], ur.at[pl.ds(3, 2 * NX)], k, False).wait_send()
        trade(yv, yw, ws, wr, k, False).wait_send()
    for d in (0, 1):
        edge(d, False).wait_send()
    for i in range(3):
        twin(i, False).wait_send()
    ring.drain()
    side.drain()


def call(kernel, ins, outs, scratch, ident, args):
    return pl.pallas_call(
        kernel,
        out_shape=[s for s, _ in outs],
        in_specs=[pl.BlockSpec(memory_space=m) for m in ins],
        out_specs=[pl.BlockSpec(memory_space=m) for _, m in outs],
        scratch_shapes=scratch,
        compiler_params=pltpu.CompilerParams(
            collective_id=ident, has_side_effects=True, vmem_limit_bytes=64_000_000
        ),
    )(*args)


def body(
    n, tokens, norm_gain, query_diff, key_diff, value_diff, lam, output_norm_gain,
    query_win, keyval_win, sink, proj_diff, proj_win,
):
    block, model = tokens.shape
    rows = block * 2 * NX
    depth = query_diff.shape[0]
    kvd = key_diff.shape[1] + value_diff.shape[1]
    part = keyval_win.shape[2] // 2
    wide = kvd + query_diff.shape[1] + query_win.shape[1] + part
    heads_win = sink.shape[0]
    shape = jax.ShapeDtypeStruct
    kv, q, qw, kvw, pwg = call(
        functools.partial(project_kernel, n, heads_win),
        [ANY, VMEM] + [ANY] * 6,
        [
            (shape((rows, kvd), BF16), VMEM),
            (shape((rows, query_diff.shape[1]), BF16), VMEM),
            (shape((rows, query_win.shape[1]), BF16), VMEM),
            (shape((rows, part), BF16), VMEM),
            (shape((2 * NX,) + proj_win.shape, BF16), ANY),
        ],
        [
            VMEM((n, depth, wide), BF16),
            VMEM((2 * NX, block, model), BF16),
            VMEM((n, rows, depth), BF16),
            VMEM((rows, wide), F32),
            VMEM(proj_win.shape, BF16),
            DMA((8,)),
            DMA((2, n // 2, 2)),
            DMA((2, n // 2, 2)),
        ]
        + side_sems()
        + side_sems(),
        0,
        (
            tokens, norm_gain.reshape(1, model), key_diff, value_diff, query_diff, query_win,
            keyval_win, proj_win,
        ),
    )
    (mixed,) = call(
        functools.partial(attend_kernel, n),
        [VMEM, ANY, VMEM, ANY, VMEM, VMEM, VMEM, ANY, ANY],
        [(shape((block, model), BF16), VMEM)],
        [
            VMEM((n, rows, kvd), BF16),
            VMEM((2, rows + 2 * WINDOW, part), BF16),
            VMEM((2 * NX,) + proj_diff.shape, BF16),
            VMEM((2 * NX,) + proj_win.shape, BF16),
            VMEM((2, rows, HEAD), F32),
            VMEM((2, rows, HEAD), F32),
            VMEM((2, rows, VDIM), F32),
            VMEM((2 * NX, block, VDIM), BF16),
            VMEM((2 * NX, block, VDIM), BF16),
            VMEM((2 * NX, block, query_win.shape[1]), BF16),
            VMEM((2 * NX, block, query_win.shape[1]), BF16),
            VMEM((block, model), F32),
            DMA((4,)),
            DMA((2, n // 2, 2)),
            DMA((2, n // 2, 2)),
            DMA((2,)),
            DMA((2,)),
            DMA((3 + 2 * NX,)),
            DMA((3 + 2 * NX,)),
            DMA((2 * NX,)),
            DMA((2 * NX,)),
        ]
        + side_sems(),
        1,
        (
            q, kv, qw, kvw,
            jnp.broadcast_to(lam[:, None], (1, VDIM)),
            output_norm_gain.reshape(1, VDIM),
            jnp.broadcast_to(sink[:, None], (heads_win, HEAD)),
            proj_diff, pwg,
        ),
    )
    return mixed


def solution(mesh):
    torus = Mesh(
        mesh.devices.reshape(mesh.shape["grp"], mesh.shape["sp"], NX, 2),
        ("grp", "sp", "tp_0", "tp_1"),
    )
    return jax.shard_map(
        functools.partial(body, mesh.shape["sp"]),
        mesh=torus,
        in_specs=(
            P(GRP_SP_TP, None),
            P(),
            P("sp", TP),
            P("sp", TP),
            P("sp", TP),
            P(TP),
            P(),
            P("sp", TP),
            P(None, "sp", None),
            P(TP),
            P(TP, None),
            P(TP, None),
        ),
        out_specs=P(GRP_SP_TP, None),
        check_vma=False,
    )
```

```python
import functools

import jax
import jax.numpy as jnp
from jax import lax
from jax.experimental import pallas as pl
from jax.experimental.pallas import tpu as pltpu
from jax.sharding import Mesh
from jax.sharding import PartitionSpec as P

HEAD = 128
WIN_HEADS = 16
KV_HEADS = 4
WINDOW = 128
VDIM = 256
NX = 4
CUT = 80
TP = ("tp_0", "tp_1")
GRP_SP_TP = ("grp", "sp", "tp_0", "tp_1")
EPS = 1e-06
LOG2E = 1.4426950408889634
BF16 = jnp.bfloat16
F32 = jnp.float32
MESH = pl.DeviceIdType.MESH
DMA = pltpu.SemaphoreType.DMA
VMEM = pltpu.VMEM
ANY = pl.ANY


def remote(src, dst, send_sem, recv_sem, where):
    return pltpu.make_async_remote_copy(
        src_ref=src,
        dst_ref=dst,
        send_sem=send_sem,
        recv_sem=recv_sem,
        device_id=where,
        device_id_type=MESH,
    )


def greet(peers):
    barrier = pltpu.get_barrier_semaphore()
    for peer in peers:
        pl.semaphore_signal(barrier, inc=1, device_id=peer, device_id_type=MESH)
    pl.semaphore_wait(barrier, len(peers))


class Ring:
    def __init__(self, n, buf, base, cuts, send, recv):
        self.n, self.buf, self.send, self.recv = n, buf, send, recv
        self.spans = (pl.ds(base, cuts[0]), pl.ds(base + cuts[0], cuts[1]))
        self.me = lax.axis_index("sp")
        self.to = (
            {"sp": lax.rem(self.me + 1, n)},
            {"sp": lax.rem(self.me + n - 1, n)},
        )

    def origin(self, d, s):
        return lax.rem(self.me + (self.n - s if d == 0 else s), self.n)

    def piece(self, d, s, k, hops):
        ref = self.buf.at[self.origin(d, hops), self.spans[k if d == 0 else 1 - k]]
        return remote(ref, ref, self.send.at[d, s, k], self.recv.at[d, s, k], self.to[d])

    def start(self, s, k):
        for d in (0, 1):
            self.piece(d, s, k, s).start()

    def land(self, s, k):
        for d in (0, 1):
            self.piece(d, s, k, s + 1).wait_recv()

    def drain(self):
        last = self.n // 2 - 1

        def one(s, carry):
            for k in (0, 1):
                for d in (0, 1):
                    self.piece(d, s, k, s).wait_send()
            return carry

        lax.fori_loop(0, last, one, 0)
        for d in (0, 1):
            self.piece(d, last, 0, last).wait_send()


class Swap:
    def __init__(self, n, buf, cut, send, recv):
        self.n, self.buf, self.cut, self.send, self.recv = n, buf, cut, send, recv
        g = lax.axis_index("grp")
        self.odd = lax.rem(g, 2)
        self.to = {"grp": g + 1 - 2 * self.odd}
        self.kept = buf.shape[1] - cut
        self.base = pl.multiple_of(self.odd * cut, 16)

    def piece(self, o, odd):
        ref = self.buf.at[o, pl.ds(pl.multiple_of(odd * self.kept, 16), self.cut)]
        return remote(ref, ref, self.send.at[o], self.recv.at[o], self.to)

    def start(self, o):
        self.piece(o, self.odd).start()

    def land(self, o):
        self.piece(o, 1 - self.odd).wait_recv()

    def drain(self):
        def one(i, carry):
            self.piece(lax.rem(lax.axis_index("sp") + i, self.n), self.odd).wait_send()
            return carry

        lax.fori_loop(1, self.n, one, 0)


class Side:
    def __init__(self, own, slots, half, xs, xr, cs, cr):
        self.own, self.slots, self.half = own, slots, half
        self.xs, self.xr, self.cs, self.cr = xs, xr, cs, cr
        self.x = lax.axis_index("tp_0")
        self.c = lax.axis_index("tp_1")
        self.to = (
            {"tp_0": lax.rem(self.x + 1, NX)},
            {"tp_0": lax.rem(self.x + NX - 1, NX)},
        )
        self.other = {"tp_1": 1 - self.c}

    def spot(self, rel, h, core):
        slot = 2 * lax.rem(self.x + rel, NX) + core
        return self.slots.at[slot, pl.ds(h * self.half, self.half)]

    def source(self, rel, h):
        if rel == 0 and self.own is not None:
            return self.own.at[pl.ds(h * self.half, self.half)]
        return self.spot(rel, h, self.c)

    def half_of(self, d, k):
        return (0, 1, 0)[k] if d == 0 else (1, 0, 1)[k]

    def out(self, d, k):
        rel = 0 if k < 2 else (3 if d == 0 else 1)
        h = self.half_of(d, k)
        return remote(
            self.source(rel, h), self.spot(rel, h, self.c), self.xs.at[d, k], self.xr.at[d, k], self.to[d]
        )

    def inward(self, d, k):
        rel = (3 if d == 0 else 1) if k < 2 else 2
        h = self.half_of(d, k)
        ref = self.spot(rel, h, self.c)
        return rel, h, remote(ref, ref, self.xs.at[d, k], self.xr.at[d, k], self.to[d])

    def across(self, rel, h):
        return remote(
            self.source(rel, h), self.spot(rel, h, self.c), self.cs.at[rel, h], self.cr.at[rel, h], self.other
        )

    def start(self):
        for k in (0, 1):
            for d in (0, 1):
                self.out(d, k).start()
        for h in (0, 1):
            self.across(0, h).start()

    def step(self, k):
        for d in (0, 1):
            rel, h, copy = self.inward(d, k)
            copy.wait_recv()
            if k == 0:
                self.out(d, 2).start()
            self.across(rel, h).start()

    def finish(self):
        for rel in range(NX):
            for h in (0, 1):
                ref = self.spot(rel, h, 1 - self.c)
                remote(ref, ref, self.cs.at[rel, h], self.cr.at[rel, h], self.other).wait_recv()

    def drain(self):
        for k in (0, 1, 2):
            for d in (0, 1):
                self.out(d, k).wait_send()
        for rel in range(NX):
            for h in (0, 1):
                self.across(rel, h).wait_send()


def side_sems():
    return [DMA((2, 3)), DMA((2, 3)), DMA((NX, 2)), DMA((NX, 2))]


def project_kernel(
    n, heads_win, tok, gain, kd, vd, qd, qw, kvw,
    kv_out, q_out, qw_out, kvw_out,
    wbuf, raw, nbuf, acc, lsem, zs, zr, ys, yr, *sems,
):
    me, x, c = (lax.axis_index(a) for a in ("sp", "tp_0", "tp_1"))
    t = 2 * x + c
    group = WIN_HEADS // KV_HEADS
    local = []
    at = 0
    for w in (kd, vd, qd, qw):
        width = w.shape[1]
        local.append((w, wbuf.at[me, :, pl.ds(at, width)]))
        at += width
    part = kvw.shape[2] // 2
    local.append(
        (
            kvw.at[t * heads_win // group, :, pl.ds(pl.multiple_of(c * part, part), part)],
            wbuf.at[me, :, pl.ds(at, part)],
        )
    )
    local.append((tok, raw.at[t]))
    local = [pltpu.make_async_copy(a, b, lsem.at[i]) for i, (a, b) in enumerate(local)]
    for copy in local:
        copy.start()

    swap = Swap(n, wbuf, CUT, ys, yr)
    ring = Ring(n, wbuf, swap.base, (96, swap.kept - 96), zs, zr)
    rows = raw.shape[1]
    side = Side(None, raw, rows // 2, *sems)
    greet([ring.to[0], ring.to[1], side.to[0], side.to[1], side.other, swap.to])
    for copy in local[:5]:
        copy.wait()
    for k in (0, 1):
        ring.start(0, k)
    local[5].wait()
    side.start()
    acc[...] = jnp.zeros_like(acc)

    def normalise():
        tile = 16

        def one(i, carry):
            slot, r = i // (rows // tile), lax.rem(i, rows // tile)
            v = raw[slot, pl.ds(pl.multiple_of(r * tile, tile), tile), :].astype(F32)
            v = v * lax.rsqrt(jnp.mean(v * v, axis=-1, keepdims=True) + EPS) * gain[...]
            v = v.astype(BF16)
            depth = nbuf.shape[2]
            for o in range(n):
                nbuf[o, pl.ds(pl.multiple_of(i * tile, tile), tile), :] = v[:, o * depth : (o + 1) * depth]
            return carry

        lax.fori_loop(0, raw.shape[0] * rows // tile, one, 0)

    def accumulate(o):
        tile = 256

        @pl.when(o != me)
        def _():
            swap.land(o)

        def one(i, carry):
            r = pl.ds(pl.multiple_of(i * tile, tile), tile)
            acc[r, :] += jnp.dot(nbuf[o, r, :], wbuf[o], preferred_element_type=F32)
            return carry

        lax.fori_loop(0, acc.shape[0] // tile, one, 0)

    last = n // 2 - 1
    ready = 3

    def spread(count):
        def one(i, carry):
            accumulate(lax.rem(me + n - count + i, n))
            return carry

        lax.fori_loop(0, 2 * count + 1, one, 0)

    def step(s, carry):
        ring.land(s, 0)
        ring.start(s + 1, 0)

        @pl.when(s == 1)
        def _():
            side.step(0)

        @pl.when(s == 2)
        def _():
            side.step(1)

        @pl.when(s > ready)
        def _():
            accumulate(ring.origin(0, s))

        ring.land(s, 1)
        ring.start(s + 1, 1)
        for d in (0, 1):
            swap.start(ring.origin(d, s + 1))

        @pl.when(s == 2)
        def _():
            side.step(2)

        @pl.when(s == ready)
        def _():
            side.finish()
            normalise()
            spread(ready)

        @pl.when(s > ready)
        def _():
            accumulate(ring.origin(1, s))

        return carry

    lax.fori_loop(0, last - 1, step, 0)
    ring.land(last - 1, 0)
    ring.start(last, 0)
    accumulate(ring.origin(0, last - 1))
    ring.land(last - 1, 1)
    for d in (0, 1):
        swap.start(ring.origin(d, last))
    accumulate(ring.origin(1, last - 1))
    ring.land(last, 0)
    swap.start(ring.origin(0, last + 1))

    def rest(i, carry):
        accumulate(lax.rem(me + jnp.where(i == 0, n - last, last + i - 1), n))
        return carry

    lax.fori_loop(0, 3, rest, 0)
    at = 0
    for out in (kv_out, q_out, qw_out, kvw_out):
        out[...] = acc[:, at : at + out.shape[1]].astype(out.dtype)
        at += out.shape[1]
    ring.drain()
    swap.drain()
    side.drain()


def attend_kernel(
    n, q, kv, qw, kvw, lam, ogain, sink, pd, pw, out,
    kbuf, kw, pdb, top, tot, acc, y, yd, yv, give, take, sums,
    lsem, zs, zr, hs, hr, us, ur, ws, wr, *sems,
):
    me, x, c = (lax.axis_index(a) for a in ("sp", "tp_0", "tp_1"))
    t = 2 * x + c
    rows = q.shape[0]
    block = rows // (2 * NX)
    local = [
        pltpu.make_async_copy(kv, kbuf.at[me], lsem.at[0]),
        pltpu.make_async_copy(kvw, kw.at[c, pl.ds(WINDOW, rows)], lsem.at[1]),
        pltpu.make_async_copy(pd, pdb.at[t], lsem.at[2]),
    ]
    for copy in local:
        copy.start()
    ring = Ring(n, kbuf, 0, (kbuf.shape[1] // 2,) * 2, zs, zr)
    side = Side(None, pdb, pd.shape[0] // 2, *sems)

    def peer(k):
        return {"tp_0": lax.rem(x + k // 2, NX), "tp_1": lax.rem(c + k % 2, 2)}

    def slot(px, pc):
        return 2 * lax.rem(px, NX) + lax.rem(pc, 2)

    others = range(1, 2 * NX)
    greet([ring.to[0], ring.to[1]] + [peer(k) for k in others])

    def edge(d, inward):
        src = pl.ds(rows, WINDOW) if d == 0 else pl.ds(WINDOW, WINDOW)
        dst = pl.ds(0, WINDOW) if d == 0 else pl.ds(rows + WINDOW, WINDOW)
        target = kw.at[c, dst]
        return remote(target if inward else kw.at[c, src], target, hs.at[d], hr.at[d], ring.to[d])

    spans = (pl.ds(WINDOW, rows), pl.ds(0, WINDOW), pl.ds(rows + WINDOW, WINDOW))

    def twin(i, inward):
        ref = kw.at[1 - c if inward else c, spans[i]]
        return remote(ref, ref, us.at[i], ur.at[i], side.other)

    def trade(src, dst, send, recv, k, inward):
        if inward:
            ref = dst.at[slot(x + NX - k // 2, c + k % 2)]
            return remote(ref, ref, send.at[k], recv.at[k], peer(k))
        return remote(src.at[slot(x + k // 2, c + k % 2)], dst.at[t], send.at[k], recv.at[k], peer(k))

    pass_on = remote(give, take, ws.at[0], wr.at[0], side.other)

    def deal(k, inward):
        to = lax.rem(x + k, NX)
        return remote(sums.at[k - 1] if inward else take.at[to], sums.at[k - 1], ws.at[k], wr.at[k], {"tp_0": to})

    local[0].wait()
    for k in (0, 1):
        ring.start(0, k)
    local[1].wait()
    for d in (0, 1):
        edge(d, False).start()
    twin(0, False).start()
    local[2].wait()
    side.start()

    top[...] = jnp.full_like(top, -jnp.inf)
    tot[...] = jnp.zeros_like(tot)
    acc[...] = jnp.zeros_like(acc)
    scale = HEAD**-0.5
    tile = 256
    lanes = HEAD
    contract_last = (((1,), (1,)), ((), ()))

    def attend(o):
        def one(i, carry):
            r = pl.ds(pl.multiple_of(i * tile, tile), tile)
            values = kbuf[o, :, 2 * HEAD :]
            for m in range(2):
                cols = pl.ds(m * HEAD, HEAD)
                s = lax.dot_general(q[r, cols], kbuf[o, :, cols], contract_last, preferred_element_type=F32)
                s = s * (scale * LOG2E)
                reps = s.shape[1] // lanes
                was = top[m, r, :]
                now = jnp.maximum(was, jnp.max(s, axis=1, keepdims=True))
                fade = jnp.exp2(was - now)
                e = jnp.exp2(s - jnp.concatenate([now] * reps, axis=1))
                part = e[:, :lanes]
                for j in range(1, reps):
                    part = part + e[:, j * lanes : (j + 1) * lanes]
                tot[m, r, :] = tot[m, r, :] * fade + part
                top[m, r, :] = now
                acc[m, r, :] = acc[m, r, :] * jnp.concatenate([fade] * (VDIM // lanes), axis=1) + jnp.dot(
                    e.astype(BF16), values, preferred_element_type=F32
                )
            return carry

        lax.fori_loop(0, rows // tile, one, 0)

    def window():
        span = 3 * WINDOW
        heads = qw.shape[1] // HEAD
        i_q = lax.broadcasted_iota(jnp.int32, (WINDOW, span), 0)
        i_k = lax.broadcasted_iota(jnp.int32, (WINDOW, span), 1)
        near = jnp.abs(i_k - WINDOW - i_q) <= WINDOW

        def one(b, carry):
            r = pl.ds(pl.multiple_of(b * WINDOW, WINDOW), WINDOW)
            band = pl.ds(pl.multiple_of(b * WINDOW, WINDOW), span)
            where = i_k + (me * rows + b * WINDOW - WINDOW)
            valid = near & (where >= 0) & (where < n * rows)
            for h in range(heads):
                cols = pl.ds(h * HEAD, HEAD)
                s = lax.dot_general(qw[r, cols], kw[0, band, :], contract_last, preferred_element_type=F32)
                s = jnp.where(valid, s * scale, -jnp.inf)
                sunk = jnp.broadcast_to(sink[h : h + 1, :], (WINDOW, lanes))
                peak = jnp.maximum(jnp.max(s, axis=1, keepdims=True), sunk)
                e = jnp.exp(s - jnp.concatenate([peak] * 3, axis=1))
                whole = jnp.sum(e, axis=1, keepdims=True) + jnp.exp(sunk - peak)
                w = (e / jnp.concatenate([whole] * 3, axis=1)).astype(BF16)
                res = jnp.dot(w, kw[1, band, :], preferred_element_type=F32).astype(BF16)
                for j in range(WINDOW // block):
                    yv[j % 2, b * (WINDOW // block // 2) + j // 2, :, cols] = res[j * block : (j + 1) * block]
            return carry

        lax.fori_loop(0, rows // WINDOW, one, 0)

    width = 512

    def columns(one):
        def run(j, carry):
            one(pl.ds(pl.multiple_of(j * width, width), width))
            return carry

        lax.fori_loop(0, out.shape[1] // width, run, 0)

    def window_rows(core, cols):
        ys = yv[core].reshape(NX * block, yv.shape[3])
        return jnp.dot(ys, pw[:, cols], preferred_element_type=F32).reshape(NX, block, width)

    def to_give(cols):
        give[:, :, cols] = window_rows(1 - c, cols).astype(BF16)

    def to_sum(cols):
        take[:, :, cols] = (window_rows(c, cols) + take[:, :, cols].astype(F32)).astype(BF16)

    def to_out(cols):
        total = take[x, :, cols].astype(F32)
        for k in range(1, NX):
            total = total + sums[k - 1, :, cols].astype(F32)
        for i in range(2 * NX):
            total = total + jnp.dot(yd[i], pdb[i, :, cols], preferred_element_type=F32)
        out[:, cols] = total.astype(out.dtype)

    attend(me)
    last = n // 2 - 1

    def step(s, carry):
        ring.land(s, 0)
        ring.start(s + 1, 0)

        @pl.when(s == 0)
        def _():
            for d in (0, 1):
                edge(d, True).wait_recv()
                twin(d + 1, False).start()

        @pl.when(s > 0)
        def _():
            attend(ring.origin(0, s))

        ring.land(s, 1)
        ring.start(s + 1, 1)

        @pl.when(s > 0)
        def _():
            attend(ring.origin(1, s))

        @pl.when(s == 1)
        def _():
            for i in range(3):
                twin(i, True).wait_recv()
            window()

        @pl.when(s == 2)
        def _():
            side.step(0)
            columns(to_give)
            pass_on.start()

        @pl.when(s == 3)
        def _():
            pass_on.wait_recv()
            columns(to_sum)

        @pl.when(s == 4)
        def _():
            for k in range(1, NX):
                deal(k, False).start()
            side.step(1)

        return carry

    lax.fori_loop(0, last - 1, step, 0)
    ring.land(last - 1, 0)
    ring.start(last, 0)
    attend(ring.origin(0, last - 1))
    ring.land(last - 1, 1)
    attend(ring.origin(1, last - 1))
    side.step(2)

    def both(i, carry):
        attend(lax.rem(me + n - last + 2 * last * i, n))
        return carry

    lax.fori_loop(0, 2, both, 0)
    side.finish()
    for k in range(1, NX):
        deal(k, True).wait_recv()
    ring.land(last, 0)
    attend(lax.rem(me + last + 1, n))

    def close(j, carry):
        r = pl.ds(pl.multiple_of(j * block, block), block)
        maps = [acc[m, r, :] / jnp.sum(tot[m, r, :], axis=1, keepdims=True) for m in range(2)]
        d = maps[0] - lam[...] * maps[1]
        d = d * lax.rsqrt(jnp.mean(d * d, axis=-1, keepdims=True) + EPS) * ogain[...]
        y[j] = d.astype(BF16)
        return carry

    lax.fori_loop(0, 2 * NX, close, 0)
    for k in others:
        trade(y, yd, us.at[pl.ds(3, 2 * NX)], ur.at[pl.ds(3, 2 * NX)], k, False).start()
    yd[t] = y[t]
    for k in others:
        trade(y, yd, us.at[pl.ds(3, 2 * NX)], ur.at[pl.ds(3, 2 * NX)], k, True).wait_recv()
    columns(to_out)
    for k in others:
        trade(y, yd, us.at[pl.ds(3, 2 * NX)], ur.at[pl.ds(3, 2 * NX)], k, False).wait_send()
    for d in (0, 1):
        edge(d, False).wait_send()
    for i in range(3):
        twin(i, False).wait_send()
    pass_on.wait_send()
    for k in range(1, NX):
        deal(k, False).wait_send()
    ring.drain()
    side.drain()


def call(kernel, ins, outs, scratch, ident, args):
    return pl.pallas_call(
        kernel,
        out_shape=[s for s, _ in outs],
        in_specs=[pl.BlockSpec(memory_space=m) for m in ins],
        out_specs=[pl.BlockSpec(memory_space=m) for _, m in outs],
        scratch_shapes=scratch,
        compiler_params=pltpu.CompilerParams(
            collective_id=ident, has_side_effects=True, vmem_limit_bytes=64_000_000
        ),
    )(*args)


def body(
    n, tokens, norm_gain, query_diff, key_diff, value_diff, lam, output_norm_gain,
    query_win, keyval_win, sink, proj_diff, proj_win,
):
    block, model = tokens.shape
    rows = block * 2 * NX
    depth = query_diff.shape[0]
    kvd = key_diff.shape[1] + value_diff.shape[1]
    part = keyval_win.shape[2] // 2
    wide = kvd + query_diff.shape[1] + query_win.shape[1] + part
    heads_win = sink.shape[0]
    shape = jax.ShapeDtypeStruct
    kv, q, qw, kvw = call(
        functools.partial(project_kernel, n, heads_win),
        [ANY, VMEM] + [ANY] * 5,
        [
            (shape((rows, kvd), BF16), VMEM),
            (shape((rows, query_diff.shape[1]), BF16), VMEM),
            (shape((rows, query_win.shape[1]), BF16), VMEM),
            (shape((rows, part), BF16), VMEM),
        ],
        [
            VMEM((n, depth, wide), BF16),
            VMEM((2 * NX, block, model), BF16),
            VMEM((n, rows, depth), BF16),
            VMEM((rows, wide), F32),
            DMA((6,)),
            DMA((2, n // 2, 2)),
            DMA((2, n // 2, 2)),
            DMA((n,)),
            DMA((n,)),
        ]
        + side_sems(),
        0,
        (
            tokens, norm_gain.reshape(1, model), key_diff, value_diff, query_diff, query_win,
            keyval_win,
        ),
    )
    (mixed,) = call(
        functools.partial(attend_kernel, n),
        [VMEM, ANY, VMEM, ANY, VMEM, VMEM, VMEM, ANY, VMEM],
        [(shape((block, model), BF16), VMEM)],
        [
            VMEM((n, rows, kvd), BF16),
            VMEM((2, rows + 2 * WINDOW, part), BF16),
            VMEM((2 * NX,) + proj_diff.shape, BF16),
            VMEM((2, rows, HEAD), F32),
            VMEM((2, rows, HEAD), F32),
            VMEM((2, rows, VDIM), F32),
            VMEM((2 * NX, block, VDIM), BF16),
            VMEM((2 * NX, block, VDIM), BF16),
            VMEM((2, NX, block, query_win.shape[1]), BF16),
            VMEM((NX, block, model), BF16),
            VMEM((NX, block, model), BF16),
            VMEM((NX - 1, block, model), BF16),
            DMA((3,)),
            DMA((2, n // 2, 2)),
            DMA((2, n // 2, 2)),
            DMA((2,)),
            DMA((2,)),
            DMA((3 + 2 * NX,)),
            DMA((3 + 2 * NX,)),
            DMA((NX,)),
            DMA((NX,)),
        ]
        + side_sems(),
        1,
        (
            q, kv, qw, kvw,
            jnp.broadcast_to(lam[:, None], (1, VDIM)),
            output_norm_gain.reshape(1, VDIM),
            jnp.broadcast_to(sink[:, None], (heads_win, HEAD)),
            proj_diff, proj_win,
        ),
    )
    return mixed


def solution(mesh):
    torus = Mesh(
        mesh.devices.reshape(mesh.shape["grp"], mesh.shape["sp"], NX, 2),
        ("grp", "sp", "tp_0", "tp_1"),
    )
    return jax.shard_map(
        functools.partial(body, mesh.shape["sp"]),
        mesh=torus,
        in_specs=(
            P(GRP_SP_TP, None),
            P(),
            P("sp", TP),
            P("sp", TP),
            P("sp", TP),
            P(TP),
            P(),
            P("sp", TP),
            P(None, "sp", None),
            P(TP),
            P(TP, None),
            P(TP, None),
        ),
        out_specs=P(GRP_SP_TP, None),
        check_vma=False,
    )
```

```python
import functools

import jax
import jax.numpy as jnp
from jax import lax
from jax.experimental import pallas as pl
from jax.experimental.pallas import tpu as pltpu
from jax.sharding import Mesh
from jax.sharding import PartitionSpec as P

HEAD = 128
WIN_HEADS = 16
KV_HEADS = 4
WINDOW = 128
VDIM = 256
NX = 4
CUT = 80
TP = ("tp_0", "tp_1")
GRP_SP_TP = ("grp", "sp", "tp_0", "tp_1")
EPS = 1e-06
LOG2E = 1.4426950408889634
BF16 = jnp.bfloat16
F32 = jnp.float32
MESH = pl.DeviceIdType.MESH
DMA = pltpu.SemaphoreType.DMA
VMEM = pltpu.VMEM
ANY = pl.ANY


def remote(src, dst, send_sem, recv_sem, where):
    return pltpu.make_async_remote_copy(
        src_ref=src,
        dst_ref=dst,
        send_sem=send_sem,
        recv_sem=recv_sem,
        device_id=where,
        device_id_type=MESH,
    )


def greet(peers):
    barrier = pltpu.get_barrier_semaphore()
    for peer in peers:
        pl.semaphore_signal(barrier, inc=1, device_id=peer, device_id_type=MESH)
    pl.semaphore_wait(barrier, len(peers))


class Ring:
    def __init__(self, n, buf, base, cuts, send, recv):
        self.n, self.buf, self.send, self.recv = n, buf, send, recv
        self.spans = []
        for cut in cuts:
            self.spans.append(pl.ds(base, cut))
            base = base + cut
        self.count = len(cuts)
        self.me = lax.axis_index("sp")
        self.to = (
            {"sp": lax.rem(self.me + 1, n)},
            {"sp": lax.rem(self.me + n - 1, n)},
        )

    def origin(self, d, s):
        return lax.rem(self.me + (self.n - s if d == 0 else s), self.n)

    def piece(self, d, s, k, hops):
        ref = self.buf.at[self.origin(d, hops), self.spans[k if d == 0 else self.count - 1 - k]]
        return remote(ref, ref, self.send.at[d, s, k], self.recv.at[d, s, k], self.to[d])

    def start(self, s, k):
        for d in (0, 1):
            self.piece(d, s, k, s).start()

    def land(self, s, k):
        for d in (0, 1):
            self.piece(d, s, k, s + 1).wait_recv()

    def drain(self):
        last = self.n // 2 - 1

        def one(s, carry):
            for k in range(self.count):
                for d in (0, 1):
                    self.piece(d, s, k, s).wait_send()
            return carry

        lax.fori_loop(0, last, one, 0)
        for k in range(self.count // 2):
            for d in (0, 1):
                self.piece(d, last, k, last).wait_send()


class Swap:
    def __init__(self, n, buf, cut, send, recv):
        self.n, self.buf, self.cut, self.send, self.recv = n, buf, cut, send, recv
        g = lax.axis_index("grp")
        self.odd = lax.rem(g, 2)
        self.to = {"grp": g + 1 - 2 * self.odd}
        self.kept = buf.shape[1] - cut
        self.base = pl.multiple_of(self.odd * cut, 16)

    def piece(self, o, odd):
        ref = self.buf.at[o, pl.ds(pl.multiple_of(odd * self.kept, 16), self.cut)]
        return remote(ref, ref, self.send.at[o], self.recv.at[o], self.to)

    def start(self, o):
        self.piece(o, self.odd).start()

    def land(self, o):
        self.piece(o, 1 - self.odd).wait_recv()

    def drain(self):
        def one(i, carry):
            self.piece(lax.rem(lax.axis_index("sp") + i, self.n), self.odd).wait_send()
            return carry

        lax.fori_loop(1, self.n, one, 0)


class Side:
    def __init__(self, own, slots, half, xs, xr, cs, cr):
        self.own, self.slots, self.half = own, slots, half
        self.xs, self.xr, self.cs, self.cr = xs, xr, cs, cr
        self.x = lax.axis_index("tp_0")
        self.c = lax.axis_index("tp_1")
        self.to = (
            {"tp_0": lax.rem(self.x + 1, NX)},
            {"tp_0": lax.rem(self.x + NX - 1, NX)},
        )
        self.other = {"tp_1": 1 - self.c}

    def spot(self, rel, h, core):
        slot = 2 * lax.rem(self.x + rel, NX) + core
        return self.slots.at[slot, pl.ds(h * self.half, self.half)]

    def source(self, rel, h):
        if rel == 0 and self.own is not None:
            return self.own.at[pl.ds(h * self.half, self.half)]
        return self.spot(rel, h, self.c)

    def half_of(self, d, k):
        return (0, 1, 0)[k] if d == 0 else (1, 0, 1)[k]

    def out(self, d, k):
        rel = 0 if k < 2 else (3 if d == 0 else 1)
        h = self.half_of(d, k)
        return remote(
            self.source(rel, h), self.spot(rel, h, self.c), self.xs.at[d, k], self.xr.at[d, k], self.to[d]
        )

    def inward(self, d, k):
        rel = (3 if d == 0 else 1) if k < 2 else 2
        h = self.half_of(d, k)
        ref = self.spot(rel, h, self.c)
        return rel, h, remote(ref, ref, self.xs.at[d, k], self.xr.at[d, k], self.to[d])

    def across(self, rel, h):
        return remote(
            self.source(rel, h), self.spot(rel, h, self.c), self.cs.at[rel, h], self.cr.at[rel, h], self.other
        )

    def start(self):
        for k in (0, 1):
            for d in (0, 1):
                self.out(d, k).start()
        for h in (0, 1):
            self.across(0, h).start()

    def step(self, k):
        for d in (0, 1):
            rel, h, copy = self.inward(d, k)
            copy.wait_recv()
            if k == 0:
                self.out(d, 2).start()
            self.across(rel, h).start()

    def finish(self):
        for rel in range(NX):
            for h in (0, 1):
                ref = self.spot(rel, h, 1 - self.c)
                remote(ref, ref, self.cs.at[rel, h], self.cr.at[rel, h], self.other).wait_recv()

    def drain(self):
        for k in (0, 1, 2):
            for d in (0, 1):
                self.out(d, k).wait_send()
        for rel in range(NX):
            for h in (0, 1):
                self.across(rel, h).wait_send()


def side_sems():
    return [DMA((2, 3)), DMA((2, 3)), DMA((NX, 2)), DMA((NX, 2))]


def layer_kernel(
    n, heads_win, tok, gain, kd, vd, qd, qwd, kvw, pd, pw, lam, sink, ogain, out,
    w1, w2, raw, nbuf, acc1, acc2, kbuf, pdb, pwb, q, qw, kw, top, tot, acc, y, yd, yv, give, take, sums, facc,
    lsem, z1s, z1r, y1s, y1r, z2s, z2r, y2s, y2r, zks, zkr, hs, hr, us, ur, ts, tr, ws, wr, *sems,
):
    me, x, c = (lax.axis_index(a) for a in ("sp", "tp_0", "tp_1"))
    t = 2 * x + c
    block = raw.shape[1]
    rows = 2 * NX * block
    depth = w1.shape[1]
    part = kvw.shape[2] // 2
    head = t * heads_win // (WIN_HEADS // KV_HEADS)
    wq = qwd.shape[1]
    local = []
    at = 0
    for w in (kd, vd, qd):
        local.append((w, w1.at[me, :, pl.ds(at, w.shape[1])]))
        at += w.shape[1]
    local += [
        (qwd, w2.at[me, :, pl.ds(0, wq)]),
        (kvw.at[head, :, pl.ds(pl.multiple_of(c * part, part), part)], w2.at[me, :, pl.ds(wq, part)]),
        (tok, raw.at[t]),
        (pd, pdb.at[t]),
        (pw, pwb),
    ]
    local = [pltpu.make_async_copy(a, b, lsem.at[i]) for i, (a, b) in enumerate(local)]
    for copy in local:
        copy.start()

    swap1 = Swap(n, w1, CUT, y1s, y1r)
    swap2 = Swap(n, w2, depth // 2, y2s, y2r)
    ring1 = Ring(n, w1, swap1.base, (48, 48, 48, swap1.kept - 144), z1s, z1r)
    ring2 = Ring(n, w2, swap2.base, (depth // 4,) * 2, z2s, z2r)
    ring = Ring(n, kbuf, 0, (rows // 4,) * 4, zks, zkr)
    side = Side(None, raw, block // 2, *sems[:4])
    late = Side(None, pdb, depth // 2, *sems[4:])

    def peer(k):
        return {"tp_0": lax.rem(x + k // 2, NX), "tp_1": lax.rem(c + k % 2, 2)}

    greet([ring.to[0], ring.to[1], swap1.to] + [peer(k) for k in range(1, 2 * NX)])

    for copy in local[:3]:
        copy.wait()
    for k in range(4):
        ring1.start(0, k)
    local[5].wait()
    side.start()
    acc1[...] = jnp.zeros_like(acc1)
    acc2[...] = jnp.zeros_like(acc2)
    top[...] = jnp.full_like(top, -jnp.inf)
    tot[...] = jnp.zeros_like(tot)
    acc[...] = jnp.zeros_like(acc)
    for copy in local[3:5] + local[6:]:
        copy.wait()

    def normalise(quarter):
        tile = 32
        per = raw.shape[0] * block // tile // 4

        def one(j, carry):
            i = quarter * per + j
            slot, r = i // (block // tile), lax.rem(i, block // tile)
            v = raw[slot, pl.ds(pl.multiple_of(r * tile, tile), tile), :].astype(F32)
            v = v * lax.rsqrt(jnp.mean(v * v, axis=-1, keepdims=True) + EPS) * gain[...]
            v = v.astype(BF16)
            for o in range(n):
                nbuf[o, pl.ds(pl.multiple_of(i * tile, tile), tile), :] = v[:, o * depth : (o + 1) * depth]
            return carry

        lax.fori_loop(0, per, one, 0)

    def gather(w, swap, total, lo, hi):
        def one(j, carry):
            o = lax.rem(me + jnp.where(lax.rem(j, 2) == 1, (j + 1) // 2, n - j // 2), n)

            @pl.when(j > 0)
            def _():
                swap.land(o)

            total[...] += jnp.dot(nbuf[o], w[o], preferred_element_type=F32)
            return carry

        lax.fori_loop(lo, hi, one, 0)

    last = n // 2 - 1

    def swap_both(swap, ring_, hops):
        for d in (0, 1):
            swap.start(ring_.origin(d, hops))

    def hop2(s, k):
        ring2.land(s, k)
        ring2.start(s + 1, k)
        if k == 1:
            swap_both(swap2, ring2, s + 1)

    def phase1(s, carry):
        for k in range(4):
            ring1.land(s, k)
            ring1.start(s + 1, k)
            if k == 0:
                for i in range(3):

                    @pl.when(s == i + 1)
                    def _():
                        side.step(i)

                @pl.when(s == last - 3)
                def _():
                    side.finish()
                    late.start()

            @pl.when(s == last - 3)
            def _():
                normalise(k)

            @pl.when(s == last - 2)
            def _():
                gather(w1, swap1, acc1, 3 * k, min(3 * k + 3, 2 * last - 3))

            if k % 2 == 1:

                @pl.when(s >= 2)
                def _():
                    hop2(s - 2, k // 2)

        swap_both(swap1, ring1, s + 1)

        @pl.when(s == 1)
        def _():
            for k in (0, 1):
                ring2.start(0, k)

        return carry

    lax.fori_loop(0, last - 1, phase1, 0)
    done = 2 * last - 3
    for k in range(4):
        ring1.land(last - 1, k)
        if k < 2:
            ring1.start(last, k)
        if k % 2 == 0:
            gather(w1, swap1, acc1, done + k // 2, done + k // 2 + 1)
        else:
            hop2(last - 3, k // 2)
    swap_both(swap1, ring1, last)
    for k in (0, 1):
        ring1.land(last, k)
    swap1.start(ring1.origin(0, last + 1))
    late.step(0)
    for k in (0, 1):
        hop2(last - 2, k)
    gather(w1, swap1, acc1, done + 2, done + 4)
    ring2.land(last - 1, 0)
    ring2.start(last, 0)
    ring2.land(last - 1, 1)
    swap_both(swap2, ring2, last)
    gather(w1, swap1, acc1, n - 1, n)
    kvd = kbuf.shape[2]
    kbuf[me] = acc1[:, :kvd].astype(BF16)
    q[...] = acc1[:, kvd:].astype(BF16)
    for k in range(4):
        ring.start(0, k)

    def edge(d, inward):
        src = pl.ds(rows, WINDOW) if d == 0 else pl.ds(WINDOW, WINDOW)
        dst = pl.ds(0, WINDOW) if d == 0 else pl.ds(rows + WINDOW, WINDOW)
        target = kw.at[c, dst]
        return remote(target if inward else kw.at[c, src], target, hs.at[d], hr.at[d], ring.to[d])

    spans = (pl.ds(WINDOW, rows), pl.ds(0, WINDOW), pl.ds(rows + WINDOW, WINDOW))

    def twin(i, inward):
        ref = kw.at[1 - c if inward else c, spans[i]]
        return remote(ref, ref, us.at[i], ur.at[i], side.other)

    def trade(k, inward):
        if inward:
            ref = yd.at[2 * lax.rem(x + NX - k // 2, NX) + lax.rem(c + k % 2, 2)]
            return remote(ref, ref, ts.at[k], tr.at[k], peer(k))
        src = y.at[2 * lax.rem(x + k // 2, NX) + lax.rem(c + k % 2, 2)]
        return remote(src, yd.at[t], ts.at[k], tr.at[k], peer(k))

    pass_on = remote(give, take, ws.at[0], wr.at[0], side.other)

    def deal(k, inward):
        to = lax.rem(x + k, NX)
        return remote(sums.at[k - 1] if inward else take.at[to], sums.at[k - 1], ws.at[k], wr.at[k], {"tp_0": to})

    scale = HEAD**-0.5
    lanes = HEAD
    contract_last = (((1,), (1,)), ((), ()))

    def attend(o):
        def one(m, carry):
            cols = pl.ds(pl.multiple_of(m * HEAD, HEAD), HEAD)
            s = lax.dot_general(q[:, cols], kbuf[o, :, cols], contract_last, preferred_element_type=F32)
            s = s * (scale * LOG2E)
            reps = s.shape[1] // lanes
            was = top[m]
            now = jnp.maximum(was, jnp.max(s, axis=1, keepdims=True))
            fade = jnp.exp2(was - now)
            e = jnp.exp2(s - jnp.concatenate([now] * reps, axis=1))
            some = e[:, :lanes]
            for j in range(1, reps):
                some = some + e[:, j * lanes : (j + 1) * lanes]
            tot[m] = tot[m] * fade + some
            top[m] = now
            acc[m] = acc[m] * jnp.concatenate([fade] * (VDIM // lanes), axis=1) + jnp.dot(
                e.astype(BF16), kbuf[o, :, 2 * HEAD :], preferred_element_type=F32
            )
            return carry

        for m in range(2):
            one(m, 0)

    def window(lo, hi):
        span = 3 * WINDOW
        heads = wq // HEAD
        i_q = lax.broadcasted_iota(jnp.int32, (WINDOW, span), 0)
        i_k = lax.broadcasted_iota(jnp.int32, (WINDOW, span), 1)
        near = jnp.abs(i_k - WINDOW - i_q) <= WINDOW

        def one(b, carry):
            r = pl.ds(pl.multiple_of(b * WINDOW, WINDOW), WINDOW)
            band = pl.ds(pl.multiple_of(b * WINDOW, WINDOW), span)
            where = i_k + (me * rows + b * WINDOW - WINDOW)
            valid = near & (where >= 0) & (where < n * rows)
            for h in range(heads):
                cols = pl.ds(h * HEAD, HEAD)
                s = lax.dot_general(qw[r, cols], kw[0, band, :], contract_last, preferred_element_type=F32)
                s = jnp.where(valid, s * scale, -jnp.inf)
                sunk = jnp.full((WINDOW, lanes), sink[h], F32)
                peak = jnp.maximum(jnp.max(s, axis=1, keepdims=True), sunk)
                e = jnp.exp(s - jnp.concatenate([peak] * 3, axis=1))
                whole = jnp.sum(e, axis=1, keepdims=True) + jnp.exp(sunk - peak)
                w = (e / jnp.concatenate([whole] * 3, axis=1)).astype(BF16)
                res = jnp.dot(w, kw[1, band, :], preferred_element_type=F32).astype(BF16)
                for j in range(WINDOW // block):
                    yv[j % 2, b * (WINDOW // block // 2) + j // 2, :, cols] = res[j * block : (j + 1) * block]
            return carry

        lax.fori_loop(lo, hi, one, 0)

    width = 512

    def columns(one):
        def run(j, carry):
            one(pl.ds(pl.multiple_of(j * width, width), width))
            return carry

        lax.fori_loop(0, out.shape[1] // width, run, 0)

    def window_rows(core, cols):
        ys = yv[core].reshape(NX * block, wq)
        return jnp.dot(ys, pwb[:, cols], preferred_element_type=F32).reshape(NX, block, width)

    def to_give(cols):
        give[:, :, cols] = window_rows(1 - c, cols).astype(BF16)

    def to_sum(cols):
        take[:, :, cols] = (window_rows(c, cols) + take[:, :, cols].astype(F32)).astype(BF16)

    attend(me)

    def phase2(s, carry):
        for k in range(4):
            ring.land(s, k)
            ring.start(s + 1, k)
            if k == 0:

                @pl.when(s == 0)
                def _():
                    ring2.land(last, 0)
                    swap2.start(ring2.origin(0, last + 1))

                @pl.when(s == 1)
                def _():
                    gather(w2, swap2, acc2, 0, n // 2)

                @pl.when(s == 2)
                def _():
                    for d in (0, 1):
                        edge(d, True).wait_recv()
                        twin(d + 1, False).start()
                    late.step(2)

                @pl.when(s == 3)
                def _():
                    window(rows // WINDOW // 2, rows // WINDOW)

                @pl.when(s == 4)
                def _():
                    pass_on.wait_recv()
                    columns(to_sum)
                    for i in range(1, NX):
                        deal(i, False).start()

            if k == 2:

                @pl.when(s == 0)
                def _():
                    late.step(1)

                @pl.when(s == 1)
                def _():
                    gather(w2, swap2, acc2, n // 2, n)
                    kw[c, spans[0]] = acc2[:, wq:].astype(BF16)
                    qw[...] = acc2[:, :wq].astype(BF16)
                    for d in (0, 1):
                        edge(d, False).start()
                    twin(0, False).start()

                @pl.when(s == 2)
                def _():
                    for i in range(3):
                        twin(i, True).wait_recv()
                    window(0, rows // WINDOW // 2)

                @pl.when(s == 3)
                def _():
                    columns(to_give)
                    pass_on.start()

            if k % 2 == 1:

                @pl.when(s > 0)
                def _():
                    attend(ring.origin(k // 2, s))

        return carry

    lax.fori_loop(0, last - 1, phase2, 0)
    for k in range(4):
        ring.land(last - 1, k)
        if k < 2:
            ring.start(last, k)
        if k % 2 == 1:
            attend(ring.origin(k // 2, last - 1))
    late.finish()
    for k in range(1, NX):
        deal(k, True).wait_recv()
    facc[...] = take[x].astype(F32)
    for k in range(1, NX):
        facc[...] += sums[k - 1].astype(F32)

    def both(i, carry):
        attend(lax.rem(me + n - last + 2 * last * i, n))
        return carry

    lax.fori_loop(0, 2, both, 0)
    for k in (0, 1):
        ring.land(last, k)
    attend(lax.rem(me + last + 1, n))

    def close(j, carry):
        r = pl.ds(pl.multiple_of(j * block, block), block)
        maps = [acc[m, r, :] / jnp.sum(tot[m, r, :], axis=1, keepdims=True) for m in range(2)]
        d = maps[0] - lam[0] * maps[1]
        d = d * lax.rsqrt(jnp.mean(d * d, axis=-1, keepdims=True) + EPS) * ogain[...]
        y[j] = d.astype(BF16)
        return carry

    lax.fori_loop(0, 2 * NX, close, 0)
    for k in (4, 5, 2, 3, 6, 7, 1):
        trade(k, False).start()
    yd[t] = y[t]
    wide = 1024
    for i, away in enumerate((0, 1, 3, 2)):
        for k in (2 * away, 2 * away + 1):
            if k > 0:
                trade(k, True).wait_recv()
        first = 2 * lax.rem(x + NX - away, NX)

        def add(j, carry):
            cols = pl.ds(pl.multiple_of(j * wide, wide), wide)
            total = facc[:, cols]
            for h in (0, 1):
                total = total + jnp.dot(yd[first + h], pdb[first + h, :, cols], preferred_element_type=F32)
            if i == NX - 1:
                out[:, cols] = total.astype(out.dtype)
            else:
                facc[:, cols] = total
            return carry

        lax.fori_loop(0, out.shape[1] // wide, add, 0)
    for k in range(1, 2 * NX):
        trade(k, False).wait_send()
    for d in (0, 1):
        edge(d, False).wait_send()
    for i in range(3):
        twin(i, False).wait_send()
    pass_on.wait_send()
    for k in range(1, NX):
        deal(k, False).wait_send()
    for r in (ring1, ring2, ring, swap1, swap2, side, late):
        r.drain()


def body(
    n, tokens, norm_gain, query_diff, key_diff, value_diff, lam, output_norm_gain,
    query_win, keyval_win, sink, proj_diff, proj_win,
):
    block, model = tokens.shape
    rows = block * 2 * NX
    depth, wq = query_win.shape
    kvd = key_diff.shape[1] + value_diff.shape[1]
    dq = query_diff.shape[1]
    part = keyval_win.shape[2] // 2
    hops = n // 2

    def pair(*shape):
        return [DMA(shape), DMA(shape)]

    return pl.pallas_call(
        functools.partial(layer_kernel, n, sink.shape[0]),
        out_shape=jax.ShapeDtypeStruct((block, model), BF16),
        in_specs=[
            pl.BlockSpec(memory_space=m)
            for m in [ANY, VMEM] + [ANY] * 7 + [pltpu.SMEM, pltpu.SMEM, VMEM]
        ],
        out_specs=pl.BlockSpec(memory_space=VMEM),
        scratch_shapes=[
            VMEM((n, depth, kvd + dq), BF16),
            VMEM((n, depth, wq + part), BF16),
            VMEM((2 * NX, block, model), BF16),
            VMEM((n, rows, depth), BF16),
            VMEM((rows, kvd + dq), F32),
            VMEM((rows, wq + part), F32),
            VMEM((n, rows, kvd), BF16),
            VMEM((2 * NX,) + proj_diff.shape, BF16),
            VMEM(proj_win.shape, BF16),
            VMEM((rows, dq), BF16),
            VMEM((rows, wq), BF16),
            VMEM((2, rows + 2 * WINDOW, part), BF16),
            VMEM((2, rows, HEAD), F32),
            VMEM((2, rows, HEAD), F32),
            VMEM((2, rows, VDIM), F32),
            VMEM((2 * NX, block, VDIM), BF16),
            VMEM((2 * NX, block, VDIM), BF16),
            VMEM((2, NX, block, wq), BF16),
            VMEM((NX, block, model), BF16),
            VMEM((NX, block, model), BF16),
            VMEM((NX - 1, block, model), BF16),
            VMEM((block, model), F32),
            DMA((8,)),
        ]
        + pair(2, hops, 4)
        + pair(n)
        + pair(2, hops, 2)
        + pair(n)
        + pair(2, hops, 4)
        + pair(2)
        + pair(3)
        + pair(2 * NX)
        + pair(NX)
        + side_sems()
        + side_sems(),
        compiler_params=pltpu.CompilerParams(
            collective_id=0, has_side_effects=True, vmem_limit_bytes=67_000_000
        ),
    )(
        tokens, norm_gain.reshape(1, model), key_diff, value_diff, query_diff, query_win, keyval_win,
        proj_diff, proj_win, lam, sink, output_norm_gain.reshape(1, VDIM),
    )


def solution(mesh):
    torus = Mesh(
        mesh.devices.reshape(mesh.shape["grp"], mesh.shape["sp"], NX, 2),
        ("grp", "sp", "tp_0", "tp_1"),
    )
    return jax.shard_map(
        functools.partial(body, mesh.shape["sp"]),
        mesh=torus,
        in_specs=(
            P(GRP_SP_TP, None),
            P(),
            P("sp", TP),
            P("sp", TP),
            P("sp", TP),
            P(TP),
            P(),
            P("sp", TP),
            P(None, "sp", None),
            P(TP),
            P(TP, None),
            P(TP, None),
        ),
        out_specs=P(GRP_SP_TP, None),
        check_vma=False,
    )
```

```python
import functools

import jax
import jax.numpy as jnp
from jax import lax
from jax.experimental import pallas as pl
from jax.experimental.pallas import tpu as pltpu
from jax.sharding import Mesh
from jax.sharding import PartitionSpec as P

HEAD = 128
WIN_HEADS = 16
KV_HEADS = 4
WINDOW = 128
VDIM = 256
NX = 4
CUT = 80
TP = ("tp_0", "tp_1")
GRP_SP_TP = ("grp", "sp", "tp_0", "tp_1")
EPS = 1e-06
LOG2E = 1.4426950408889634
BF16 = jnp.bfloat16
F32 = jnp.float32
MESH = pl.DeviceIdType.MESH
DMA = pltpu.SemaphoreType.DMA
VMEM = pltpu.VMEM
ANY = pl.ANY


def remote(src, dst, send_sem, recv_sem, where):
    return pltpu.make_async_remote_copy(
        src_ref=src,
        dst_ref=dst,
        send_sem=send_sem,
        recv_sem=recv_sem,
        device_id=where,
        device_id_type=MESH,
    )


def greet(peers):
    barrier = pltpu.get_barrier_semaphore()
    for peer in peers:
        pl.semaphore_signal(barrier, inc=1, device_id=peer, device_id_type=MESH)
    pl.semaphore_wait(barrier, len(peers))


class Ring:
    def __init__(self, n, buf, base, cuts, send, recv):
        self.n, self.buf, self.send, self.recv = n, buf, send, recv
        self.spans = []
        for cut in cuts:
            self.spans.append(pl.ds(base, cut))
            base = base + cut
        self.count = len(cuts)
        self.me = lax.axis_index("sp")
        self.to = (
            {"sp": lax.rem(self.me + 1, n)},
            {"sp": lax.rem(self.me + n - 1, n)},
        )

    def origin(self, d, s):
        return lax.rem(self.me + (self.n - s if d == 0 else s), self.n)

    def piece(self, d, s, k, hops):
        ref = self.buf.at[self.origin(d, hops), self.spans[k if d == 0 else self.count - 1 - k]]
        return remote(ref, ref, self.send.at[d, s, k], self.recv.at[d, s, k], self.to[d])

    def start(self, s, k):
        for d in (0, 1):
            self.piece(d, s, k, s).start()

    def land(self, s, k):
        for d in (0, 1):
            self.piece(d, s, k, s + 1).wait_recv()

    def drain(self):
        last = self.n // 2 - 1

        def one(s, carry):
            for k in range(self.count):
                for d in (0, 1):
                    self.piece(d, s, k, s).wait_send()
            return carry

        lax.fori_loop(0, last, one, 0)
        for k in range(self.count // 2):
            for d in (0, 1):
                self.piece(d, last, k, last).wait_send()


class Swap:
    def __init__(self, n, buf, cut, send, recv):
        self.n, self.buf, self.cut, self.send, self.recv = n, buf, cut, send, recv
        g = lax.axis_index("grp")
        self.odd = lax.rem(g, 2)
        self.to = {"grp": g + 1 - 2 * self.odd}
        self.kept = buf.shape[1] - cut
        self.base = pl.multiple_of(self.odd * cut, 16)

    def piece(self, o, odd):
        ref = self.buf.at[o, pl.ds(pl.multiple_of(odd * self.kept, 16), self.cut)]
        return remote(ref, ref, self.send.at[o], self.recv.at[o], self.to)

    def start(self, o):
        self.piece(o, self.odd).start()

    def land(self, o):
        self.piece(o, 1 - self.odd).wait_recv()

    def drain(self):
        def one(i, carry):
            self.piece(lax.rem(lax.axis_index("sp") + i, self.n), self.odd).wait_send()
            return carry

        lax.fori_loop(1, self.n, one, 0)


class Side:
    def __init__(self, own, slots, half, xs, xr, cs, cr):
        self.own, self.slots, self.half = own, slots, half
        self.xs, self.xr, self.cs, self.cr = xs, xr, cs, cr
        self.x = lax.axis_index("tp_0")
        self.c = lax.axis_index("tp_1")
        self.to = (
            {"tp_0": lax.rem(self.x + 1, NX)},
            {"tp_0": lax.rem(self.x + NX - 1, NX)},
        )
        self.other = {"tp_1": 1 - self.c}

    def spot(self, rel, h, core):
        slot = 2 * lax.rem(self.x + rel, NX) + core
        return self.slots.at[slot, pl.ds(h * self.half, self.half)]

    def source(self, rel, h):
        if rel == 0 and self.own is not None:
            return self.own.at[pl.ds(h * self.half, self.half)]
        return self.spot(rel, h, self.c)

    def half_of(self, d, k):
        return (0, 1, 0)[k] if d == 0 else (1, 0, 1)[k]

    def out(self, d, k):
        rel = 0 if k < 2 else (3 if d == 0 else 1)
        h = self.half_of(d, k)
        return remote(
            self.source(rel, h), self.spot(rel, h, self.c), self.xs.at[d, k], self.xr.at[d, k], self.to[d]
        )

    def inward(self, d, k):
        rel = (3 if d == 0 else 1) if k < 2 else 2
        h = self.half_of(d, k)
        ref = self.spot(rel, h, self.c)
        return rel, h, remote(ref, ref, self.xs.at[d, k], self.xr.at[d, k], self.to[d])

    def across(self, rel, h):
        return remote(
            self.source(rel, h), self.spot(rel, h, self.c), self.cs.at[rel, h], self.cr.at[rel, h], self.other
        )

    def start(self):
        for k in (0, 1):
            for d in (0, 1):
                self.out(d, k).start()
        for h in (0, 1):
            self.across(0, h).start()

    def step(self, k):
        for d in (0, 1):
            rel, h, copy = self.inward(d, k)
            copy.wait_recv()
            if k == 0:
                self.out(d, 2).start()
            self.across(rel, h).start()

    def finish(self):
        for rel in range(NX):
            for h in (0, 1):
                ref = self.spot(rel, h, 1 - self.c)
                remote(ref, ref, self.cs.at[rel, h], self.cr.at[rel, h], self.other).wait_recv()

    def drain(self):
        for k in (0, 1, 2):
            for d in (0, 1):
                self.out(d, k).wait_send()
        for rel in range(NX):
            for h in (0, 1):
                self.across(rel, h).wait_send()


def side_sems():
    return [DMA((2, 3)), DMA((2, 3)), DMA((NX, 2)), DMA((NX, 2))]


def layer_kernel(
    n, heads_win, tok, gain, kd, vd, qd, qwd, kvw, pd, pw, lam, sink, ogain, out,
    w1, w2, raw, nbuf, acc1, acc2, kbuf, pdb, pwb, q, qw, kw, top, tot, acc, y, yd, yv, give, take, sums, facc,
    lsem, z1s, z1r, y1s, y1r, z2s, z2r, y2s, y2r, zks, zkr, hs, hr, us, ur, ts, tr, ws, wr, *sems,
):
    me, x, c = (lax.axis_index(a) for a in ("sp", "tp_0", "tp_1"))
    t = 2 * x + c
    block = raw.shape[1]
    rows = 2 * NX * block
    depth = w1.shape[1]
    part = kvw.shape[2] // 2
    head = t * heads_win // (WIN_HEADS // KV_HEADS)
    wq = qwd.shape[1]
    local = []
    at = 0
    for w in (kd, vd, qd):
        local.append((w, w1.at[me, :, pl.ds(at, w.shape[1])]))
        at += w.shape[1]
    local += [
        (qwd, w2.at[me, :, pl.ds(0, wq)]),
        (kvw.at[head, :, pl.ds(pl.multiple_of(c * part, part), part)], w2.at[me, :, pl.ds(wq, part)]),
        (tok, raw.at[t]),
        (pd, pdb.at[t]),
        (pw, pwb),
    ]
    local = [pltpu.make_async_copy(a, b, lsem.at[i]) for i, (a, b) in enumerate(local)]
    for copy in local:
        copy.start()

    swap1 = Swap(n, w1, CUT, y1s, y1r)
    swap2 = Swap(n, w2, depth // 2, y2s, y2r)
    ring1 = Ring(n, w1, swap1.base, (48, 48, 48, swap1.kept - 144), z1s, z1r)
    ring2 = Ring(n, w2, swap2.base, (depth // 4,) * 2, z2s, z2r)
    ring = Ring(n, kbuf, 0, (rows // 4,) * 4, zks, zkr)
    side = Side(None, raw, block // 2, *sems[:4])
    late = Side(None, pdb, depth // 2, *sems[4:])

    def peer(k):
        return {"tp_0": lax.rem(x + k // 2, NX), "tp_1": lax.rem(c + k % 2, 2)}

    greet([ring.to[0], ring.to[1], swap1.to] + [peer(k) for k in range(1, 2 * NX)])

    for copy in local[:3]:
        copy.wait()
    for k in range(4):
        ring1.start(0, k)
    local[5].wait()
    side.start()
    acc1[...] = jnp.zeros_like(acc1)
    acc2[...] = jnp.zeros_like(acc2)
    top[...] = jnp.full_like(top, -jnp.inf)
    tot[...] = jnp.zeros_like(tot)
    acc[...] = jnp.zeros_like(acc)
    for copy in local[3:5] + local[6:]:
        copy.wait()

    def normalise(quarter):
        tile = 32
        per = raw.shape[0] * block // tile // 4

        def one(j, carry):
            i = quarter * per + j
            slot, r = i // (block // tile), lax.rem(i, block // tile)
            v = raw[slot, pl.ds(pl.multiple_of(r * tile, tile), tile), :].astype(F32)
            v = v * lax.rsqrt(jnp.mean(v * v, axis=-1, keepdims=True) + EPS) * gain[...]
            v = v.astype(BF16)
            for o in range(n):
                nbuf[o, pl.ds(pl.multiple_of(i * tile, tile), tile), :] = v[:, o * depth : (o + 1) * depth]
            return carry

        lax.fori_loop(0, per, one, 0)

    def gather(w, swap, total, lo, hi):
        def one(j, carry):
            o = lax.rem(me + jnp.where(lax.rem(j, 2) == 1, (j + 1) // 2, n - j // 2), n)

            @pl.when(j > 0)
            def _():
                swap.land(o)

            total[...] += jnp.dot(nbuf[o], w[o], preferred_element_type=F32)
            return carry

        lax.fori_loop(lo, hi, one, 0)

    last = n // 2 - 1

    def swap_both(swap, ring_, hops):
        for d in (0, 1):
            swap.start(ring_.origin(d, hops))

    def hop2(s, k):
        ring2.land(s, k)
        ring2.start(s + 1, k)

    def late_swaps(lo, hi):
        def one(h, carry):
            swap_both(swap2, ring2, h)
            return carry

        lax.fori_loop(lo, hi, one, 0)

    def phase1(s, carry):
        for k in range(4):
            ring1.land(s, k)
            ring1.start(s + 1, k)
            if k == 0:
                for i in range(3):

                    @pl.when(s == i + 1)
                    def _():
                        side.step(i)
                        if i == 2:
                            late.start()

                @pl.when(s == last - 3)
                def _():
                    side.finish()

            @pl.when(s == last - 3)
            def _():
                normalise(k)

            @pl.when(s == last - 2)
            def _():
                gather(w1, swap1, acc1, 3 * k, min(3 * k + 3, 2 * last - 3))

            if k % 2 == 1:

                @pl.when(s >= 2)
                def _():
                    hop2(s - 2, k // 2)

        swap_both(swap1, ring1, s + 1)

        @pl.when(s == 1)
        def _():
            for k in (0, 1):
                ring2.start(0, k)

        return carry

    lax.fori_loop(0, last - 1, phase1, 0)
    done = 2 * last - 3
    for k in range(4):
        ring1.land(last - 1, k)
        if k < 2:
            ring1.start(last, k)
        if k % 2 == 1:
            hop2(last - 3, k // 2)
        if k == 2:
            gather(w1, swap1, acc1, done, done + 1)
    swap_both(swap1, ring1, last)
    gather(w1, swap1, acc1, done + 1, done + 2)
    for k in (0, 1):
        ring1.land(last, k)
    swap1.start(ring1.origin(0, last + 1))
    for k in (0, 1):
        hop2(last - 2, k)
    late_swaps(1, last)
    gather(w1, swap1, acc1, done + 2, done + 4)
    ring2.land(last - 1, 0)
    ring2.start(last, 0)
    ring2.land(last - 1, 1)
    swap_both(swap2, ring2, last)
    gather(w1, swap1, acc1, n - 1, n)
    kvd = kbuf.shape[2]
    kbuf[me] = acc1[:, :kvd].astype(BF16)
    q[...] = acc1[:, kvd:].astype(BF16)
    for k in range(4):
        ring.start(0, k)

    def edge(d, inward):
        src = pl.ds(rows, WINDOW) if d == 0 else pl.ds(WINDOW, WINDOW)
        dst = pl.ds(0, WINDOW) if d == 0 else pl.ds(rows + WINDOW, WINDOW)
        target = kw.at[c, dst]
        return remote(target if inward else kw.at[c, src], target, hs.at[d], hr.at[d], ring.to[d])

    spans = (pl.ds(WINDOW, rows), pl.ds(0, WINDOW), pl.ds(rows + WINDOW, WINDOW))

    def twin(i, inward):
        ref = kw.at[1 - c if inward else c, spans[i]]
        return remote(ref, ref, us.at[i], ur.at[i], side.other)

    def trade(k, inward):
        if inward:
            ref = yd.at[2 * lax.rem(x + NX - k // 2, NX) + lax.rem(c + k % 2, 2)]
            return remote(ref, ref, ts.at[k], tr.at[k], peer(k))
        src = y.at[2 * lax.rem(x + k // 2, NX) + lax.rem(c + k % 2, 2)]
        return remote(src, yd.at[t], ts.at[k], tr.at[k], peer(k))

    pass_on = remote(give, take, ws.at[0], wr.at[0], side.other)

    def deal(k, inward):
        to = lax.rem(x + k, NX)
        return remote(sums.at[k - 1] if inward else take.at[to], sums.at[k - 1], ws.at[k], wr.at[k], {"tp_0": to})

    scale = HEAD**-0.5
    lanes = HEAD
    contract_last = (((1,), (1,)), ((), ()))

    def attend(o):
        def one(m, carry):
            cols = pl.ds(pl.multiple_of(m * HEAD, HEAD), HEAD)
            s = lax.dot_general(q[:, cols], kbuf[o, :, cols], contract_last, preferred_element_type=F32)
            s = s * (scale * LOG2E)
            reps = s.shape[1] // lanes
            was = top[m]
            now = jnp.maximum(was, jnp.max(s, axis=1, keepdims=True))
            fade = jnp.exp2(was - now)
            e = jnp.exp2(s - jnp.concatenate([now] * reps, axis=1))
            some = e[:, :lanes]
            for j in range(1, reps):
                some = some + e[:, j * lanes : (j + 1) * lanes]
            tot[m] = tot[m] * fade + some
            top[m] = now
            acc[m] = acc[m] * jnp.concatenate([fade] * (VDIM // lanes), axis=1) + jnp.dot(
                e.astype(BF16), kbuf[o, :, 2 * HEAD :], preferred_element_type=F32
            )
            return carry

        for m in range(2):
            one(m, 0)

    def window(lo, hi):
        span = 3 * WINDOW
        heads = wq // HEAD
        i_q = lax.broadcasted_iota(jnp.int32, (WINDOW, span), 0)
        i_k = lax.broadcasted_iota(jnp.int32, (WINDOW, span), 1)
        near = jnp.abs(i_k - WINDOW - i_q) <= WINDOW

        def one(b, carry):
            r = pl.ds(pl.multiple_of(b * WINDOW, WINDOW), WINDOW)
            band = pl.ds(pl.multiple_of(b * WINDOW, WINDOW), span)
            where = i_k + (me * rows + b * WINDOW - WINDOW)
            valid = near & (where >= 0) & (where < n * rows)
            for h in range(heads):
                cols = pl.ds(h * HEAD, HEAD)
                s = lax.dot_general(qw[r, cols], kw[0, band, :], contract_last, preferred_element_type=F32)
                s = jnp.where(valid, s * scale, -jnp.inf)
                sunk = jnp.full((WINDOW, lanes), sink[h], F32)
                peak = jnp.maximum(jnp.max(s, axis=1, keepdims=True), sunk)
                e = jnp.exp(s - jnp.concatenate([peak] * 3, axis=1))
                whole = jnp.sum(e, axis=1, keepdims=True) + jnp.exp(sunk - peak)
                w = (e / jnp.concatenate([whole] * 3, axis=1)).astype(BF16)
                res = jnp.dot(w, kw[1, band, :], preferred_element_type=F32).astype(BF16)
                for j in range(WINDOW // block):
                    yv[j % 2, b * (WINDOW // block // 2) + j // 2, :, cols] = res[j * block : (j + 1) * block]
            return carry

        lax.fori_loop(lo, hi, one, 0)

    width = 512

    def columns(one):
        def run(j, carry):
            one(pl.ds(pl.multiple_of(j * width, width), width))
            return carry

        lax.fori_loop(0, out.shape[1] // width, run, 0)

    def window_rows(core, cols):
        ys = yv[core].reshape(NX * block, wq)
        return jnp.dot(ys, pwb[:, cols], preferred_element_type=F32).reshape(NX, block, width)

    def to_give(cols):
        give[:, :, cols] = window_rows(1 - c, cols).astype(BF16)

    def to_sum(cols):
        take[:, :, cols] = (window_rows(c, cols) + take[:, :, cols].astype(F32)).astype(BF16)

    attend(me)

    def phase2(s, carry):
        for k in range(4):
            ring.land(s, k)
            ring.start(s + 1, k)
            if k == 0:

                @pl.when(s == 0)
                def _():
                    ring2.land(last, 0)
                    swap2.start(ring2.origin(0, last + 1))
                    late.step(0)

                @pl.when(s == 1)
                def _():
                    late.step(1)

                @pl.when(s == 3)
                def _():
                    gather(w2, swap2, acc2, n // 2, n)
                    kw[c, spans[0]] = acc2[:, wq:].astype(BF16)
                    qw[...] = acc2[:, :wq].astype(BF16)
                    for d in (0, 1):
                        edge(d, False).start()
                    twin(0, False).start()

                @pl.when(s == 4)
                def _():
                    for i in range(3):
                        twin(i, True).wait_recv()
                    window(0, rows // WINDOW // 2)

                @pl.when(s == 5)
                def _():
                    columns(to_give)
                    pass_on.start()

            if k == 2:

                @pl.when(s == 2)
                def _():
                    gather(w2, swap2, acc2, 0, n // 2)

                @pl.when(s == 3)
                def _():
                    for d in (0, 1):
                        edge(d, True).wait_recv()
                        twin(d + 1, False).start()
                    late.step(2)

                @pl.when(s == 4)
                def _():
                    window(rows // WINDOW // 2, rows // WINDOW)

                @pl.when(s == 5)
                def _():
                    pass_on.wait_recv()
                    columns(to_sum)
                    for i in (2, 1, 3):
                        deal(i, False).start()

            if k % 2 == 1:

                @pl.when(s > 0)
                def _():
                    attend(ring.origin(k // 2, s))

        return carry

    lax.fori_loop(0, last - 1, phase2, 0)
    for k in range(4):
        ring.land(last - 1, k)
        if k < 2:
            ring.start(last, k)
        if k % 2 == 1:
            attend(ring.origin(k // 2, last - 1))
    late.finish()
    for r in (ring1, ring2, swap1, swap2, side, late):
        r.drain()
    for d in (0, 1):
        edge(d, False).wait_send()
    for i in range(3):
        twin(i, False).wait_send()
    pass_on.wait_send()

    def both(i, carry):
        attend(lax.rem(me + n - last + 2 * last * i, n))
        return carry

    lax.fori_loop(0, 2, both, 0)
    for k in (0, 1):
        ring.land(last, k)
    attend(lax.rem(me + last + 1, n))

    def close(j):
        r = pl.ds(pl.multiple_of(j * block, block), block)
        parts = [1.0 / jnp.sum(tot[m, r, :], axis=1, keepdims=True) for m in range(2)]
        d = acc[0, r, :] * parts[0] - acc[1, r, :] * (lam[0] * parts[1])
        d = d * lax.rsqrt(jnp.mean(d * d, axis=-1, keepdims=True) + EPS) * ogain[...]
        return d.astype(BF16)

    for k in (4, 5, 2, 6, 3, 7, 1):
        j = 2 * lax.rem(x + k // 2, NX) + lax.rem(c + k % 2, 2)
        y[j] = close(j)
        trade(k, False).start()
    yd[t] = close(t)
    wide = 1024

    def add(total, away, cols):
        first = 2 * lax.rem(x + NX - away, NX)
        for h in (0, 1):
            total = total + jnp.dot(yd[first + h], pdb[first + h, :, cols], preferred_element_type=F32)
        return total

    def begin(j, carry):
        cols = pl.ds(pl.multiple_of(j * wide, wide), wide)
        total = take[x, :, cols].astype(F32)
        for k in range(1, NX):
            total = total + sums[k - 1, :, cols].astype(F32)
        facc[:, cols] = add(total, 0, cols)
        return carry

    def finish(j, carry):
        cols = pl.ds(pl.multiple_of(j * wide, wide), wide)
        total = facc[:, cols]
        for away in (1, 3, 2):
            total = add(total, away, cols)
        out[:, cols] = total.astype(out.dtype)
        return carry

    for k in range(1, NX):
        deal(k, True).wait_recv()
    trade(1, True).wait_recv()
    lax.fori_loop(0, out.shape[1] // wide, begin, 0)
    for k in range(2, 2 * NX):
        trade(k, True).wait_recv()
    lax.fori_loop(0, out.shape[1] // wide, finish, 0)
    for k in range(1, 2 * NX):
        trade(k, False).wait_send()
    for k in range(1, NX):
        deal(k, False).wait_send()
    ring.drain()


def body(
    n, tokens, norm_gain, query_diff, key_diff, value_diff, lam, output_norm_gain,
    query_win, keyval_win, sink, proj_diff, proj_win,
):
    block, model = tokens.shape
    rows = block * 2 * NX
    depth, wq = query_win.shape
    kvd = key_diff.shape[1] + value_diff.shape[1]
    dq = query_diff.shape[1]
    part = keyval_win.shape[2] // 2
    hops = n // 2

    def pair(*shape):
        return [DMA(shape), DMA(shape)]

    return pl.pallas_call(
        functools.partial(layer_kernel, n, sink.shape[0]),
        out_shape=jax.ShapeDtypeStruct((block, model), BF16),
        in_specs=[
            pl.BlockSpec(memory_space=m)
            for m in [ANY, VMEM] + [ANY] * 7 + [pltpu.SMEM, pltpu.SMEM, VMEM]
        ],
        out_specs=pl.BlockSpec(memory_space=VMEM),
        scratch_shapes=[
            VMEM((n, depth, kvd + dq), BF16),
            VMEM((n, depth, wq + part), BF16),
            VMEM((2 * NX, block, model), BF16),
            VMEM((n, rows, depth), BF16),
            VMEM((rows, kvd + dq), F32),
            VMEM((rows, wq + part), F32),
            VMEM((n, rows, kvd), BF16),
            VMEM((2 * NX,) + proj_diff.shape, BF16),
            VMEM(proj_win.shape, BF16),
            VMEM((rows, dq), BF16),
            VMEM((rows, wq), BF16),
            VMEM((2, rows + 2 * WINDOW, part), BF16),
            VMEM((2, rows, HEAD), F32),
            VMEM((2, rows, HEAD), F32),
            VMEM((2, rows, VDIM), F32),
            VMEM((2 * NX, block, VDIM), BF16),
            VMEM((2 * NX, block, VDIM), BF16),
            VMEM((2, NX, block, wq), BF16),
            VMEM((NX, block, model), BF16),
            VMEM((NX, block, model), BF16),
            VMEM((NX - 1, block, model), BF16),
            VMEM((block, model), F32),
            DMA((8,)),
        ]
        + pair(2, hops, 4)
        + pair(n)
        + pair(2, hops, 2)
        + pair(n)
        + pair(2, hops, 4)
        + pair(2)
        + pair(3)
        + pair(2 * NX)
        + pair(NX)
        + side_sems()
        + side_sems(),
        compiler_params=pltpu.CompilerParams(
            collective_id=0, has_side_effects=True, vmem_limit_bytes=67_000_000
        ),
    )(
        tokens, norm_gain.reshape(1, model), key_diff, value_diff, query_diff, query_win, keyval_win,
        proj_diff, proj_win, lam, sink, output_norm_gain.reshape(1, VDIM),
    )


def solution(mesh):
    torus = Mesh(
        mesh.devices.reshape(mesh.shape["grp"], mesh.shape["sp"], NX, 2),
        ("grp", "sp", "tp_0", "tp_1"),
    )
    return jax.shard_map(
        functools.partial(body, mesh.shape["sp"]),
        mesh=torus,
        in_specs=(
            P(GRP_SP_TP, None),
            P(),
            P("sp", TP),
            P("sp", TP),
            P("sp", TP),
            P(TP),
            P(),
            P("sp", TP),
            P(None, "sp", None),
            P(TP),
            P(TP, None),
            P(TP, None),
        ),
        out_specs=P(GRP_SP_TP, None),
        check_vma=False,
    )
```

```python
import functools

import jax
import jax.numpy as jnp
from jax import lax
from jax.experimental import pallas as pl
from jax.experimental.pallas import tpu as pltpu
from jax.sharding import Mesh
from jax.sharding import PartitionSpec as P

HEAD = 128
WIN_HEADS = 16
KV_HEADS = 4
WINDOW = 128
VDIM = 256
NX = 4
CUT = 96
TP = ("tp_0", "tp_1")
GRP_SP_TP = ("grp", "sp", "tp_0", "tp_1")
EPS = 1e-06
LOG2E = 1.4426950408889634
BF16 = jnp.bfloat16
F32 = jnp.float32
MESH = pl.DeviceIdType.MESH
DMA = pltpu.SemaphoreType.DMA
VMEM = pltpu.VMEM
ANY = pl.ANY


def remote(src, dst, send_sem, recv_sem, where):
    return pltpu.make_async_remote_copy(
        src_ref=src,
        dst_ref=dst,
        send_sem=send_sem,
        recv_sem=recv_sem,
        device_id=where,
        device_id_type=MESH,
    )


def greet(peers):
    barrier = pltpu.get_barrier_semaphore()
    for peer in peers:
        pl.semaphore_signal(barrier, inc=1, device_id=peer, device_id_type=MESH)
    pl.semaphore_wait(barrier, len(peers))


class Ring:
    def __init__(self, n, buf, base, cuts, send, recv):
        self.n, self.buf, self.send, self.recv = n, buf, send, recv
        self.spans = []
        for cut in cuts:
            self.spans.append(pl.ds(base, cut))
            base = base + cut
        self.count = len(cuts)
        self.me = lax.axis_index("sp")
        self.to = (
            {"sp": lax.rem(self.me + 1, n)},
            {"sp": lax.rem(self.me + n - 1, n)},
        )

    def origin(self, d, s):
        return lax.rem(self.me + (self.n - s if d == 0 else s), self.n)

    def piece(self, d, s, k, hops):
        ref = self.buf.at[self.origin(d, hops), self.spans[k if d == 0 else self.count - 1 - k]]
        return remote(ref, ref, self.send.at[d, s, k], self.recv.at[d, s, k], self.to[d])

    def start(self, s, k):
        for d in (0, 1):
            self.piece(d, s, k, s).start()

    def land(self, s, k):
        for d in (0, 1):
            self.piece(d, s, k, s + 1).wait_recv()

    def drain(self):
        last = self.n // 2 - 1

        def one(s, carry):
            for k in range(self.count):
                for d in (0, 1):
                    self.piece(d, s, k, s).wait_send()
            return carry

        lax.fori_loop(0, last, one, 0)
        for k in range(self.count // 2):
            for d in (0, 1):
                self.piece(d, last, k, last).wait_send()


class Swap:
    def __init__(self, n, buf, cut, send, recv):
        self.n, self.buf, self.cut, self.send, self.recv = n, buf, cut, send, recv
        g = lax.axis_index("grp")
        self.odd = lax.rem(g, 2)
        self.to = {"grp": g + 1 - 2 * self.odd}
        self.kept = buf.shape[1] - cut
        self.base = pl.multiple_of(self.odd * cut, 16)

    def piece(self, o, odd):
        ref = self.buf.at[o, pl.ds(pl.multiple_of(odd * self.kept, 16), self.cut)]
        return remote(ref, ref, self.send.at[o], self.recv.at[o], self.to)

    def start(self, o):
        self.piece(o, self.odd).start()

    def land(self, o):
        self.piece(o, 1 - self.odd).wait_recv()

    def drain(self):
        def one(i, carry):
            self.piece(lax.rem(lax.axis_index("sp") + i, self.n), self.odd).wait_send()
            return carry

        lax.fori_loop(1, self.n, one, 0)


class Side:
    def __init__(self, own, slots, half, xs, xr, cs, cr):
        self.own, self.slots, self.half = own, slots, half
        self.xs, self.xr, self.cs, self.cr = xs, xr, cs, cr
        self.x = lax.axis_index("tp_0")
        self.c = lax.axis_index("tp_1")
        self.to = (
            {"tp_0": lax.rem(self.x + 1, NX)},
            {"tp_0": lax.rem(self.x + NX - 1, NX)},
        )
        self.other = {"tp_1": 1 - self.c}

    def spot(self, rel, h, core):
        slot = 2 * lax.rem(self.x + rel, NX) + core
        return self.slots.at[slot, pl.ds(h * self.half, self.half)]

    def source(self, rel, h):
        if rel == 0 and self.own is not None:
            return self.own.at[pl.ds(h * self.half, self.half)]
        return self.spot(rel, h, self.c)

    def half_of(self, d, k):
        return (0, 1, 0)[k] if d == 0 else (1, 0, 1)[k]

    def out(self, d, k):
        rel = 0 if k < 2 else (3 if d == 0 else 1)
        h = self.half_of(d, k)
        return remote(
            self.source(rel, h), self.spot(rel, h, self.c), self.xs.at[d, k], self.xr.at[d, k], self.to[d]
        )

    def inward(self, d, k):
        rel = (3 if d == 0 else 1) if k < 2 else 2
        h = self.half_of(d, k)
        ref = self.spot(rel, h, self.c)
        return rel, h, remote(ref, ref, self.xs.at[d, k], self.xr.at[d, k], self.to[d])

    def across(self, rel, h):
        return remote(
            self.source(rel, h), self.spot(rel, h, self.c), self.cs.at[rel, h], self.cr.at[rel, h], self.other
        )

    def start(self):
        for k in (0, 1):
            for d in (0, 1):
                self.out(d, k).start()
        for h in (0, 1):
            self.across(0, h).start()

    def step(self, k):
        for d in (0, 1):
            rel, h, copy = self.inward(d, k)
            copy.wait_recv()
            if k == 0:
                self.out(d, 2).start()
            self.across(rel, h).start()

    def finish(self):
        for rel in range(NX):
            for h in (0, 1):
                ref = self.spot(rel, h, 1 - self.c)
                remote(ref, ref, self.cs.at[rel, h], self.cr.at[rel, h], self.other).wait_recv()

    def drain(self):
        for k in (0, 1, 2):
            for d in (0, 1):
                self.out(d, k).wait_send()
        for rel in range(NX):
            for h in (0, 1):
                self.across(rel, h).wait_send()


def side_sems():
    return [DMA((2, 3)), DMA((2, 3)), DMA((NX, 2)), DMA((NX, 2))]


def layer_kernel(
    n, heads_win, tok, gain, kd, vd, qd, qwd, kvw, pd, pw, lam, sink, ogain, out,
    w1, w2, raw, nbuf, acc1, acc2, kbuf, pdb, pwb, q, qw, kw, top, tot, acc, y, yd, yv, give, take, far, sums, facc,
    lsem, z1s, z1r, y1s, y1r, z2s, z2r, y2s, y2r, zks, zkr, hs, hr, us, ur, ts, tr, ws, wr, *sems,
):
    me, x, c = (lax.axis_index(a) for a in ("sp", "tp_0", "tp_1"))
    t = 2 * x + c
    block = raw.shape[1]
    rows = 2 * NX * block
    depth = w1.shape[1]
    part = kvw.shape[2] // 2
    head = t * heads_win // (WIN_HEADS // KV_HEADS)
    wq = qwd.shape[1]
    local = []
    at = 0
    for w in (kd, vd, qd):
        local.append((w, w1.at[me, :, pl.ds(at, w.shape[1])]))
        at += w.shape[1]
    local += [
        (qwd, w2.at[me, :, pl.ds(0, wq)]),
        (kvw.at[head, :, pl.ds(pl.multiple_of(c * part, part), part)], w2.at[me, :, pl.ds(wq, part)]),
        (tok, raw.at[t]),
        (pd, pdb.at[t]),
        (pw, pwb),
    ]
    local = [pltpu.make_async_copy(a, b, lsem.at[i]) for i, (a, b) in enumerate(local)]
    for copy in local:
        copy.start()

    swap1 = Swap(n, w1, CUT, y1s, y1r)
    swap2 = Swap(n, w2, depth // 2, y2s, y2r)
    ring1 = Ring(n, w1, swap1.base, (48, 32, 32, swap1.kept - 112), z1s, z1r)
    ring2 = Ring(n, w2, swap2.base, (depth // 4,) * 2, z2s, z2r)
    ring = Ring(n, kbuf, 0, (rows // 4,) * 4, zks, zkr)
    side = Side(None, raw, block // 2, *sems[:4])
    late = Side(None, pdb, depth // 2, *sems[4:])

    def peer(k):
        return {"tp_0": lax.rem(x + k // 2, NX), "tp_1": lax.rem(c + k % 2, 2)}

    greet([ring.to[0], ring.to[1], swap1.to] + [peer(k) for k in range(1, 2 * NX)])

    for copy in local[:3]:
        copy.wait()
    for k in range(4):
        ring1.start(0, k)
    local[5].wait()
    side.start()
    acc1[...] = jnp.zeros_like(acc1)
    acc2[...] = jnp.zeros_like(acc2)
    top[...] = jnp.full_like(top, -jnp.inf)
    tot[...] = jnp.zeros_like(tot)
    acc[...] = jnp.zeros_like(acc)
    for copy in local[3:5] + local[6:]:
        copy.wait()

    def normalise(quarter):
        tile = 32
        per = raw.shape[0] * block // tile // 4

        def one(j, carry):
            i = quarter * per + j
            slot, r = i // (block // tile), lax.rem(i, block // tile)
            v = raw[slot, pl.ds(pl.multiple_of(r * tile, tile), tile), :].astype(F32)
            v = v * lax.rsqrt(jnp.mean(v * v, axis=-1, keepdims=True) + EPS) * gain[...]
            v = v.astype(BF16)
            for o in range(n):
                nbuf[o, pl.ds(pl.multiple_of(i * tile, tile), tile), :] = v[:, o * depth : (o + 1) * depth]
            return carry

        lax.fori_loop(0, per, one, 0)

    def gather(w, swap, total, lo, hi):
        def one(j, carry):
            o = lax.rem(me + jnp.where(lax.rem(j, 2) == 1, (j + 1) // 2, n - j // 2), n)

            @pl.when(j > 0)
            def _():
                swap.land(o)

            total[...] += jnp.dot(nbuf[o], w[o], preferred_element_type=F32)
            return carry

        lax.fori_loop(lo, hi, one, 0)

    last = n // 2 - 1

    def swap_both(swap, ring_, hops):
        for d in (0, 1):
            swap.start(ring_.origin(d, hops))

    def hop2(s, k):
        ring2.land(s, k)
        ring2.start(s + 1, k)

    def late_swaps(lo, hi):
        def one(h, carry):
            swap_both(swap2, ring2, h)
            return carry

        lax.fori_loop(lo, hi, one, 0)

    def phase1(s, carry):
        for k in range(4):
            ring1.land(s, k)
            ring1.start(s + 1, k)
            if k == 0:
                for i in range(3):

                    @pl.when(s == i + 1)
                    def _():
                        side.step(i)
                        if i == 2:
                            late.start()

                @pl.when(s == last - 3)
                def _():
                    side.finish()

            @pl.when(s == last - 3)
            def _():
                normalise(k)

            @pl.when(s == last - 2)
            def _():
                gather(w1, swap1, acc1, 3 * k, min(3 * k + 3, 2 * last - 3))

            if k % 2 == 1:

                @pl.when(s >= 2)
                def _():
                    hop2(s - 2, k // 2)

        swap_both(swap1, ring1, s + 1)

        @pl.when(s == 0)
        def _():
            for k in (0, 1):
                ring2.start(0, k)

        return carry

    lax.fori_loop(0, last - 1, phase1, 0)
    done = 2 * last - 3
    for k in range(4):
        ring1.land(last - 1, k)
        if k < 2:
            ring1.start(last, k)
        if k % 2 == 1:
            hop2(last - 3, k // 2)
        if k == 2:
            gather(w1, swap1, acc1, done, done + 1)
    swap_both(swap1, ring1, last)
    gather(w1, swap1, acc1, done + 1, done + 2)
    for k in (0, 1):
        ring1.land(last, k)
    swap1.start(ring1.origin(0, last + 1))
    for k in (0, 1):
        hop2(last - 2, k)
    late_swaps(1, last)
    gather(w1, swap1, acc1, done + 2, done + 4)
    ring2.land(last - 1, 0)
    ring2.start(last, 0)
    ring2.land(last - 1, 1)
    swap_both(swap2, ring2, last)
    gather(w1, swap1, acc1, n - 1, n)
    kvd = kbuf.shape[2]
    kbuf[me] = acc1[:, :kvd].astype(BF16)
    q[...] = acc1[:, kvd:].astype(BF16)
    for k in range(4):
        ring.start(0, k)

    def edge(d, inward):
        src = pl.ds(rows, WINDOW) if d == 0 else pl.ds(WINDOW, WINDOW)
        dst = pl.ds(0, WINDOW) if d == 0 else pl.ds(rows + WINDOW, WINDOW)
        target = kw.at[c, dst]
        return remote(target if inward else kw.at[c, src], target, hs.at[d], hr.at[d], ring.to[d])

    spans = (pl.ds(WINDOW, rows), pl.ds(0, WINDOW), pl.ds(rows + WINDOW, WINDOW))

    def twin(i, inward):
        ref = kw.at[1 - c if inward else c, spans[i]]
        return remote(ref, ref, us.at[i], ur.at[i], side.other)

    def trade(k, inward):
        if inward:
            ref = yd.at[2 * lax.rem(x + NX - k // 2, NX) + lax.rem(c + k % 2, 2)]
            return remote(ref, ref, ts.at[k], tr.at[k], peer(k))
        src = y.at[2 * lax.rem(x + k // 2, NX) + lax.rem(c + k % 2, 2)]
        return remote(src, yd.at[t], ts.at[k], tr.at[k], peer(k))

    pass_on = remote(give, take, ws.at[0], wr.at[0], side.other)

    def relay(d, inward):
        src = far.at[d] if inward else take.at[lax.rem(x + 2, NX), pl.ds(d * (block // 2), block // 2)]
        return remote(src, far.at[d], ws.at[1 + d], wr.at[1 + d], side.to[d])

    def deal(d, inward):
        src = sums.at[d] if inward else take.at[lax.rem(x + (1, NX - 1)[d], NX)]
        return remote(src, sums.at[d], ws.at[3 + d], wr.at[3 + d], side.to[d])

    def merge():
        for d in (0, 1):
            relay(d, True).wait_recv()
            to = lax.rem(x + (1, NX - 1)[d], NX)
            half = pl.ds(d * (block // 2), block // 2)
            take[to, half, :] = (take[to, half, :].astype(F32) + far[d].astype(F32)).astype(BF16)
        for d in (0, 1):
            deal(d, False).start()

    scale = HEAD**-0.5
    lanes = HEAD
    contract_last = (((1,), (1,)), ((), ()))

    def attend(o):
        def one(m, carry):
            cols = pl.ds(pl.multiple_of(m * HEAD, HEAD), HEAD)
            s = lax.dot_general(q[:, cols], kbuf[o, :, cols], contract_last, preferred_element_type=F32)
            s = s * (scale * LOG2E)
            reps = s.shape[1] // lanes
            was = top[m]
            now = jnp.maximum(was, jnp.max(s, axis=1, keepdims=True))
            fade = jnp.exp2(was - now)
            e = jnp.exp2(s - jnp.concatenate([now] * reps, axis=1))
            some = e[:, :lanes]
            for j in range(1, reps):
                some = some + e[:, j * lanes : (j + 1) * lanes]
            tot[m] = tot[m] * fade + some
            top[m] = now
            acc[m] = acc[m] * jnp.concatenate([fade] * (VDIM // lanes), axis=1) + jnp.dot(
                e.astype(BF16), kbuf[o, :, 2 * HEAD :], preferred_element_type=F32
            )
            return carry

        for m in range(2):
            one(m, 0)

    def window(lo, hi, stride):
        span = 3 * WINDOW
        heads = wq // HEAD
        i_q = lax.broadcasted_iota(jnp.int32, (WINDOW, span), 0)
        i_k = lax.broadcasted_iota(jnp.int32, (WINDOW, span), 1)
        near = jnp.abs(i_k - WINDOW - i_q) <= WINDOW

        def one(i, carry):
            b = i * stride
            r = pl.ds(pl.multiple_of(b * WINDOW, WINDOW), WINDOW)
            band = pl.ds(pl.multiple_of(b * WINDOW, WINDOW), span)
            where = i_k + (me * rows + b * WINDOW - WINDOW)
            valid = near & (where >= 0) & (where < n * rows)
            for h in range(heads):
                cols = pl.ds(h * HEAD, HEAD)
                s = lax.dot_general(qw[r, cols], kw[0, band, :], contract_last, preferred_element_type=F32)
                s = jnp.where(valid, s * scale, -jnp.inf)
                sunk = jnp.full((WINDOW, lanes), sink[h], F32)
                peak = jnp.maximum(jnp.max(s, axis=1, keepdims=True), sunk)
                e = jnp.exp(s - jnp.concatenate([peak] * 3, axis=1))
                whole = jnp.sum(e, axis=1, keepdims=True) + jnp.exp(sunk - peak)
                w = (e / jnp.concatenate([whole] * 3, axis=1)).astype(BF16)
                res = jnp.dot(w, kw[1, band, :], preferred_element_type=F32).astype(BF16)
                for j in range(WINDOW // block):
                    yv[j % 2, b * (WINDOW // block // 2) + j // 2, :, cols] = res[j * block : (j + 1) * block]
            return carry

        lax.fori_loop(lo, hi, one, 0)

    width = 512

    def columns(one):
        def run(j, carry):
            one(pl.ds(pl.multiple_of(j * width, width), width))
            return carry

        lax.fori_loop(0, out.shape[1] // width, run, 0)

    def window_rows(core, cols):
        ys = yv[core].reshape(NX * block, wq)
        return jnp.dot(ys, pwb[:, cols], preferred_element_type=F32).reshape(NX, block, width)

    def to_give(cols):
        give[:, :, cols] = window_rows(1 - c, cols).astype(BF16)

    def to_sum(cols):
        take[:, :, cols] = (window_rows(c, cols) + take[:, :, cols].astype(F32)).astype(BF16)

    attend(me)

    def phase2(s, carry):
        for k in range(4):
            ring.land(s, k)
            ring.start(s + 1, k)
            if k == 0:

                @pl.when(s == 0)
                def _():
                    ring2.land(last, 0)
                    swap2.start(ring2.origin(0, last + 1))
                    late.step(0)

                @pl.when(s == 1)
                def _():
                    late.step(1)

                @pl.when(s == 2)
                def _():
                    gather(w2, swap2, acc2, 0, n // 2)

                @pl.when(s == 3)
                def _():
                    twin(0, True).wait_recv()
                    window(1, rows // WINDOW - 1, 1)

                @pl.when(s == 4)
                def _():
                    for i in (1, 2):
                        twin(i, True).wait_recv()
                    window(0, 2, rows // WINDOW - 1)

                @pl.when(s == 5)
                def _():
                    pass_on.wait_recv()
                    columns(to_sum)
                    for d in (0, 1):
                        relay(d, False).start()

            if k == 2:

                @pl.when(s == 2)
                def _():
                    gather(w2, swap2, acc2, n // 2, n)
                    kw[c, spans[0]] = acc2[:, wq:].astype(BF16)
                    qw[...] = acc2[:, :wq].astype(BF16)
                    for d in (0, 1):
                        edge(d, False).start()
                    twin(0, False).start()

                @pl.when(s == 3)
                def _():
                    for d in (0, 1):
                        edge(d, True).wait_recv()
                        twin(d + 1, False).start()
                    late.step(2)

                @pl.when(s == 4)
                def _():
                    columns(to_give)
                    pass_on.start()

            if k % 2 == 1:

                @pl.when(s > 0)
                def _():
                    attend(ring.origin(k // 2, s))

        return carry

    lax.fori_loop(0, last - 1, phase2, 0)
    for k in range(4):
        ring.land(last - 1, k)
        if k < 2:
            ring.start(last, k)
        if k == 0:
            merge()
        if k % 2 == 1:
            attend(ring.origin(k // 2, last - 1))
    late.finish()
    for r in (ring1, ring2, swap1, swap2, side, late):
        r.drain()
    for d in (0, 1):
        edge(d, False).wait_send()
    for i in range(3):
        twin(i, False).wait_send()
    pass_on.wait_send()

    def both(i, carry):
        attend(lax.rem(me + n - last + 2 * last * i, n))
        return carry

    lax.fori_loop(0, 2, both, 0)
    for k in (0, 1):
        ring.land(last, k)
    attend(lax.rem(me + last + 1, n))

    def close(j):
        r = pl.ds(pl.multiple_of(j * block, block), block)
        parts = [1.0 / jnp.sum(tot[m, r, :], axis=1, keepdims=True) for m in range(2)]
        d = acc[0, r, :] * parts[0] - acc[1, r, :] * (lam[0] * parts[1])
        d = d * lax.rsqrt(jnp.mean(d * d, axis=-1, keepdims=True) + EPS) * ogain[...]
        return d.astype(BF16)

    for k in (4, 5, 2, 6, 3, 7, 1):
        j = 2 * lax.rem(x + k // 2, NX) + lax.rem(c + k % 2, 2)
        y[j] = close(j)
        trade(k, False).start()
    yd[t] = close(t)
    wide = 1024

    def add(total, away, cols):
        first = 2 * lax.rem(x + NX - away, NX)
        for h in (0, 1):
            total = total + jnp.dot(yd[first + h], pdb[first + h, :, cols], preferred_element_type=F32)
        return total

    def begin(j, carry):
        cols = pl.ds(pl.multiple_of(j * wide, wide), wide)
        total = take[x, :, cols].astype(F32)
        for d in (0, 1):
            total = total + sums[d, :, cols].astype(F32)
        facc[:, cols] = add(total, 0, cols)
        return carry

    def finish(j, carry):
        cols = pl.ds(pl.multiple_of(j * wide, wide), wide)
        total = facc[:, cols]
        for away in (1, 3, 2):
            total = add(total, away, cols)
        out[:, cols] = total.astype(out.dtype)
        return carry

    for d in (0, 1):
        deal(d, True).wait_recv()
    trade(1, True).wait_recv()
    lax.fori_loop(0, out.shape[1] // wide, begin, 0)
    for k in range(2, 2 * NX):
        trade(k, True).wait_recv()
    lax.fori_loop(0, out.shape[1] // wide, finish, 0)
    for k in range(1, 2 * NX):
        trade(k, False).wait_send()
    for d in (0, 1):
        relay(d, False).wait_send()
        deal(d, False).wait_send()
    ring.drain()


def body(
    n, tokens, norm_gain, query_diff, key_diff, value_diff, lam, output_norm_gain,
    query_win, keyval_win, sink, proj_diff, proj_win,
):
    block, model = tokens.shape
    rows = block * 2 * NX
    depth, wq = query_win.shape
    kvd = key_diff.shape[1] + value_diff.shape[1]
    dq = query_diff.shape[1]
    part = keyval_win.shape[2] // 2
    hops = n // 2

    def pair(*shape):
        return [DMA(shape), DMA(shape)]

    return pl.pallas_call(
        functools.partial(layer_kernel, n, sink.shape[0]),
        out_shape=jax.ShapeDtypeStruct((block, model), BF16),
        in_specs=[
            pl.BlockSpec(memory_space=m)
            for m in [ANY, VMEM] + [ANY] * 7 + [pltpu.SMEM, pltpu.SMEM, VMEM]
        ],
        out_specs=pl.BlockSpec(memory_space=VMEM),
        scratch_shapes=[
            VMEM((n, depth, kvd + dq), BF16),
            VMEM((n, depth, wq + part), BF16),
            VMEM((2 * NX, block, model), BF16),
            VMEM((n, rows, depth), BF16),
            VMEM((rows, kvd + dq), F32),
            VMEM((rows, wq + part), F32),
            VMEM((n, rows, kvd), BF16),
            VMEM((2 * NX,) + proj_diff.shape, BF16),
            VMEM(proj_win.shape, BF16),
            VMEM((rows, dq), BF16),
            VMEM((rows, wq), BF16),
            VMEM((2, rows + 2 * WINDOW, part), BF16),
            VMEM((2, rows, HEAD), F32),
            VMEM((2, rows, HEAD), F32),
            VMEM((2, rows, VDIM), F32),
            VMEM((2 * NX, block, VDIM), BF16),
            VMEM((2 * NX, block, VDIM), BF16),
            VMEM((2, NX, block, wq), BF16),
            VMEM((NX, block, model), BF16),
            VMEM((NX, block, model), BF16),
            VMEM((2, block // 2, model), BF16),
            VMEM((2, block, model), BF16),
            VMEM((block, model), F32),
            DMA((8,)),
        ]
        + pair(2, hops, 4)
        + pair(n)
        + pair(2, hops, 2)
        + pair(n)
        + pair(2, hops, 4)
        + pair(2)
        + pair(3)
        + pair(2 * NX)
        + pair(5)
        + side_sems()
        + side_sems(),
        compiler_params=pltpu.CompilerParams(
            collective_id=0, has_side_effects=True, vmem_limit_bytes=67_000_000
        ),
    )(
        tokens, norm_gain.reshape(1, model), key_diff, value_diff, query_diff, query_win, keyval_win,
        proj_diff, proj_win, lam, sink, output_norm_gain.reshape(1, VDIM),
    )


def solution(mesh):
    torus = Mesh(
        mesh.devices.reshape(mesh.shape["grp"], mesh.shape["sp"], NX, 2),
        ("grp", "sp", "tp_0", "tp_1"),
    )
    return jax.shard_map(
        functools.partial(body, mesh.shape["sp"]),
        mesh=torus,
        in_specs=(
            P(GRP_SP_TP, None),
            P(),
            P("sp", TP),
            P("sp", TP),
            P("sp", TP),
            P(TP),
            P(),
            P("sp", TP),
            P(None, "sp", None),
            P(TP),
            P(TP, None),
            P(TP, None),
        ),
        out_specs=P(GRP_SP_TP, None),
        check_vma=False,
    )
```

```python
import functools

import jax
import jax.numpy as jnp
from jax import lax
from jax.experimental import pallas as pl
from jax.experimental.pallas import tpu as pltpu
from jax.sharding import Mesh
from jax.sharding import PartitionSpec as P

HEAD = 128
WIN_HEADS = 16
KV_HEADS = 4
WINDOW = 128
VDIM = 256
NX = 4
CUT = 96
TP = ("tp_0", "tp_1")
GRP_SP_TP = ("grp", "sp", "tp_0", "tp_1")
EPS = 1e-06
LOG2E = 1.4426950408889634
BF16 = jnp.bfloat16
F32 = jnp.float32
MESH = pl.DeviceIdType.MESH
DMA = pltpu.SemaphoreType.DMA
VMEM = pltpu.VMEM
ANY = pl.ANY


def remote(src, dst, send_sem, recv_sem, where):
    return pltpu.make_async_remote_copy(
        src_ref=src,
        dst_ref=dst,
        send_sem=send_sem,
        recv_sem=recv_sem,
        device_id=where,
        device_id_type=MESH,
    )


def greet(peers):
    barrier = pltpu.get_barrier_semaphore()
    for peer in peers:
        pl.semaphore_signal(barrier, inc=1, device_id=peer, device_id_type=MESH)
    pl.semaphore_wait(barrier, len(peers))


class Ring:
    def __init__(self, n, buf, base, cuts, send, recv):
        self.n, self.buf, self.send, self.recv = n, buf, send, recv
        self.base, self.cuts = base, cuts
        self.spans = []
        for cut in cuts:
            self.spans.append(pl.ds(base, cut))
            base = base + cut
        self.count = len(cuts)
        self.me = lax.axis_index("sp")
        self.to = (
            {"sp": lax.rem(self.me + 1, n)},
            {"sp": lax.rem(self.me + n - 1, n)},
        )

    def origin(self, d, s):
        return lax.rem(self.me + (self.n - s if d == 0 else s), self.n)

    def piece(self, d, s, k, hops):
        ref = self.buf.at[self.origin(d, hops), self.spans[k if d == 0 else self.count - 1 - k]]
        return remote(ref, ref, self.send.at[0], self.recv.at[s, k], self.to[d])

    def start(self, s, k):
        for d in (0, 1):
            self.piece(d, s, k, s).start()

    def land(self, s, k):
        both = pl.ds(self.base, self.cuts[k] + self.cuts[self.count - 1 - k])
        ref = self.buf.at[self.me, both]
        remote(ref, ref, self.send.at[0], self.recv.at[s, k], self.to[0]).wait_recv()

    def drain(self):
        ref = self.buf.at[pl.ds(0, self.n - 1), pl.ds(self.base, sum(self.cuts))]
        remote(ref, ref, self.send.at[0], self.recv.at[0, 0], self.to[0]).wait_send()


class Swap:
    def __init__(self, n, buf, cut, send, recv):
        self.n, self.buf, self.cut, self.send, self.recv = n, buf, cut, send, recv
        g = lax.axis_index("grp")
        self.odd = lax.rem(g, 2)
        self.to = {"grp": g + 1 - 2 * self.odd}
        self.kept = buf.shape[1] - cut
        self.base = pl.multiple_of(self.odd * cut, 16)

    def piece(self, o, odd, sem):
        ref = self.buf.at[o, pl.ds(pl.multiple_of(odd * self.kept, 16), self.cut)]
        return remote(ref, ref, self.send.at[0], self.recv.at[sem], self.to)

    def start(self, o, sem=None):
        self.piece(o, self.odd, o if sem is None else sem).start()

    def land(self, o):
        self.piece(o, 1 - self.odd, o).wait_recv()

    def several(self, count, sem):
        ref = self.buf.at[pl.ds(0, count), pl.ds(0, self.cut)]
        return remote(ref, ref, self.send.at[0], self.recv.at[sem], self.to)

    def drain(self):
        self.several(self.n - 1, 0).wait_send()


class Side:
    def __init__(self, own, slots, half, xs, xr, cs, cr):
        self.own, self.slots, self.half = own, slots, half
        self.xs, self.xr, self.cs, self.cr = xs, xr, cs, cr
        self.x = lax.axis_index("tp_0")
        self.c = lax.axis_index("tp_1")
        self.to = (
            {"tp_0": lax.rem(self.x + 1, NX)},
            {"tp_0": lax.rem(self.x + NX - 1, NX)},
        )
        self.other = {"tp_1": 1 - self.c}

    def spot(self, rel, h, core):
        slot = 2 * lax.rem(self.x + rel, NX) + core
        return self.slots.at[slot, pl.ds(h * self.half, self.half)]

    def source(self, rel, h):
        if rel == 0 and self.own is not None:
            return self.own.at[pl.ds(h * self.half, self.half)]
        return self.spot(rel, h, self.c)

    def half_of(self, d, k):
        return (0, 1, 0)[k] if d == 0 else (1, 0, 1)[k]

    def out(self, d, k):
        rel = 0 if k < 2 else (3 if d == 0 else 1)
        h = self.half_of(d, k)
        return remote(
            self.source(rel, h), self.spot(rel, h, self.c), self.xs.at[0], self.xr.at[k], self.to[d]
        )

    def inward(self, d, k):
        return (3 if d == 0 else 1) if k < 2 else 2, self.half_of(d, k)

    def blocks(self, count, send, recv, where):
        ref = self.slots.at[pl.ds(0, count)]
        return remote(ref, ref, send, recv, where)

    def across(self, rel, h):
        return remote(
            self.source(rel, h), self.spot(rel, h, self.c), self.cs.at[0], self.cr.at[0], self.other
        )

    def start(self):
        for k in (0, 1):
            for d in (0, 1):
                self.out(d, k).start()
        for h in (0, 1):
            self.across(0, h).start()

    def step(self, k):
        self.blocks(1, self.xs.at[0], self.xr.at[k], self.to[0]).wait_recv()
        for d in (0, 1):
            if k == 0:
                self.out(d, 2).start()
            self.across(*self.inward(d, k)).start()

    def finish(self):
        self.blocks(NX, self.cs.at[0], self.cr.at[0], self.other).wait_recv()

    def drain(self):
        self.blocks(NX - 1, self.xs.at[0], self.xr.at[0], self.to[0]).wait_send()
        self.blocks(NX, self.cs.at[0], self.cr.at[0], self.other).wait_send()


def side_sems():
    return [DMA((1,)), DMA((3,)), DMA((1,)), DMA((1,))]


def layer_kernel(
    n, heads_win, tok, gain, kd, vd, qd, qwd, kvw, pd, pw, lam, sink, ogain, out,
    w1, w2, raw, nbuf, acc1, acc2, kbuf, pdb, pwb, q, qw, kw, top, tot, acc, y, yd, yv, give, take, far, sums, facc,
    lsem, z1s, z1r, y1s, y1r, z2s, z2r, y2s, y2r, zks, zkr, hs, hr, us, ur, ts, tr, ws, wr, *sems,
):
    me, x, c = (lax.axis_index(a) for a in ("sp", "tp_0", "tp_1"))
    t = 2 * x + c
    block = raw.shape[1]
    rows = 2 * NX * block
    depth = w1.shape[1]
    part = kvw.shape[2] // 2
    head = t * heads_win // (WIN_HEADS // KV_HEADS)
    wq = qwd.shape[1]
    local = []
    at = 0
    for w in (kd, vd, qd):
        local.append((w, w1.at[me, :, pl.ds(at, w.shape[1])]))
        at += w.shape[1]
    local += [
        (qwd, w2.at[me, :, pl.ds(0, wq)]),
        (kvw.at[head, :, pl.ds(pl.multiple_of(c * part, part), part)], w2.at[me, :, pl.ds(wq, part)]),
        (tok, raw.at[t]),
        (pd, pdb.at[t]),
        (pw, pwb),
    ]
    local = [pltpu.make_async_copy(a, b, lsem.at[i]) for i, (a, b) in enumerate(local)]
    for copy in local:
        copy.start()

    swap1 = Swap(n, w1, CUT, y1s, y1r)
    swap2 = Swap(n, w2, depth // 2, y2s, y2r)
    ring1 = Ring(n, w1, swap1.base, (48, 32, 32, swap1.kept - 112), z1s, z1r)
    ring2 = Ring(n, w2, swap2.base, (depth // 4,) * 2, z2s, z2r)
    ring = Ring(n, kbuf, 0, (rows // 4,) * 4, zks, zkr)
    side = Side(None, raw, block // 2, *sems[:4])
    late = Side(None, pdb, depth // 2, *sems[4:])

    def peer(k):
        return {"tp_0": lax.rem(x + k // 2, NX), "tp_1": lax.rem(c + k % 2, 2)}

    greet([ring.to[0], ring.to[1], swap1.to] + [peer(k) for k in range(1, 2 * NX)])

    for copy in local[:3]:
        copy.wait()
    for k in range(4):
        ring1.start(0, k)
    local[5].wait()
    side.start()
    acc1[...] = jnp.zeros_like(acc1)
    acc2[...] = jnp.zeros_like(acc2)
    top[...] = jnp.full_like(top, -jnp.inf)
    tot[...] = jnp.zeros_like(tot)
    acc[...] = jnp.zeros_like(acc)
    for copy in local[3:5] + local[6:]:
        copy.wait()

    def normalise(quarter):
        tile = 32
        per = raw.shape[0] * block // tile // 4

        def one(j, carry):
            i = quarter * per + j
            slot, r = i // (block // tile), lax.rem(i, block // tile)
            v = raw[slot, pl.ds(pl.multiple_of(r * tile, tile), tile), :].astype(F32)
            v = v * lax.rsqrt(jnp.mean(v * v, axis=-1, keepdims=True) + EPS) * gain[...]
            v = v.astype(BF16)
            for o in range(n):
                nbuf[o, pl.ds(pl.multiple_of(i * tile, tile), tile), :] = v[:, o * depth : (o + 1) * depth]
            return carry

        lax.fori_loop(0, per, one, 0)

    def gather(w, swap, total, lo, hi):
        def one(j, carry):
            o = lax.rem(me + jnp.where(lax.rem(j, 2) == 1, (j + 1) // 2, n - j // 2), n)

            if swap is not None:

                @pl.when(j > 0)
                def _():
                    swap.land(o)

            total[...] += jnp.dot(nbuf[o], w[o], preferred_element_type=F32)
            return carry

        lax.fori_loop(lo, hi, one, 0)

    last = n // 2 - 1

    def swap_both(swap, ring_, hops):
        for d in (0, 1):
            swap.start(ring_.origin(d, hops))

    def swap_late(hops):
        for d in (0, 1):
            swap2.start(ring2.origin(d, hops), jnp.where(2 * hops - d < n // 2, 0, 1))

    def hop2(s, k):
        ring2.land(s, k)
        ring2.start(s + 1, k)

    def late_swaps(lo, hi):
        def one(h, carry):
            swap_late(h)
            return carry

        lax.fori_loop(lo, hi, one, 0)

    def phase1(s, carry):
        for k in range(4):
            ring1.land(s, k)
            ring1.start(s + 1, k)
            if k == 0:
                for i in range(3):

                    @pl.when(s == i + 1)
                    def _():
                        side.step(i)
                        if i == 2:
                            late.start()

                @pl.when(s == last - 3)
                def _():
                    side.finish()

            @pl.when(s == last - 3)
            def _():
                normalise(k)

            @pl.when(s == last - 2)
            def _():
                gather(w1, swap1, acc1, 3 * k, min(3 * k + 3, 2 * last - 3))

            if k % 2 == 1:

                @pl.when(s >= 2)
                def _():
                    hop2(s - 2, k // 2)

        swap_both(swap1, ring1, s + 1)

        @pl.when(s == 0)
        def _():
            for k in (0, 1):
                ring2.start(0, k)

        return carry

    lax.fori_loop(0, last - 1, phase1, 0)
    done = 2 * last - 3
    for k in range(4):
        ring1.land(last - 1, k)
        if k < 2:
            ring1.start(last, k)
        if k % 2 == 1:
            hop2(last - 3, k // 2)
        if k == 2:
            gather(w1, swap1, acc1, done, done + 1)
    swap_both(swap1, ring1, last)
    gather(w1, swap1, acc1, done + 1, done + 2)
    for k in (0, 1):
        ring1.land(last, k)
    swap1.start(ring1.origin(0, last + 1))
    for k in (0, 1):
        hop2(last - 2, k)
    late_swaps(1, last)
    gather(w1, swap1, acc1, done + 2, done + 4)
    ring2.land(last - 1, 0)
    ring2.start(last, 0)
    ring2.land(last - 1, 1)
    swap_late(last)
    gather(w1, swap1, acc1, n - 1, n)
    kvd = kbuf.shape[2]
    kbuf[me] = acc1[:, :kvd].astype(BF16)
    q[...] = acc1[:, kvd:].astype(BF16)
    for k in range(4):
        ring.start(0, k)

    def edge(d, inward):
        src = pl.ds(rows, WINDOW) if d == 0 else pl.ds(WINDOW, WINDOW)
        dst = pl.ds(0, WINDOW) if d == 0 else pl.ds(rows + WINDOW, WINDOW)
        target = kw.at[c, dst]
        return remote(target if inward else kw.at[c, src], target, hs.at[d], hr.at[d], ring.to[d])

    spans = (pl.ds(WINDOW, rows), pl.ds(0, WINDOW), pl.ds(rows + WINDOW, WINDOW))

    def twin(i, inward):
        ref = kw.at[1 - c if inward else c, spans[i]]
        return remote(ref, ref, us.at[i], ur.at[i], side.other)

    def trade(k):
        src = y.at[2 * lax.rem(x + k // 2, NX) + lax.rem(c + k % 2, 2)]
        return remote(src, yd.at[t], ts.at[0], tr.at[min(k - 1, 1)], peer(k))

    def traded(count, sem):
        ref = yd.at[pl.ds(0, count)]
        return remote(ref, ref, ts.at[0], tr.at[sem], side.other)

    pass_on = remote(give, take, ws.at[0], wr.at[0], side.other)

    def relay(d, inward):
        src = far.at[d] if inward else take.at[lax.rem(x + 2, NX), pl.ds(d * (block // 2), block // 2)]
        return remote(src, far.at[d], ws.at[1 + d], wr.at[1 + d], side.to[d])

    def deal(d, inward):
        src = sums.at[d] if inward else take.at[lax.rem(x + (1, NX - 1)[d], NX)]
        return remote(src, sums.at[d], ws.at[3 + d], wr.at[3 + d], side.to[d])

    def merge():
        for d in (0, 1):
            relay(d, True).wait_recv()
            to = lax.rem(x + (1, NX - 1)[d], NX)
            half = pl.ds(d * (block // 2), block // 2)
            take[to, half, :] = (take[to, half, :].astype(F32) + far[d].astype(F32)).astype(BF16)
        for d in (0, 1):
            deal(d, False).start()

    scale = HEAD**-0.5
    lanes = HEAD
    contract_last = (((1,), (1,)), ((), ()))

    def attend(o):
        def one(m, carry):
            cols = pl.ds(pl.multiple_of(m * HEAD, HEAD), HEAD)
            s = lax.dot_general(q[:, cols], kbuf[o, :, cols], contract_last, preferred_element_type=F32)
            s = s * (scale * LOG2E)
            reps = s.shape[1] // lanes
            was = top[m]
            now = jnp.maximum(was, jnp.max(s, axis=1, keepdims=True))
            fade = jnp.exp2(was - now)
            e = jnp.exp2(s - jnp.concatenate([now] * reps, axis=1))
            some = e[:, :lanes]
            for j in range(1, reps):
                some = some + e[:, j * lanes : (j + 1) * lanes]
            tot[m] = tot[m] * fade + some
            top[m] = now
            acc[m] = acc[m] * jnp.concatenate([fade] * (VDIM // lanes), axis=1) + jnp.dot(
                e.astype(BF16), kbuf[o, :, 2 * HEAD :], preferred_element_type=F32
            )
            return carry

        for m in range(2):
            one(m, 0)

    def window(lo, hi, stride):
        span = 3 * WINDOW
        heads = wq // HEAD
        i_q = lax.broadcasted_iota(jnp.int32, (WINDOW, span), 0)
        i_k = lax.broadcasted_iota(jnp.int32, (WINDOW, span), 1)
        near = jnp.abs(i_k - WINDOW - i_q) <= WINDOW

        def one(i, carry):
            b = i * stride
            r = pl.ds(pl.multiple_of(b * WINDOW, WINDOW), WINDOW)
            band = pl.ds(pl.multiple_of(b * WINDOW, WINDOW), span)
            where = i_k + (me * rows + b * WINDOW - WINDOW)
            valid = near & (where >= 0) & (where < n * rows)
            for h in range(heads):
                cols = pl.ds(h * HEAD, HEAD)
                s = lax.dot_general(qw[r, cols], kw[0, band, :], contract_last, preferred_element_type=F32)
                s = jnp.where(valid, s * scale, -jnp.inf)
                sunk = jnp.full((WINDOW, lanes), sink[h], F32)
                peak = jnp.maximum(jnp.max(s, axis=1, keepdims=True), sunk)
                e = jnp.exp(s - jnp.concatenate([peak] * 3, axis=1))
                whole = jnp.sum(e, axis=1, keepdims=True) + jnp.exp(sunk - peak)
                w = (e / jnp.concatenate([whole] * 3, axis=1)).astype(BF16)
                res = jnp.dot(w, kw[1, band, :], preferred_element_type=F32).astype(BF16)
                for j in range(WINDOW // block):
                    yv[j % 2, b * (WINDOW // block // 2) + j // 2, :, cols] = res[j * block : (j + 1) * block]
            return carry

        lax.fori_loop(lo, hi, one, 0)

    width = 512

    def columns(one):
        def run(j, carry):
            one(pl.ds(pl.multiple_of(j * width, width), width))
            return carry

        lax.fori_loop(0, out.shape[1] // width, run, 0)

    def window_rows(core, cols):
        ys = yv[core].reshape(NX * block, wq)
        return jnp.dot(ys, pwb[:, cols], preferred_element_type=F32).reshape(NX, block, width)

    def to_give(cols):
        give[:, :, cols] = window_rows(1 - c, cols).astype(BF16)

    def to_sum(cols):
        take[:, :, cols] = (window_rows(c, cols) + take[:, :, cols].astype(F32)).astype(BF16)

    attend(me)

    def phase2(s, carry):
        for k in range(4):
            ring.land(s, k)
            ring.start(s + 1, k)
            if k == 0:

                @pl.when(s == 0)
                def _():
                    ring2.land(last, 0)
                    swap2.start(ring2.origin(0, last + 1), 1)
                    late.step(0)

                @pl.when(s == 1)
                def _():
                    late.step(1)

                @pl.when(s == 2)
                def _():
                    swap2.several(n // 2 - 1, 0).wait_recv()
                    gather(w2, None, acc2, 0, n // 2)

                @pl.when(s == 3)
                def _():
                    twin(0, True).wait_recv()
                    window(1, rows // WINDOW - 1, 1)

                @pl.when(s == 4)
                def _():
                    columns(to_give)
                    pass_on.start()

            if k == 2:

                @pl.when(s == 2)
                def _():
                    swap2.several(n // 2, 1).wait_recv()
                    gather(w2, None, acc2, n // 2, n)
                    kw[c, spans[0]] = acc2[:, wq:].astype(BF16)
                    qw[...] = acc2[:, :wq].astype(BF16)
                    for d in (0, 1):
                        edge(d, False).start()
                    twin(0, False).start()

                @pl.when(s == 3)
                def _():
                    for d in (0, 1):
                        edge(d, True).wait_recv()
                        twin(d + 1, False).start()
                    late.step(2)

                @pl.when(s == 4)
                def _():
                    pass_on.wait_recv()
                    columns(to_sum)
                    for d in (0, 1):
                        relay(d, False).start()

                @pl.when(s == 5)
                def _():
                    merge()

            if k == 3:

                @pl.when(s == 3)
                def _():
                    for i in (1, 2):
                        twin(i, True).wait_recv()
                    window(0, 2, rows // WINDOW - 1)

            if k % 2 == 1:

                @pl.when(s > 0)
                def _():
                    attend(ring.origin(k // 2, s))

        return carry

    lax.fori_loop(0, last - 1, phase2, 0)
    for k in range(4):
        ring.land(last - 1, k)
        if k < 2:
            ring.start(last, k)
        if k % 2 == 1:
            attend(ring.origin(k // 2, last - 1))
    late.finish()
    for r in (ring1, ring2, swap1, swap2, side, late):
        r.drain()
    for d in (0, 1):
        edge(d, False).wait_send()
    for i in range(3):
        twin(i, False).wait_send()
    pass_on.wait_send()

    def both(i, carry):
        attend(lax.rem(me + n - last + 2 * last * i, n))
        return carry

    lax.fori_loop(0, 2, both, 0)
    for k in (0, 1):
        ring.land(last, k)
    attend(lax.rem(me + last + 1, n))

    def close(j):
        r = pl.ds(pl.multiple_of(j * block, block), block)
        parts = [1.0 / jnp.sum(tot[m, r, :], axis=1, keepdims=True) for m in range(2)]
        d = acc[0, r, :] * parts[0] - acc[1, r, :] * (lam[0] * parts[1])
        d = d * lax.rsqrt(jnp.mean(d * d, axis=-1, keepdims=True) + EPS) * ogain[...]
        return d.astype(BF16)

    for k in (4, 5, 2, 6, 3, 7, 1):
        j = 2 * lax.rem(x + k // 2, NX) + lax.rem(c + k % 2, 2)
        y[j] = close(j)
        trade(k).start()
    yd[t] = close(t)
    wide = 1024

    def add(total, away, cols):
        first = 2 * lax.rem(x + NX - away, NX)
        for h in (0, 1):
            total = total + jnp.dot(yd[first + h], pdb[first + h, :, cols], preferred_element_type=F32)
        return total

    def begin(j, carry):
        cols = pl.ds(pl.multiple_of(j * wide, wide), wide)
        total = take[x, :, cols].astype(F32)
        for d in (0, 1):
            total = total + sums[d, :, cols].astype(F32)
        facc[:, cols] = add(total, 0, cols)
        return carry

    def finish(j, carry):
        cols = pl.ds(pl.multiple_of(j * wide, wide), wide)
        total = facc[:, cols]
        for away in (1, 3, 2):
            total = add(total, away, cols)
        out[:, cols] = total.astype(out.dtype)
        return carry

    for d in (0, 1):
        deal(d, True).wait_recv()
    traded(1, 0).wait_recv()
    lax.fori_loop(0, out.shape[1] // wide, begin, 0)
    traded(2 * NX - 2, 1).wait_recv()
    lax.fori_loop(0, out.shape[1] // wide, finish, 0)
    traded(2 * NX - 1, 0).wait_send()
    for d in (0, 1):
        relay(d, False).wait_send()
        deal(d, False).wait_send()
    ring.drain()


def body(
    n, tokens, norm_gain, query_diff, key_diff, value_diff, lam, output_norm_gain,
    query_win, keyval_win, sink, proj_diff, proj_win,
):
    block, model = tokens.shape
    rows = block * 2 * NX
    depth, wq = query_win.shape
    kvd = key_diff.shape[1] + value_diff.shape[1]
    dq = query_diff.shape[1]
    part = keyval_win.shape[2] // 2
    hops = n // 2

    def pair(*shape):
        return [DMA(shape), DMA(shape)]

    return pl.pallas_call(
        functools.partial(layer_kernel, n, sink.shape[0]),
        out_shape=jax.ShapeDtypeStruct((block, model), BF16),
        in_specs=[
            pl.BlockSpec(memory_space=m)
            for m in [ANY, VMEM] + [ANY] * 7 + [pltpu.SMEM, pltpu.SMEM, VMEM]
        ],
        out_specs=pl.BlockSpec(memory_space=VMEM),
        scratch_shapes=[
            VMEM((n, depth, kvd + dq), BF16),
            VMEM((n, depth, wq + part), BF16),
            VMEM((2 * NX, block, model), BF16),
            VMEM((n, rows, depth), BF16),
            VMEM((rows, kvd + dq), F32),
            VMEM((rows, wq + part), F32),
            VMEM((n, rows, kvd), BF16),
            VMEM((2 * NX,) + proj_diff.shape, BF16),
            VMEM(proj_win.shape, BF16),
            VMEM((rows, dq), BF16),
            VMEM((rows, wq), BF16),
            VMEM((2, rows + 2 * WINDOW, part), BF16),
            VMEM((2, rows, HEAD), F32),
            VMEM((2, rows, HEAD), F32),
            VMEM((2, rows, VDIM), F32),
            VMEM((2 * NX, block, VDIM), BF16),
            VMEM((2 * NX, block, VDIM), BF16),
            VMEM((2, NX, block, wq), BF16),
            VMEM((NX, block, model), BF16),
            VMEM((NX, block, model), BF16),
            VMEM((2, block // 2, model), BF16),
            VMEM((2, block, model), BF16),
            VMEM((block, model), F32),
            DMA((8,)),
        ]
        + [DMA((1,)), DMA((hops, 4)), DMA((1,)), DMA((n,))]
        + [DMA((1,)), DMA((hops, 2)), DMA((1,)), DMA((2,))]
        + [DMA((1,)), DMA((hops, 4))]
        + pair(2)
        + pair(3)
        + [DMA((1,)), DMA((2,))]
        + pair(5)
        + side_sems()
        + side_sems(),
        compiler_params=pltpu.CompilerParams(
            collective_id=0, has_side_effects=True, vmem_limit_bytes=67_000_000
        ),
    )(
        tokens, norm_gain.reshape(1, model), key_diff, value_diff, query_diff, query_win, keyval_win,
        proj_diff, proj_win, lam, sink, output_norm_gain.reshape(1, VDIM),
    )


def solution(mesh):
    torus = Mesh(
        mesh.devices.reshape(mesh.shape["grp"], mesh.shape["sp"], NX, 2),
        ("grp", "sp", "tp_0", "tp_1"),
    )
    return jax.shard_map(
        functools.partial(body, mesh.shape["sp"]),
        mesh=torus,
        in_specs=(
            P(GRP_SP_TP, None),
            P(),
            P("sp", TP),
            P("sp", TP),
            P("sp", TP),
            P(TP),
            P(),
            P("sp", TP),
            P(None, "sp", None),
            P(TP),
            P(TP, None),
            P(TP, None),
        ),
        out_specs=P(GRP_SP_TP, None),
        check_vma=False,
    )
```

```python
import functools

import jax
import jax.numpy as jnp
from jax import lax
from jax.experimental import pallas as pl
from jax.experimental.pallas import tpu as pltpu
from jax.sharding import Mesh
from jax.sharding import PartitionSpec as P

HEAD = 128
WIN_HEADS = 16
KV_HEADS = 4
WINDOW = 128
VDIM = 256
NX = 4
CUT = 80
TP = ("tp_0", "tp_1")
GRP_SP_TP = ("grp", "sp", "tp_0", "tp_1")
EPS = 1e-06
LOG2E = 1.4426950408889634
BF16 = jnp.bfloat16
F32 = jnp.float32
MESH = pl.DeviceIdType.MESH
DMA = pltpu.SemaphoreType.DMA
VMEM = pltpu.VMEM
ANY = pl.ANY


def remote(src, dst, send_sem, recv_sem, where):
    return pltpu.make_async_remote_copy(
        src_ref=src,
        dst_ref=dst,
        send_sem=send_sem,
        recv_sem=recv_sem,
        device_id=where,
        device_id_type=MESH,
    )


def greet(peers):
    barrier = pltpu.get_barrier_semaphore()
    for peer in peers:
        pl.semaphore_signal(barrier, inc=1, device_id=peer, device_id_type=MESH)
    pl.semaphore_wait(barrier, len(peers))


class Ring:
    def __init__(self, n, buf, base, cuts, send, recv):
        self.n, self.buf, self.send, self.recv = n, buf, send, recv
        self.base, self.cuts = base, cuts
        self.spans = []
        for cut in cuts:
            self.spans.append(pl.ds(base, cut))
            base = base + cut
        self.count = len(cuts)
        self.me = lax.axis_index("sp")
        self.to = (
            {"sp": lax.rem(self.me + 1, n)},
            {"sp": lax.rem(self.me + n - 1, n)},
        )

    def origin(self, d, s):
        return lax.rem(self.me + (self.n - s if d == 0 else s), self.n)

    def piece(self, d, s, k, hops):
        ref = self.buf.at[self.origin(d, hops), self.spans[k if d == 0 else self.count - 1 - k]]
        return remote(ref, ref, self.send.at[0], self.recv.at[s, k], self.to[d])

    def start(self, s, k):
        for d in (0, 1):
            self.piece(d, s, k, s).start()

    def land(self, s, k):
        both = pl.ds(self.base, self.cuts[k] + self.cuts[self.count - 1 - k])
        ref = self.buf.at[self.me, both]
        remote(ref, ref, self.send.at[0], self.recv.at[s, k], self.to[0]).wait_recv()

    def drain(self):
        ref = self.buf.at[pl.ds(0, self.n - 1), pl.ds(self.base, sum(self.cuts))]
        remote(ref, ref, self.send.at[0], self.recv.at[0, 0], self.to[0]).wait_send()


class Swap:
    def __init__(self, n, buf, cut, send, recv):
        self.n, self.buf, self.cut, self.send, self.recv = n, buf, cut, send, recv
        g = lax.axis_index("grp")
        self.odd = lax.rem(g, 2)
        self.to = {"grp": g + 1 - 2 * self.odd}
        self.kept = buf.shape[1] - cut
        self.base = pl.multiple_of(self.odd * cut, 16)

    def piece(self, o, odd, sem):
        ref = self.buf.at[o, pl.ds(pl.multiple_of(odd * self.kept, 16), self.cut)]
        return remote(ref, ref, self.send.at[0], self.recv.at[sem], self.to)

    def start(self, o, sem=None):
        self.piece(o, self.odd, o if sem is None else sem).start()

    def land(self, o):
        self.piece(o, 1 - self.odd, o).wait_recv()

    def several(self, count, sem):
        ref = self.buf.at[pl.ds(0, count), pl.ds(0, self.cut)]
        return remote(ref, ref, self.send.at[0], self.recv.at[sem], self.to)

    def drain(self):
        self.several(self.n - 1, 0).wait_send()


class Side:
    def __init__(self, own, slots, half, xs, xr, cs, cr):
        self.own, self.slots, self.half = own, slots, half
        self.xs, self.xr, self.cs, self.cr = xs, xr, cs, cr
        self.x = lax.axis_index("tp_0")
        self.c = lax.axis_index("tp_1")
        self.to = (
            {"tp_0": lax.rem(self.x + 1, NX)},
            {"tp_0": lax.rem(self.x + NX - 1, NX)},
        )
        self.other = {"tp_1": 1 - self.c}

    def spot(self, rel, h, core):
        slot = 2 * lax.rem(self.x + rel, NX) + core
        return self.slots.at[slot, pl.ds(h * self.half, self.half)]

    def source(self, rel, h):
        if rel == 0 and self.own is not None:
            return self.own.at[pl.ds(h * self.half, self.half)]
        return self.spot(rel, h, self.c)

    def half_of(self, d, k):
        return (0, 1, 0)[k] if d == 0 else (1, 0, 1)[k]

    def out(self, d, k):
        rel = 0 if k < 2 else (3 if d == 0 else 1)
        h = self.half_of(d, k)
        return remote(
            self.source(rel, h), self.spot(rel, h, self.c), self.xs.at[0], self.xr.at[k], self.to[d]
        )

    def inward(self, d, k):
        return (3 if d == 0 else 1) if k < 2 else 2, self.half_of(d, k)

    def blocks(self, count, send, recv, where):
        ref = self.slots.at[pl.ds(0, count)]
        return remote(ref, ref, send, recv, where)

    def across(self, rel, h):
        return remote(
            self.source(rel, h), self.spot(rel, h, self.c), self.cs.at[0], self.cr.at[0], self.other
        )

    def start(self):
        for k in (0, 1):
            for d in (0, 1):
                self.out(d, k).start()
        for h in (0, 1):
            self.across(0, h).start()

    def step(self, k):
        self.blocks(1, self.xs.at[0], self.xr.at[k], self.to[0]).wait_recv()
        for d in (0, 1):
            if k == 0:
                self.out(d, 2).start()
            self.across(*self.inward(d, k)).start()

    def finish(self):
        self.blocks(NX, self.cs.at[0], self.cr.at[0], self.other).wait_recv()

    def drain(self):
        self.blocks(NX - 1, self.xs.at[0], self.xr.at[0], self.to[0]).wait_send()
        self.blocks(NX, self.cs.at[0], self.cr.at[0], self.other).wait_send()


def side_sems():
    return [DMA((1,)), DMA((3,)), DMA((1,)), DMA((1,))]


def layer_kernel(
    n, heads_win, tok, gain, kd, vd, qd, qwd, kvw, pd, pw, lam, sink, ogain, out,
    w1, w2, raw, nbuf, acc1, acc2, kbuf, pdb, pwb, q, qw, kw, top, tot, acc, y, yd, yv, give, take, far, sums, facc,
    lsem, z1s, z1r, y1s, y1r, z2s, z2r, y2s, y2r, zks, zkr, hs, hr, us, ur, ts, tr, ws, wr, *sems,
):
    me, x, c = (lax.axis_index(a) for a in ("sp", "tp_0", "tp_1"))
    t = 2 * x + c
    block = raw.shape[1]
    rows = 2 * NX * block
    depth = w1.shape[1]
    part = kvw.shape[2] // 2
    head = t * heads_win // (WIN_HEADS // KV_HEADS)
    wq = qwd.shape[1]
    local = []
    at = 0
    for w in (kd, vd, qd):
        local.append((w, w1.at[me, :, pl.ds(at, w.shape[1])]))
        at += w.shape[1]
    local += [
        (qwd, w2.at[me, :, pl.ds(0, wq)]),
        (kvw.at[head, :, pl.ds(pl.multiple_of(c * part, part), part)], w2.at[me, :, pl.ds(wq, part)]),
        (tok, raw.at[t]),
        (pd, pdb.at[t]),
        (pw, pwb),
    ]
    local = [pltpu.make_async_copy(a, b, lsem.at[i]) for i, (a, b) in enumerate(local)]
    for copy in local:
        copy.start()

    swap1 = Swap(n, w1, CUT, y1s, y1r)
    swap2 = Swap(n, w2, depth // 2, y2s, y2r)
    ring1 = Ring(n, w1, swap1.base, (48, 48, 32, swap1.kept - 128), z1s, z1r)
    ring2 = Ring(n, w2, swap2.base, (depth // 4,) * 2, z2s, z2r)
    ring = Ring(n, kbuf, 0, (rows // 4,) * 4, zks, zkr)
    side = Side(None, raw, block // 2, *sems[:4])
    late = Side(None, pdb, depth // 2, *sems[4:])

    def peer(k):
        return {"tp_0": lax.rem(x + k // 2, NX), "tp_1": lax.rem(c + k % 2, 2)}

    greet([ring.to[0], ring.to[1], swap1.to] + [peer(k) for k in range(1, 2 * NX)])

    for copy in local[:3]:
        copy.wait()
    for k in range(4):
        ring1.start(0, k)
    local[5].wait()
    side.start()
    acc1[...] = jnp.zeros_like(acc1)
    acc2[...] = jnp.zeros_like(acc2)
    top[...] = jnp.full_like(top, -jnp.inf)
    tot[...] = jnp.zeros_like(tot)
    acc[...] = jnp.zeros_like(acc)
    for copy in local[3:5] + local[6:]:
        copy.wait()

    def normalise(quarter):
        tile = 32
        per = raw.shape[0] * block // tile // 4

        def one(j, carry):
            i = quarter * per + j
            slot, r = i // (block // tile), lax.rem(i, block // tile)
            v = raw[slot, pl.ds(pl.multiple_of(r * tile, tile), tile), :].astype(F32)
            v = v * lax.rsqrt(jnp.mean(v * v, axis=-1, keepdims=True) + EPS) * gain[...]
            v = v.astype(BF16)
            for o in range(n):
                nbuf[o, pl.ds(pl.multiple_of(i * tile, tile), tile), :] = v[:, o * depth : (o + 1) * depth]
            return carry

        lax.fori_loop(0, per, one, 0)

    def gather(w, swap, total, lo, hi):
        def one(j, carry):
            o = lax.rem(me + jnp.where(lax.rem(j, 2) == 1, (j + 1) // 2, n - j // 2), n)

            if swap is not None:

                @pl.when(j > 0)
                def _():
                    swap.land(o)

            total[...] += jnp.dot(nbuf[o], w[o], preferred_element_type=F32)
            return carry

        lax.fori_loop(lo, hi, one, 0)

    last = n // 2 - 1

    def swap_both(swap, ring_, hops):
        for d in (0, 1):
            swap.start(ring_.origin(d, hops))

    def swap_late(hops):
        for d in (0, 1):
            swap2.start(ring2.origin(d, hops), jnp.where(2 * hops - d < n // 2, 0, 1))

    def hop2(s, k):
        ring2.land(s, k)
        ring2.start(s + 1, k)

    def late_swaps(lo, hi):
        def one(h, carry):
            swap_late(h)
            return carry

        lax.fori_loop(lo, hi, one, 0)

    done = 9

    def phase1(s, carry):
        for k in range(4):
            ring1.land(s, k)
            ring1.start(s + 1, k)
            if k == 0:
                for i in range(3):

                    @pl.when(s == i + 1)
                    def _():
                        side.step(i)
                        if i == 2:
                            late.start()

                @pl.when(s == last - 3)
                def _():
                    side.finish()

            @pl.when(s == last - 3)
            def _():
                normalise(k)

            @pl.when(s == last - 2)
            def _():
                gather(w1, swap1, acc1, (0, 3, 6, 8)[k], (3, 6, 8, done)[k])

            if k % 2 == 1:

                @pl.when(s == last - 2)
                def _():
                    hop2(0, k // 2)

        swap_both(swap1, ring1, s + 1)

        @pl.when(s == last - 4)
        def _():
            for k in (0, 1):
                ring2.start(0, k)

        return carry

    lax.fori_loop(0, last - 1, phase1, 0)
    for k in range(4):
        ring1.land(last - 1, k)
        if k < 2:
            ring1.start(last, k)
        if k % 2 == 1:
            hop2(1, k // 2)
    swap_both(swap1, ring1, last)
    gather(w1, swap1, acc1, done, done + 2)
    for k in (0, 1):
        ring1.land(last, k)
    swap1.start(ring1.origin(0, last + 1))
    for s in (2, 3, 4):
        for k in (0, 1):
            hop2(s, k)
        if s == 2:
            late_swaps(1, s + 2)
        else:
            swap_late(s + 1)
        gather(w1, swap1, acc1, done + 2 * s - 2, min(done + 2 * s, n))
    kvd = kbuf.shape[2]
    kbuf[me] = acc1[:, :kvd].astype(BF16)
    q[...] = acc1[:, kvd:].astype(BF16)
    for k in range(4):
        ring.start(0, k)

    def edge(d, inward):
        src = pl.ds(rows, WINDOW) if d == 0 else pl.ds(WINDOW, WINDOW)
        dst = pl.ds(0, WINDOW) if d == 0 else pl.ds(rows + WINDOW, WINDOW)
        target = kw.at[c, dst]
        return remote(target if inward else kw.at[c, src], target, hs.at[d], hr.at[d], ring.to[d])

    spans = (pl.ds(WINDOW, rows), pl.ds(0, WINDOW), pl.ds(rows + WINDOW, WINDOW))

    def twin(i, inward):
        ref = kw.at[1 - c if inward else c, spans[i]]
        return remote(ref, ref, us.at[i], ur.at[i], side.other)

    def trade(k):
        src = y.at[2 * lax.rem(x + k // 2, NX) + lax.rem(c + k % 2, 2)]
        return remote(src, yd.at[t], ts.at[0], tr.at[min(k - 1, 1)], peer(k))

    def traded(count, sem):
        ref = yd.at[pl.ds(0, count)]
        return remote(ref, ref, ts.at[0], tr.at[sem], side.other)

    pass_on = remote(give, take, ws.at[0], wr.at[0], side.other)

    def relay(d, inward):
        src = far.at[d] if inward else take.at[lax.rem(x + 2, NX), pl.ds(d * (block // 2), block // 2)]
        return remote(src, far.at[d], ws.at[1 + d], wr.at[1 + d], side.to[d])

    def deal(d, inward):
        src = sums.at[d] if inward else take.at[lax.rem(x + (1, NX - 1)[d], NX)]
        return remote(src, sums.at[d], ws.at[3 + d], wr.at[3 + d], side.to[d])

    def merge():
        for d in (0, 1):
            relay(d, True).wait_recv()
            to = lax.rem(x + (1, NX - 1)[d], NX)
            half = pl.ds(d * (block // 2), block // 2)
            take[to, half, :] = (take[to, half, :].astype(F32) + far[d].astype(F32)).astype(BF16)
        for d in (0, 1):
            deal(d, False).start()

    scale = HEAD**-0.5
    lanes = HEAD
    contract_last = (((1,), (1,)), ((), ()))

    def attend(o):
        def one(m, carry):
            cols = pl.ds(pl.multiple_of(m * HEAD, HEAD), HEAD)
            s = lax.dot_general(q[:, cols], kbuf[o, :, cols], contract_last, preferred_element_type=F32)
            s = s * (scale * LOG2E)
            reps = s.shape[1] // lanes
            was = top[m]
            now = jnp.maximum(was, jnp.max(s, axis=1, keepdims=True))
            fade = jnp.exp2(was - now)
            e = jnp.exp2(s - jnp.concatenate([now] * reps, axis=1))
            some = e[:, :lanes]
            for j in range(1, reps):
                some = some + e[:, j * lanes : (j + 1) * lanes]
            tot[m] = tot[m] * fade + some
            top[m] = now
            acc[m] = acc[m] * jnp.concatenate([fade] * (VDIM // lanes), axis=1) + jnp.dot(
                e.astype(BF16), kbuf[o, :, 2 * HEAD :], preferred_element_type=F32
            )
            return carry

        for m in range(2):
            one(m, 0)

    def window(lo, hi, stride):
        span = 3 * WINDOW
        heads = wq // HEAD
        i_q = lax.broadcasted_iota(jnp.int32, (WINDOW, span), 0)
        i_k = lax.broadcasted_iota(jnp.int32, (WINDOW, span), 1)
        near = jnp.abs(i_k - WINDOW - i_q) <= WINDOW

        def one(i, carry):
            b = i * stride
            r = pl.ds(pl.multiple_of(b * WINDOW, WINDOW), WINDOW)
            band = pl.ds(pl.multiple_of(b * WINDOW, WINDOW), span)
            where = i_k + (me * rows + b * WINDOW - WINDOW)
            valid = near & (where >= 0) & (where < n * rows)
            for h in range(heads):
                cols = pl.ds(h * HEAD, HEAD)
                s = lax.dot_general(qw[r, cols], kw[0, band, :], contract_last, preferred_element_type=F32)
                s = jnp.where(valid, s * scale, -jnp.inf)
                sunk = jnp.full((WINDOW, lanes), sink[h], F32)
                peak = jnp.maximum(jnp.max(s, axis=1, keepdims=True), sunk)
                e = jnp.exp(s - jnp.concatenate([peak] * 3, axis=1))
                whole = jnp.sum(e, axis=1, keepdims=True) + jnp.exp(sunk - peak)
                w = (e / jnp.concatenate([whole] * 3, axis=1)).astype(BF16)
                res = jnp.dot(w, kw[1, band, :], preferred_element_type=F32).astype(BF16)
                for j in range(WINDOW // block):
                    yv[j % 2, b * (WINDOW // block // 2) + j // 2, :, cols] = res[j * block : (j + 1) * block]
            return carry

        lax.fori_loop(lo, hi, one, 0)

    width = 512

    def columns(one):
        def run(j, carry):
            one(pl.ds(pl.multiple_of(j * width, width), width))
            return carry

        lax.fori_loop(0, out.shape[1] // width, run, 0)

    def window_rows(core, cols):
        ys = yv[core].reshape(NX * block, wq)
        return jnp.dot(ys, pwb[:, cols], preferred_element_type=F32).reshape(NX, block, width)

    def to_give(cols):
        give[:, :, cols] = window_rows(1 - c, cols).astype(BF16)

    def to_sum(cols):
        take[:, :, cols] = (window_rows(c, cols) + take[:, :, cols].astype(F32)).astype(BF16)

    attend(me)

    def side_work(s, k):
        def at(when):
            return pl.when(s == when)

        if k == 0:

            @at(0)
            def _():
                for i in (0, 1):
                    hop2(last - 2, i)
                swap_late(last - 1)

            @at(1)
            def _():
                ring2.land(last - 1, 0)
                ring2.start(last, 0)
                ring2.land(last - 1, 1)
                swap_late(last)

            @at(4)
            def _():
                late.step(2)

        if k == 1:

            @at(1)
            def _():
                late.step(1)

            @at(3)
            def _():
                swap2.several(n // 2, 1).wait_recv()
                gather(w2, None, acc2, n // 2, n)
                kw[c, spans[0]] = acc2[:, wq:].astype(BF16)
                qw[...] = acc2[:, :wq].astype(BF16)
                for d in (0, 1):
                    edge(d, False).start()
                twin(0, False).start()

            @at(4)
            def _():
                for d in (0, 1):
                    edge(d, True).wait_recv()
                    twin(d + 1, False).start()

            @at(5)
            def _():
                pass_on.wait_recv()
                columns(to_sum)
                for d in (0, 1):
                    relay(d, False).start()

        if k == 2:

            @at(0)
            def _():
                late.step(0)

            @at(1)
            def _():
                ring2.land(last, 0)
                swap2.start(ring2.origin(0, last + 1), 1)

            @at(2)
            def _():
                swap2.several(n // 2 - 1, 0).wait_recv()
                gather(w2, None, acc2, 0, n // 2)

            @at(3)
            def _():
                twin(0, True).wait_recv()
                window(1, rows // WINDOW - 1, 1)

            @at(4)
            def _():
                for i in (1, 2):
                    twin(i, True).wait_recv()
                window(0, 2, rows // WINDOW - 1)

        if k == 3:

            @at(4)
            def _():
                columns(to_give)
                pass_on.start()

    def phase2(s, carry):
        for k in range(4):
            ring.land(s, k)
            ring.start(s + 1, k)
            side_work(s, k)
            if k % 2 == 1:

                @pl.when(s > 0)
                def _():
                    attend(ring.origin(k // 2, s))

        return carry

    lax.fori_loop(0, last - 1, phase2, 0)
    for k in range(4):
        ring.land(last - 1, k)
        if k < 2:
            ring.start(last, k)
        if k == 1:
            merge()
        if k % 2 == 1:
            attend(ring.origin(k // 2, last - 1))
    late.finish()
    for r in (ring1, ring2, swap1, swap2, side, late):
        r.drain()
    for d in (0, 1):
        edge(d, False).wait_send()
    for i in range(3):
        twin(i, False).wait_send()
    pass_on.wait_send()

    def both(i, carry):
        attend(lax.rem(me + n - last + 2 * last * i, n))
        return carry

    lax.fori_loop(0, 2, both, 0)
    for k in (0, 1):
        ring.land(last, k)
    attend(lax.rem(me + last + 1, n))

    def close(j):
        r = pl.ds(pl.multiple_of(j * block, block), block)
        parts = [1.0 / jnp.sum(tot[m, r, :], axis=1, keepdims=True) for m in range(2)]
        d = acc[0, r, :] * parts[0] - acc[1, r, :] * (lam[0] * parts[1])
        d = d * lax.rsqrt(jnp.mean(d * d, axis=-1, keepdims=True) + EPS) * ogain[...]
        return d.astype(BF16)

    for k in (4, 5, 2, 6, 3, 7, 1):
        j = 2 * lax.rem(x + k // 2, NX) + lax.rem(c + k % 2, 2)
        y[j] = close(j)
        trade(k).start()
    yd[t] = close(t)
    wide = 1024

    def add(total, away, cols):
        first = 2 * lax.rem(x + NX - away, NX)
        for h in (0, 1):
            total = total + jnp.dot(yd[first + h], pdb[first + h, :, cols], preferred_element_type=F32)
        return total

    def begin(j, carry):
        cols = pl.ds(pl.multiple_of(j * wide, wide), wide)
        total = take[x, :, cols].astype(F32)
        for d in (0, 1):
            total = total + sums[d, :, cols].astype(F32)
        facc[:, cols] = add(total, 0, cols)
        return carry

    def finish(j, carry):
        cols = pl.ds(pl.multiple_of(j * wide, wide), wide)
        total = facc[:, cols]
        for away in (1, 3, 2):
            total = add(total, away, cols)
        out[:, cols] = total.astype(out.dtype)
        return carry

    for d in (0, 1):
        deal(d, True).wait_recv()
    traded(1, 0).wait_recv()
    lax.fori_loop(0, out.shape[1] // wide, begin, 0)
    traded(2 * NX - 2, 1).wait_recv()
    lax.fori_loop(0, out.shape[1] // wide, finish, 0)
    traded(2 * NX - 1, 0).wait_send()
    for d in (0, 1):
        relay(d, False).wait_send()
        deal(d, False).wait_send()
    ring.drain()


def body(
    n, tokens, norm_gain, query_diff, key_diff, value_diff, lam, output_norm_gain,
    query_win, keyval_win, sink, proj_diff, proj_win,
):
    block, model = tokens.shape
    rows = block * 2 * NX
    depth, wq = query_win.shape
    kvd = key_diff.shape[1] + value_diff.shape[1]
    dq = query_diff.shape[1]
    part = keyval_win.shape[2] // 2
    hops = n // 2

    def pair(*shape):
        return [DMA(shape), DMA(shape)]

    return pl.pallas_call(
        functools.partial(layer_kernel, n, sink.shape[0]),
        out_shape=jax.ShapeDtypeStruct((block, model), BF16),
        in_specs=[
            pl.BlockSpec(memory_space=m)
            for m in [ANY, VMEM] + [ANY] * 7 + [pltpu.SMEM, pltpu.SMEM, VMEM]
        ],
        out_specs=pl.BlockSpec(memory_space=VMEM),
        scratch_shapes=[
            VMEM((n, depth, kvd + dq), BF16),
            VMEM((n, depth, wq + part), BF16),
            VMEM((2 * NX, block, model), BF16),
            VMEM((n, rows, depth), BF16),
            VMEM((rows, kvd + dq), F32),
            VMEM((rows, wq + part), F32),
            VMEM((n, rows, kvd), BF16),
            VMEM((2 * NX,) + proj_diff.shape, BF16),
            VMEM(proj_win.shape, BF16),
            VMEM((rows, dq), BF16),
            VMEM((rows, wq), BF16),
            VMEM((2, rows + 2 * WINDOW, part), BF16),
            VMEM((2, rows, HEAD), F32),
            VMEM((2, rows, HEAD), F32),
            VMEM((2, rows, VDIM), F32),
            VMEM((2 * NX, block, VDIM), BF16),
            VMEM((2 * NX, block, VDIM), BF16),
            VMEM((2, NX, block, wq), BF16),
            VMEM((NX, block, model), BF16),
            VMEM((NX, block, model), BF16),
            VMEM((2, block // 2, model), BF16),
            VMEM((2, block, model), BF16),
            VMEM((block, model), F32),
            DMA((8,)),
        ]
        + [DMA((1,)), DMA((hops, 4)), DMA((1,)), DMA((n,))]
        + [DMA((1,)), DMA((hops, 2)), DMA((1,)), DMA((2,))]
        + [DMA((1,)), DMA((hops, 4))]
        + pair(2)
        + pair(3)
        + [DMA((1,)), DMA((2,))]
        + pair(5)
        + side_sems()
        + side_sems(),
        compiler_params=pltpu.CompilerParams(
            collective_id=0, has_side_effects=True, vmem_limit_bytes=67_000_000
        ),
    )(
        tokens, norm_gain.reshape(1, model), key_diff, value_diff, query_diff, query_win, keyval_win,
        proj_diff, proj_win, lam, sink, output_norm_gain.reshape(1, VDIM),
    )


def solution(mesh):
    torus = Mesh(
        mesh.devices.reshape(mesh.shape["grp"], mesh.shape["sp"], NX, 2),
        ("grp", "sp", "tp_0", "tp_1"),
    )
    return jax.shard_map(
        functools.partial(body, mesh.shape["sp"]),
        mesh=torus,
        in_specs=(
            P(GRP_SP_TP, None),
            P(),
            P("sp", TP),
            P("sp", TP),
            P("sp", TP),
            P(TP),
            P(),
            P("sp", TP),
            P(None, "sp", None),
            P(TP),
            P(TP, None),
            P(TP, None),
        ),
        out_specs=P(GRP_SP_TP, None),
        check_vma=False,
    )
```

```python
import functools

import jax
import jax.numpy as jnp
from jax import lax
from jax.experimental import pallas as pl
from jax.experimental.pallas import tpu as pltpu
from jax.sharding import Mesh
from jax.sharding import PartitionSpec as P

HEAD = 128
WIN_HEADS = 16
KV_HEADS = 4
WINDOW = 128
VDIM = 256
NX = 4
CUT = 96
TP = ("tp_0", "tp_1")
GRP_SP_TP = ("grp", "sp", "tp_0", "tp_1")
EPS = 1e-06
LOG2E = 1.4426950408889634
BF16 = jnp.bfloat16
F32 = jnp.float32
MESH = pl.DeviceIdType.MESH
DMA = pltpu.SemaphoreType.DMA
VMEM = pltpu.VMEM
ANY = pl.ANY


def remote(src, dst, send_sem, recv_sem, where):
    return pltpu.make_async_remote_copy(
        src_ref=src,
        dst_ref=dst,
        send_sem=send_sem,
        recv_sem=recv_sem,
        device_id=where,
        device_id_type=MESH,
    )


def greet(peers):
    barrier = pltpu.get_barrier_semaphore()
    for peer in peers:
        pl.semaphore_signal(barrier, inc=1, device_id=peer, device_id_type=MESH)
    pl.semaphore_wait(barrier, len(peers))


class Ring:
    def __init__(self, n, buf, base, cuts, send, recv):
        self.n, self.buf, self.send, self.recv = n, buf, send, recv
        self.base, self.cuts = base, cuts
        self.spans = []
        for cut in cuts:
            self.spans.append(pl.ds(base, cut))
            base = base + cut
        self.count = len(cuts)
        self.me = lax.axis_index("sp")
        self.to = (
            {"sp": lax.rem(self.me + 1, n)},
            {"sp": lax.rem(self.me + n - 1, n)},
        )

    def origin(self, d, s):
        return lax.rem(self.me + (self.n - s if d == 0 else s), self.n)

    def piece(self, d, s, k, hops):
        ref = self.buf.at[self.origin(d, hops), self.spans[k if d == 0 else self.count - 1 - k]]
        return remote(ref, ref, self.send.at[0], self.recv.at[s, k], self.to[d])

    def start(self, s, k):
        for d in (0, 1):
            self.piece(d, s, k, s).start()

    def land(self, s, k):
        both = pl.ds(self.base, self.cuts[k] + self.cuts[self.count - 1 - k])
        ref = self.buf.at[self.me, both]
        remote(ref, ref, self.send.at[0], self.recv.at[s, k], self.to[0]).wait_recv()

    def drain(self):
        ref = self.buf.at[pl.ds(0, self.n - 1), pl.ds(self.base, sum(self.cuts))]
        remote(ref, ref, self.send.at[0], self.recv.at[0, 0], self.to[0]).wait_send()


class Swap:
    def __init__(self, n, buf, cut, send, recv):
        self.n, self.buf, self.cut, self.send, self.recv = n, buf, cut, send, recv
        g = lax.axis_index("grp")
        self.odd = lax.rem(g, 2)
        self.to = {"grp": g + 1 - 2 * self.odd}
        self.kept = buf.shape[1] - cut
        self.base = pl.multiple_of(self.odd * cut, 16)

    def piece(self, o, odd, sem):
        ref = self.buf.at[o, pl.ds(pl.multiple_of(odd * self.kept, 16), self.cut)]
        return remote(ref, ref, self.send.at[0], self.recv.at[sem], self.to)

    def start(self, o, sem=None):
        self.piece(o, self.odd, o if sem is None else sem).start()

    def land(self, o):
        self.piece(o, 1 - self.odd, o).wait_recv()

    def several(self, count, sem):
        ref = self.buf.at[pl.ds(0, count), pl.ds(0, self.cut)]
        return remote(ref, ref, self.send.at[0], self.recv.at[sem], self.to)

    def drain(self):
        self.several(self.n - 1, 0).wait_send()


class Side:
    def __init__(self, own, slots, half, xs, xr, cs, cr):
        self.own, self.slots, self.half = own, slots, half
        self.xs, self.xr, self.cs, self.cr = xs, xr, cs, cr
        self.x = lax.axis_index("tp_0")
        self.c = lax.axis_index("tp_1")
        self.to = (
            {"tp_0": lax.rem(self.x + 1, NX)},
            {"tp_0": lax.rem(self.x + NX - 1, NX)},
        )
        self.other = {"tp_1": 1 - self.c}

    def spot(self, rel, h, core):
        slot = 2 * lax.rem(self.x + rel, NX) + core
        return self.slots.at[slot, pl.ds(h * self.half, self.half)]

    def source(self, rel, h):
        if rel == 0 and self.own is not None:
            return self.own.at[pl.ds(h * self.half, self.half)]
        return self.spot(rel, h, self.c)

    def half_of(self, d, k):
        return (0, 1, 0)[k] if d == 0 else (1, 0, 1)[k]

    def out(self, d, k):
        rel = 0 if k < 2 else (3 if d == 0 else 1)
        h = self.half_of(d, k)
        return remote(
            self.source(rel, h), self.spot(rel, h, self.c), self.xs.at[0], self.xr.at[k], self.to[d]
        )

    def inward(self, d, k):
        return (3 if d == 0 else 1) if k < 2 else 2, self.half_of(d, k)

    def blocks(self, count, send, recv, where):
        ref = self.slots.at[pl.ds(0, count)]
        return remote(ref, ref, send, recv, where)

    def across(self, rel, h):
        return remote(
            self.source(rel, h), self.spot(rel, h, self.c), self.cs.at[0], self.cr.at[0], self.other
        )

    def start(self):
        for k in (0, 1):
            for d in (0, 1):
                self.out(d, k).start()
        for h in (0, 1):
            self.across(0, h).start()

    def step(self, k):
        self.blocks(1, self.xs.at[0], self.xr.at[k], self.to[0]).wait_recv()
        for d in (0, 1):
            if k == 0:
                self.out(d, 2).start()
            self.across(*self.inward(d, k)).start()

    def finish(self):
        self.blocks(NX, self.cs.at[0], self.cr.at[0], self.other).wait_recv()

    def drain(self):
        self.blocks(NX - 1, self.xs.at[0], self.xr.at[0], self.to[0]).wait_send()
        self.blocks(NX, self.cs.at[0], self.cr.at[0], self.other).wait_send()


def side_sems():
    return [DMA((1,)), DMA((3,)), DMA((1,)), DMA((1,))]


def layer_kernel(
    n, heads_win, tok, gain, kd, vd, qd, qwd, kvw, pd, pw, lam, sink, ogain, out,
    w1, w2, raw, nbuf, acc1, acc2, kbuf, pdb, pwb, q, qw, kw, top, tot, acc, y, yd, yv, give, take, far, sums, facc,
    lsem, z1s, z1r, y1s, y1r, z2s, z2r, y2s, y2r, zks, zkr, hs, hr, us, ur, ts, tr, ws, wr, *sems,
):
    me, x, c = (lax.axis_index(a) for a in ("sp", "tp_0", "tp_1"))
    t = 2 * x + c
    block = raw.shape[1]
    rows = 2 * NX * block
    depth = w1.shape[1]
    part = kvw.shape[2] // 2
    head = t * heads_win // (WIN_HEADS // KV_HEADS)
    wq = qwd.shape[1]
    local = []
    at = 0
    for w in (kd, vd, qd):
        local.append((w, w1.at[me, :, pl.ds(at, w.shape[1])]))
        at += w.shape[1]
    local += [
        (qwd, w2.at[me, :, pl.ds(0, wq)]),
        (kvw.at[head, :, pl.ds(pl.multiple_of(c * part, part), part)], w2.at[me, :, pl.ds(wq, part)]),
        (tok, raw.at[t]),
        (pd, pdb.at[t]),
        (pw, pwb),
    ]
    local = [pltpu.make_async_copy(a, b, lsem.at[i]) for i, (a, b) in enumerate(local)]
    for copy in local:
        copy.start()

    swap1 = Swap(n, w1, CUT, y1s, y1r)
    swap2 = Swap(n, w2, depth // 2, y2s, y2r)
    ring1 = Ring(n, w1, swap1.base, (48, 32, 32, swap1.kept - 112), z1s, z1r)
    ring2 = Ring(n, w2, swap2.base, (depth // 4,) * 2, z2s, z2r)
    ring = Ring(n, kbuf, 0, (rows // 4,) * 4, zks, zkr)
    side = Side(None, raw, block // 2, *sems[:4])
    late = Side(None, pdb, depth // 2, *sems[4:])

    def peer(k):
        return {"tp_0": lax.rem(x + k // 2, NX), "tp_1": lax.rem(c + k % 2, 2)}

    greet([ring.to[0], ring.to[1], swap1.to] + [peer(k) for k in range(1, 2 * NX)])

    for copy in local[:3]:
        copy.wait()
    for k in range(4):
        ring1.start(0, k)
    local[5].wait()
    side.start()
    acc1[...] = jnp.zeros_like(acc1)
    acc2[...] = jnp.zeros_like(acc2)
    top[...] = jnp.full_like(top, -jnp.inf)
    tot[...] = jnp.zeros_like(tot)
    acc[...] = jnp.zeros_like(acc)
    for copy in local[3:5] + local[6:]:
        copy.wait()

    def normalise(quarter):
        tile = 32
        per = raw.shape[0] * block // tile // 4

        def one(j, carry):
            i = quarter * per + j
            slot, r = i // (block // tile), lax.rem(i, block // tile)
            v = raw[slot, pl.ds(pl.multiple_of(r * tile, tile), tile), :].astype(F32)
            v = v * lax.rsqrt(jnp.mean(v * v, axis=-1, keepdims=True) + EPS) * gain[...]
            v = v.astype(BF16)
            for o in range(n):
                nbuf[o, pl.ds(pl.multiple_of(i * tile, tile), tile), :] = v[:, o * depth : (o + 1) * depth]
            return carry

        lax.fori_loop(0, per, one, 0)

    def gather(w, swap, total, lo, hi):
        def one(j, carry):
            o = lax.rem(me + jnp.where(lax.rem(j, 2) == 1, (j + 1) // 2, n - j // 2), n)

            if swap is not None:

                @pl.when(j > 0)
                def _():
                    swap.land(o)

            total[...] += jnp.dot(nbuf[o], w[o], preferred_element_type=F32)
            return carry

        lax.fori_loop(lo, hi, one, 0)

    last = n // 2 - 1

    def swap_both(swap, ring_, hops):
        for d in (0, 1):
            swap.start(ring_.origin(d, hops))

    def swap_late(hops):
        for d in (0, 1):
            swap2.start(ring2.origin(d, hops), jnp.where(2 * hops - d < n // 2, 0, 1))

    def hop2(s, k):
        ring2.land(s, k)
        ring2.start(s + 1, k)

    def late_swaps(lo, hi):
        def one(h, carry):
            swap_late(h)
            return carry

        lax.fori_loop(lo, hi, one, 0)

    done = 2 * last - 3

    def phase1(s, carry):
        for k in range(4):
            ring1.land(s, k)
            ring1.start(s + 1, k)
            if k == 0:
                for i in range(3):

                    @pl.when(s == i + 1)
                    def _():
                        side.step(i)
                        if i == 2:
                            late.start()

                @pl.when(s == last - 3)
                def _():
                    side.finish()

            @pl.when(s == last - 3)
            def _():
                normalise(k)

            @pl.when(s == last - 2)
            def _():
                gather(w1, swap1, acc1, 3 * k, min(3 * k + 3, done))

            if k % 2 == 1:

                @pl.when(s >= 3)
                def _():
                    hop2(s - 3, k // 2)

        swap_both(swap1, ring1, s + 1)

        @pl.when(s == 1)
        def _():
            for k in (0, 1):
                ring2.start(0, k)

        return carry

    lax.fori_loop(0, last - 1, phase1, 0)
    for k in range(4):
        ring1.land(last - 1, k)
        if k < 2:
            ring1.start(last, k)
        if k % 2 == 1:
            hop2(last - 4, k // 2)
    swap_both(swap1, ring1, last)
    for k in (0, 1):
        ring1.land(last, k)
    swap1.start(ring1.origin(0, last + 1))
    for k in (0, 1):
        hop2(last - 3, k)
    late_swaps(1, last - 1)
    gather(w1, swap1, acc1, done, done + 2)
    for k in (0, 1):
        hop2(last - 2, k)
    swap_late(last - 1)
    gather(w1, swap1, acc1, done + 2, n)
    kvd = kbuf.shape[2]
    kbuf[me] = acc1[:, :kvd].astype(BF16)
    q[...] = acc1[:, kvd:].astype(BF16)
    for k in range(4):
        ring.start(0, k)

    def edge(d, inward):
        src = pl.ds(rows, WINDOW) if d == 0 else pl.ds(WINDOW, WINDOW)
        dst = pl.ds(0, WINDOW) if d == 0 else pl.ds(rows + WINDOW, WINDOW)
        target = kw.at[c, dst]
        return remote(target if inward else kw.at[c, src], target, hs.at[d], hr.at[d], ring.to[d])

    spans = (pl.ds(WINDOW, rows), pl.ds(0, WINDOW), pl.ds(rows + WINDOW, WINDOW))

    def twin(i, inward):
        ref = kw.at[1 - c if inward else c, spans[i]]
        return remote(ref, ref, us.at[i], ur.at[i], side.other)

    def trade(k):
        src = y.at[2 * lax.rem(x + k // 2, NX) + lax.rem(c + k % 2, 2)]
        return remote(src, yd.at[t], ts.at[0], tr.at[min(k - 1, 1)], peer(k))

    def traded(count, sem):
        ref = yd.at[pl.ds(0, count)]
        return remote(ref, ref, ts.at[0], tr.at[sem], side.other)

    pass_on = remote(give, take, ws.at[0], wr.at[0], side.other)

    def relay(d, inward):
        src = far.at[d] if inward else take.at[lax.rem(x + 2, NX), pl.ds(d * (block // 2), block // 2)]
        return remote(src, far.at[d], ws.at[1 + d], wr.at[1 + d], side.to[d])

    def deal(d, inward):
        src = sums.at[d] if inward else take.at[lax.rem(x + (1, NX - 1)[d], NX)]
        return remote(src, sums.at[d], ws.at[3 + d], wr.at[3 + d], side.to[d])

    def merge():
        for d in (0, 1):
            relay(d, True).wait_recv()
            to = lax.rem(x + (1, NX - 1)[d], NX)
            half = pl.ds(d * (block // 2), block // 2)
            take[to, half, :] = (take[to, half, :].astype(F32) + far[d].astype(F32)).astype(BF16)
        for d in (0, 1):
            deal(d, False).start()

    scale = HEAD**-0.5
    lanes = HEAD
    contract_last = (((1,), (1,)), ((), ()))

    def attend(o):
        def one(m, carry):
            cols = pl.ds(pl.multiple_of(m * HEAD, HEAD), HEAD)
            s = lax.dot_general(q[:, cols], kbuf[o, :, cols], contract_last, preferred_element_type=F32)
            s = s * (scale * LOG2E)
            reps = s.shape[1] // lanes
            was = top[m]
            now = jnp.maximum(was, jnp.max(s, axis=1, keepdims=True))
            fade = jnp.exp2(was - now)
            e = jnp.exp2(s - jnp.concatenate([now] * reps, axis=1))
            some = e[:, :lanes]
            for j in range(1, reps):
                some = some + e[:, j * lanes : (j + 1) * lanes]
            tot[m] = tot[m] * fade + some
            top[m] = now
            acc[m] = acc[m] * jnp.concatenate([fade] * (VDIM // lanes), axis=1) + jnp.dot(
                e.astype(BF16), kbuf[o, :, 2 * HEAD :], preferred_element_type=F32
            )
            return carry

        for m in range(2):
            one(m, 0)

    def window(lo, hi, stride):
        span = 3 * WINDOW
        heads = wq // HEAD
        i_q = lax.broadcasted_iota(jnp.int32, (WINDOW, span), 0)
        i_k = lax.broadcasted_iota(jnp.int32, (WINDOW, span), 1)
        near = jnp.abs(i_k - WINDOW - i_q) <= WINDOW

        def one(i, carry):
            b = i * stride
            r = pl.ds(pl.multiple_of(b * WINDOW, WINDOW), WINDOW)
            band = pl.ds(pl.multiple_of(b * WINDOW, WINDOW), span)
            where = i_k + (me * rows + b * WINDOW - WINDOW)
            valid = near & (where >= 0) & (where < n * rows)
            for h in range(heads):
                cols = pl.ds(h * HEAD, HEAD)
                s = lax.dot_general(qw[r, cols], kw[0, band, :], contract_last, preferred_element_type=F32)
                s = jnp.where(valid, s * scale, -jnp.inf)
                sunk = jnp.full((WINDOW, lanes), sink[h], F32)
                peak = jnp.maximum(jnp.max(s, axis=1, keepdims=True), sunk)
                e = jnp.exp(s - jnp.concatenate([peak] * 3, axis=1))
                whole = jnp.sum(e, axis=1, keepdims=True) + jnp.exp(sunk - peak)
                w = (e / jnp.concatenate([whole] * 3, axis=1)).astype(BF16)
                res = jnp.dot(w, kw[1, band, :], preferred_element_type=F32).astype(BF16)
                for j in range(WINDOW // block):
                    yv[j % 2, b * (WINDOW // block // 2) + j // 2, :, cols] = res[j * block : (j + 1) * block]
            return carry

        lax.fori_loop(lo, hi, one, 0)

    width = 512

    def columns(one):
        def run(j, carry):
            one(pl.ds(pl.multiple_of(j * width, width), width))
            return carry

        lax.fori_loop(0, out.shape[1] // width, run, 0)

    def window_rows(core, cols):
        ys = yv[core].reshape(NX * block, wq)
        return jnp.dot(ys, pwb[:, cols], preferred_element_type=F32).reshape(NX, block, width)

    def to_give(cols):
        give[:, :, cols] = window_rows(1 - c, cols).astype(BF16)

    def to_sum(cols):
        take[:, :, cols] = (window_rows(c, cols) + take[:, :, cols].astype(F32)).astype(BF16)

    attend(me)

    def side_work(s, k):
        def at(when):
            return pl.when(s == when)

        if k == 0:

            @at(0)
            def _():
                ring2.land(last - 1, 0)
                ring2.start(last, 0)
                ring2.land(last - 1, 1)
                swap_late(last)

            @at(1)
            def _():
                ring2.land(last, 0)
                swap2.start(ring2.origin(0, last + 1), 1)

            @at(4)
            def _():
                for i in (1, 2):
                    twin(i, True).wait_recv()
                window(0, 2, rows // WINDOW - 1)

        if k == 1:

            @at(1)
            def _():
                late.step(1)

            @at(2)
            def _():
                swap2.several(n // 2 - 1, 0).wait_recv()
                gather(w2, None, acc2, 0, n // 2)

            @at(3)
            def _():
                twin(0, True).wait_recv()
                window(1, rows // WINDOW - 1, 1)

            @at(4)
            def _():
                columns(to_give)
                pass_on.start()

        if k == 2:

            @at(0)
            def _():
                late.step(0)

        if k == 3:

            @at(2)
            def _():
                swap2.several(n // 2, 1).wait_recv()
                gather(w2, None, acc2, n // 2, n)
                kw[c, spans[0]] = acc2[:, wq:].astype(BF16)
                qw[...] = acc2[:, :wq].astype(BF16)
                for d in (0, 1):
                    edge(d, False).start()
                twin(0, False).start()

            @at(3)
            def _():
                for d in (0, 1):
                    edge(d, True).wait_recv()
                    twin(d + 1, False).start()
                late.step(2)

            @at(4)
            def _():
                pass_on.wait_recv()
                columns(to_sum)
                for d in (0, 1):
                    relay(d, False).start()

            @at(5)
            def _():
                merge()

    def phase2(s, carry):
        for k in range(4):
            ring.land(s, k)
            ring.start(s + 1, k)
            side_work(s, k)
            if k % 2 == 1:

                @pl.when(s > 0)
                def _():
                    attend(ring.origin(k // 2, s))

        return carry

    lax.fori_loop(0, last - 1, phase2, 0)
    for k in range(4):
        ring.land(last - 1, k)
        if k < 2:
            ring.start(last, k)
        if k % 2 == 1:
            attend(ring.origin(k // 2, last - 1))
    late.finish()
    for r in (ring1, ring2, swap1, swap2, side, late):
        r.drain()
    for d in (0, 1):
        edge(d, False).wait_send()
    for i in range(3):
        twin(i, False).wait_send()
    pass_on.wait_send()

    def both(i, carry):
        attend(lax.rem(me + n - last + 2 * last * i, n))
        return carry

    lax.fori_loop(0, 2, both, 0)
    for k in (0, 1):
        ring.land(last, k)
    attend(lax.rem(me + last + 1, n))

    def close(j):
        r = pl.ds(pl.multiple_of(j * block, block), block)
        parts = [1.0 / jnp.sum(tot[m, r, :], axis=1, keepdims=True) for m in range(2)]
        d = acc[0, r, :] * parts[0] - acc[1, r, :] * (lam[0] * parts[1])
        d = d * lax.rsqrt(jnp.mean(d * d, axis=-1, keepdims=True) + EPS) * ogain[...]
        return d.astype(BF16)

    for k in (4, 5, 2, 6, 3, 7, 1):
        j = 2 * lax.rem(x + k // 2, NX) + lax.rem(c + k % 2, 2)
        y[j] = close(j)
        trade(k).start()
    yd[t] = close(t)
    wide = 1024

    def add(total, away, cols):
        first = 2 * lax.rem(x + NX - away, NX)
        for h in (0, 1):
            total = total + jnp.dot(yd[first + h], pdb[first + h, :, cols], preferred_element_type=F32)
        return total

    def begin(j, carry):
        cols = pl.ds(pl.multiple_of(j * wide, wide), wide)
        total = take[x, :, cols].astype(F32)
        for d in (0, 1):
            total = total + sums[d, :, cols].astype(F32)
        facc[:, cols] = add(total, 0, cols)
        return carry

    def finish(j, carry):
        cols = pl.ds(pl.multiple_of(j * wide, wide), wide)
        total = facc[:, cols]
        for away in (1, 3, 2):
            total = add(total, away, cols)
        out[:, cols] = total.astype(out.dtype)
        return carry

    for d in (0, 1):
        deal(d, True).wait_recv()
    traded(1, 0).wait_recv()
    lax.fori_loop(0, out.shape[1] // wide, begin, 0)
    traded(2 * NX - 2, 1).wait_recv()
    lax.fori_loop(0, out.shape[1] // wide, finish, 0)
    traded(2 * NX - 1, 0).wait_send()
    for d in (0, 1):
        relay(d, False).wait_send()
        deal(d, False).wait_send()
    ring.drain()


def body(
    n, tokens, norm_gain, query_diff, key_diff, value_diff, lam, output_norm_gain,
    query_win, keyval_win, sink, proj_diff, proj_win,
):
    block, model = tokens.shape
    rows = block * 2 * NX
    depth, wq = query_win.shape
    kvd = key_diff.shape[1] + value_diff.shape[1]
    dq = query_diff.shape[1]
    part = keyval_win.shape[2] // 2
    hops = n // 2

    def pair(*shape):
        return [DMA(shape), DMA(shape)]

    return pl.pallas_call(
        functools.partial(layer_kernel, n, sink.shape[0]),
        out_shape=jax.ShapeDtypeStruct((block, model), BF16),
        in_specs=[
            pl.BlockSpec(memory_space=m)
            for m in [ANY, VMEM] + [ANY] * 7 + [pltpu.SMEM, pltpu.SMEM, VMEM]
        ],
        out_specs=pl.BlockSpec(memory_space=VMEM),
        scratch_shapes=[
            VMEM((n, depth, kvd + dq), BF16),
            VMEM((n, depth, wq + part), BF16),
            VMEM((2 * NX, block, model), BF16),
            VMEM((n, rows, depth), BF16),
            VMEM((rows, kvd + dq), F32),
            VMEM((rows, wq + part), F32),
            VMEM((n, rows, kvd), BF16),
            VMEM((2 * NX,) + proj_diff.shape, BF16),
            VMEM(proj_win.shape, BF16),
            VMEM((rows, dq), BF16),
            VMEM((rows, wq), BF16),
            VMEM((2, rows + 2 * WINDOW, part), BF16),
            VMEM((2, rows, HEAD), F32),
            VMEM((2, rows, HEAD), F32),
            VMEM((2, rows, VDIM), F32),
            VMEM((2 * NX, block, VDIM), BF16),
            VMEM((2 * NX, block, VDIM), BF16),
            VMEM((2, NX, block, wq), BF16),
            VMEM((NX, block, model), BF16),
            VMEM((NX, block, model), BF16),
            VMEM((2, block // 2, model), BF16),
            VMEM((2, block, model), BF16),
            VMEM((block, model), F32),
            DMA((8,)),
        ]
        + [DMA((1,)), DMA((hops, 4)), DMA((1,)), DMA((n,))]
        + [DMA((1,)), DMA((hops, 2)), DMA((1,)), DMA((2,))]
        + [DMA((1,)), DMA((hops, 4))]
        + pair(2)
        + pair(3)
        + [DMA((1,)), DMA((2,))]
        + pair(5)
        + side_sems()
        + side_sems(),
        compiler_params=pltpu.CompilerParams(
            collective_id=0, has_side_effects=True, vmem_limit_bytes=67_000_000
        ),
    )(
        tokens, norm_gain.reshape(1, model), key_diff, value_diff, query_diff, query_win, keyval_win,
        proj_diff, proj_win, lam, sink, output_norm_gain.reshape(1, VDIM),
    )


def solution(mesh):
    torus = Mesh(
        mesh.devices.reshape(mesh.shape["grp"], mesh.shape["sp"], NX, 2),
        ("grp", "sp", "tp_0", "tp_1"),
    )
    return jax.shard_map(
        functools.partial(body, mesh.shape["sp"]),
        mesh=torus,
        in_specs=(
            P(GRP_SP_TP, None),
            P(),
            P("sp", TP),
            P("sp", TP),
            P("sp", TP),
            P(TP),
            P(),
            P("sp", TP),
            P(None, "sp", None),
            P(TP),
            P(TP, None),
            P(TP, None),
        ),
        out_specs=P(GRP_SP_TP, None),
        check_vma=False,
    )
```

```python
import functools

import jax
import jax.numpy as jnp
from jax import lax
from jax.experimental import pallas as pl
from jax.experimental.pallas import tpu as pltpu
from jax.sharding import Mesh
from jax.sharding import PartitionSpec as P

HEAD = 128
WIN_HEADS = 16
KV_HEADS = 4
WINDOW = 128
VDIM = 256
NX = 4
CUT = 96
TP = ("tp_0", "tp_1")
GRP_SP_TP = ("grp", "sp", "tp_0", "tp_1")
EPS = 1e-06
LOG2E = 1.4426950408889634
BF16 = jnp.bfloat16
F32 = jnp.float32
MESH = pl.DeviceIdType.MESH
DMA = pltpu.SemaphoreType.DMA
VMEM = pltpu.VMEM
ANY = pl.ANY


def remote(src, dst, send_sem, recv_sem, where):
    return pltpu.make_async_remote_copy(
        src_ref=src,
        dst_ref=dst,
        send_sem=send_sem,
        recv_sem=recv_sem,
        device_id=where,
        device_id_type=MESH,
    )


def greet(peers):
    barrier = pltpu.get_barrier_semaphore()
    for peer in peers:
        pl.semaphore_signal(barrier, inc=1, device_id=peer, device_id_type=MESH)
    pl.semaphore_wait(barrier, len(peers))


class Ring:
    def __init__(self, n, buf, base, cuts, send, recv):
        self.n, self.buf, self.send, self.recv = n, buf, send, recv
        self.base, self.cuts = base, cuts
        self.spans = []
        for cut in cuts:
            self.spans.append(pl.ds(base, cut))
            base = base + cut
        self.count = len(cuts)
        self.me = lax.axis_index("sp")
        self.to = (
            {"sp": lax.rem(self.me + 1, n)},
            {"sp": lax.rem(self.me + n - 1, n)},
        )

    def origin(self, d, s):
        return lax.rem(self.me + (self.n - s if d == 0 else s), self.n)

    def piece(self, d, s, k, hops):
        ref = self.buf.at[self.origin(d, hops), self.spans[k if d == 0 else self.count - 1 - k]]
        return remote(ref, ref, self.send.at[0], self.recv.at[s, k], self.to[d])

    def start(self, s, k):
        for d in (0, 1):
            self.piece(d, s, k, s).start()

    def land(self, s, k):
        both = pl.ds(self.base, self.cuts[k] + self.cuts[self.count - 1 - k])
        ref = self.buf.at[self.me, both]
        remote(ref, ref, self.send.at[0], self.recv.at[s, k], self.to[0]).wait_recv()

    def drain(self):
        ref = self.buf.at[pl.ds(0, self.n - 1), pl.ds(self.base, sum(self.cuts))]
        remote(ref, ref, self.send.at[0], self.recv.at[0, 0], self.to[0]).wait_send()


class Swap:
    def __init__(self, n, buf, cut, send, recv):
        self.n, self.buf, self.cut, self.send, self.recv = n, buf, cut, send, recv
        g = lax.axis_index("grp")
        self.odd = lax.rem(g, 2)
        self.to = {"grp": g + 1 - 2 * self.odd}
        self.kept = buf.shape[1] - cut
        self.base = pl.multiple_of(self.odd * cut, 16)

    def piece(self, o, odd, sem):
        ref = self.buf.at[o, pl.ds(pl.multiple_of(odd * self.kept, 16), self.cut)]
        return remote(ref, ref, self.send.at[0], self.recv.at[sem], self.to)

    def start(self, o, sem=None):
        self.piece(o, self.odd, o if sem is None else sem).start()

    def land(self, o):
        self.piece(o, 1 - self.odd, o).wait_recv()

    def several(self, count, sem):
        ref = self.buf.at[pl.ds(0, count), pl.ds(0, self.cut)]
        return remote(ref, ref, self.send.at[0], self.recv.at[sem], self.to)

    def drain(self):
        self.several(self.n - 1, 0).wait_send()


class Side:
    def __init__(self, own, slots, half, xs, xr, cs, cr):
        self.own, self.slots, self.half = own, slots, half
        self.xs, self.xr, self.cs, self.cr = xs, xr, cs, cr
        self.x = lax.axis_index("tp_0")
        self.c = lax.axis_index("tp_1")
        self.to = (
            {"tp_0": lax.rem(self.x + 1, NX)},
            {"tp_0": lax.rem(self.x + NX - 1, NX)},
        )
        self.other = {"tp_1": 1 - self.c}

    def spot(self, rel, h, core):
        slot = 2 * lax.rem(self.x + rel, NX) + core
        return self.slots.at[slot, pl.ds(h * self.half, self.half)]

    def source(self, rel, h):
        if rel == 0 and self.own is not None:
            return self.own.at[pl.ds(h * self.half, self.half)]
        return self.spot(rel, h, self.c)

    def half_of(self, d, k):
        return (0, 1, 0)[k] if d == 0 else (1, 0, 1)[k]

    def out(self, d, k):
        rel = 0 if k < 2 else (3 if d == 0 else 1)
        h = self.half_of(d, k)
        return remote(
            self.source(rel, h), self.spot(rel, h, self.c), self.xs.at[0], self.xr.at[k], self.to[d]
        )

    def inward(self, d, k):
        return (3 if d == 0 else 1) if k < 2 else 2, self.half_of(d, k)

    def blocks(self, count, send, recv, where):
        ref = self.slots.at[pl.ds(0, count)]
        return remote(ref, ref, send, recv, where)

    def across(self, rel, h):
        return remote(
            self.source(rel, h), self.spot(rel, h, self.c), self.cs.at[0], self.cr.at[0], self.other
        )

    def start(self):
        for k in (0, 1):
            for d in (0, 1):
                self.out(d, k).start()
        for h in (0, 1):
            self.across(0, h).start()

    def step(self, k):
        self.blocks(1, self.xs.at[0], self.xr.at[k], self.to[0]).wait_recv()
        for d in (0, 1):
            if k == 0:
                self.out(d, 2).start()
            self.across(*self.inward(d, k)).start()

    def finish(self):
        self.blocks(NX, self.cs.at[0], self.cr.at[0], self.other).wait_recv()

    def drain(self):
        self.blocks(NX - 1, self.xs.at[0], self.xr.at[0], self.to[0]).wait_send()
        self.blocks(NX, self.cs.at[0], self.cr.at[0], self.other).wait_send()


def side_sems():
    return [DMA((1,)), DMA((3,)), DMA((1,)), DMA((1,))]


def layer_kernel(
    n, heads_win, tok, gain, kd, vd, qd, qwd, kvw, pd, pw, lam, sink, ogain, out,
    w1, w2, raw, nbuf, acc1, acc2, kbuf, pdb, pwb, q, qw, kw, top, tot, acc, y, yd, yv, give, take, far, sums, facc,
    lsem, z1s, z1r, y1s, y1r, z2s, z2r, y2s, y2r, zks, zkr, hs, hr, us, ur, ts, tr, ws, wr, *sems,
):
    me, x, c = (lax.axis_index(a) for a in ("sp", "tp_0", "tp_1"))
    t = 2 * x + c
    block = raw.shape[1]
    rows = 2 * NX * block
    depth = w1.shape[1]
    part = kvw.shape[2] // 2
    head = t * heads_win // (WIN_HEADS // KV_HEADS)
    wq = qwd.shape[1]
    local = []
    at = 0
    for w in (kd, vd, qd):
        local.append((w, w1.at[me, :, pl.ds(at, w.shape[1])]))
        at += w.shape[1]
    local += [
        (qwd, w2.at[me, :, pl.ds(0, wq)]),
        (kvw.at[head, :, pl.ds(pl.multiple_of(c * part, part), part)], w2.at[me, :, pl.ds(wq, part)]),
        (tok, raw.at[t]),
        (pd, pdb.at[t]),
        (pw, pwb),
    ]
    local = [pltpu.make_async_copy(a, b, lsem.at[i]) for i, (a, b) in enumerate(local)]
    for copy in local:
        copy.start()

    swap1 = Swap(n, w1, CUT, y1s, y1r)
    swap2 = Swap(n, w2, depth // 2, y2s, y2r)
    ring1 = Ring(n, w1, swap1.base, (48, 32, 32, swap1.kept - 112), z1s, z1r)
    ring2 = Ring(n, w2, swap2.base, (depth // 4,) * 2, z2s, z2r)
    ring = Ring(n, kbuf, 0, (rows // 4,) * 4, zks, zkr)
    side = Side(None, raw, block // 2, *sems[:4])
    late = Side(None, pdb, depth // 2, *sems[4:])

    def peer(k):
        return {"tp_0": lax.rem(x + k // 2, NX), "tp_1": lax.rem(c + k % 2, 2)}

    greet([ring.to[0], ring.to[1], swap1.to] + [peer(k) for k in range(1, 2 * NX)])

    for copy in local[:3]:
        copy.wait()
    for k in range(4):
        ring1.start(0, k)
    local[5].wait()
    side.start()
    acc1[...] = jnp.zeros_like(acc1)
    acc2[...] = jnp.zeros_like(acc2)
    top[...] = jnp.full_like(top, -jnp.inf)
    tot[...] = jnp.zeros_like(tot)
    acc[...] = jnp.zeros_like(acc)
    for copy in local[3:5] + local[6:]:
        copy.wait()

    def normalise(quarter):
        tile = 32
        per = raw.shape[0] * block // tile // 4

        def one(j, carry):
            i = quarter * per + j
            slot, r = i // (block // tile), lax.rem(i, block // tile)
            v = raw[slot, pl.ds(pl.multiple_of(r * tile, tile), tile), :].astype(F32)
            v = v * lax.rsqrt(jnp.mean(v * v, axis=-1, keepdims=True) + EPS) * gain[...]
            v = v.astype(BF16)
            for o in range(n):
                nbuf[o, pl.ds(pl.multiple_of(i * tile, tile), tile), :] = v[:, o * depth : (o + 1) * depth]
            return carry

        lax.fori_loop(0, per, one, 0)

    def gather(w, swap, total, lo, hi):
        def one(j, carry):
            o = lax.rem(me + jnp.where(lax.rem(j, 2) == 1, (j + 1) // 2, n - j // 2), n)

            if swap is not None:

                @pl.when(j > 0)
                def _():
                    swap.land(o)

            total[...] += jnp.dot(nbuf[o], w[o], preferred_element_type=F32)
            return carry

        lax.fori_loop(lo, hi, one, 0)

    last = n // 2 - 1

    def swap_both(swap, ring_, hops):
        for d in (0, 1):
            swap.start(ring_.origin(d, hops))

    def swap_late(hops):
        for d in (0, 1):
            swap2.start(ring2.origin(d, hops), jnp.where(2 * hops - d < n // 2, 0, 1))

    def hop2(s, k):
        ring2.land(s, k)
        ring2.start(s + 1, k)

    def late_swaps(lo, hi):
        def one(h, carry):
            swap_late(h)
            return carry

        lax.fori_loop(lo, hi, one, 0)

    done = 2 * last - 3

    def phase1(s, carry):
        for k in range(4):
            ring1.land(s, k)
            ring1.start(s + 1, k)
            if k == 0:
                for i in range(3):

                    @pl.when(s == i + 1)
                    def _():
                        side.step(i)
                        if i == 2:
                            late.start()

                @pl.when(s == last - 3)
                def _():
                    side.finish()

            @pl.when(s == last - 3)
            def _():
                normalise(k)

            @pl.when(s == last - 2)
            def _():
                gather(w1, swap1, acc1, 3 * k, min(3 * k + 3, done))

            if k % 2 == 1:

                @pl.when(s >= 3)
                def _():
                    hop2(s - 3, k // 2)

        swap_both(swap1, ring1, s + 1)

        @pl.when(s == 1)
        def _():
            for k in (0, 1):
                ring2.start(0, k)

        return carry

    lax.fori_loop(0, last - 1, phase1, 0)
    for k in range(4):
        ring1.land(last - 1, k)
        if k < 2:
            ring1.start(last, k)
        if k % 2 == 1:
            hop2(last - 4, k // 2)
    swap_both(swap1, ring1, last)
    for k in (0, 1):
        ring1.land(last, k)
    swap1.start(ring1.origin(0, last + 1))
    for k in (0, 1):
        hop2(last - 3, k)
    late_swaps(1, last - 1)
    gather(w1, swap1, acc1, done, done + 2)
    for k in (0, 1):
        hop2(last - 2, k)
    swap_late(last - 1)
    gather(w1, swap1, acc1, done + 2, n)
    kvd = kbuf.shape[2]
    kbuf[me] = acc1[:, :kvd].astype(BF16)
    q[...] = acc1[:, kvd:].astype(BF16)
    for k in range(4):
        ring.start(0, k)

    def edge(d, inward):
        src = pl.ds(rows, WINDOW) if d == 0 else pl.ds(WINDOW, WINDOW)
        dst = pl.ds(0, WINDOW) if d == 0 else pl.ds(rows + WINDOW, WINDOW)
        target = kw.at[c, dst]
        return remote(target if inward else kw.at[c, src], target, hs.at[d], hr.at[d], ring.to[d])

    spans = (pl.ds(WINDOW, rows), pl.ds(0, WINDOW), pl.ds(rows + WINDOW, WINDOW))

    def twin(i, inward):
        ref = kw.at[1 - c if inward else c, spans[i]]
        return remote(ref, ref, us.at[i], ur.at[i], side.other)

    def trade(k):
        src = y.at[2 * lax.rem(x + k // 2, NX) + lax.rem(c + k % 2, 2)]
        return remote(src, yd.at[t], ts.at[0], tr.at[min(k - 1, 1)], peer(k))

    def traded(count, sem):
        ref = yd.at[pl.ds(0, count)]
        return remote(ref, ref, ts.at[0], tr.at[sem], side.other)

    pass_on = remote(give, take, ws.at[0], wr.at[0], side.other)

    def relay(d, inward):
        src = far.at[d] if inward else take.at[lax.rem(x + 2, NX), pl.ds(d * (block // 2), block // 2)]
        return remote(src, far.at[d], ws.at[1 + d], wr.at[1 + d], side.to[d])

    def deal(d, inward):
        src = sums.at[d] if inward else take.at[lax.rem(x + (1, NX - 1)[d], NX)]
        return remote(src, sums.at[d], ws.at[3 + d], wr.at[3 + d], side.to[d])

    def merge():
        for d in (0, 1):
            relay(d, True).wait_recv()
            to = lax.rem(x + (1, NX - 1)[d], NX)
            half = pl.ds(d * (block // 2), block // 2)
            take[to, half, :] = (take[to, half, :].astype(F32) + far[d].astype(F32)).astype(BF16)
        for d in (0, 1):
            deal(d, False).start()

    scale = HEAD**-0.5
    lanes = HEAD
    contract_last = (((1,), (1,)), ((), ()))

    def attend(o):
        def one(m, carry):
            cols = pl.ds(pl.multiple_of(m * HEAD, HEAD), HEAD)
            s = lax.dot_general(q[:, cols], kbuf[o, :, cols], contract_last, preferred_element_type=F32)
            s = s * (scale * LOG2E)
            reps = s.shape[1] // lanes
            was = top[m]
            now = jnp.maximum(was, jnp.max(s, axis=1, keepdims=True))
            fade = jnp.exp2(was - now)
            e = jnp.exp2(s - jnp.concatenate([now] * reps, axis=1))
            some = e[:, :lanes]
            for j in range(1, reps):
                some = some + e[:, j * lanes : (j + 1) * lanes]
            tot[m] = tot[m] * fade + some
            top[m] = now
            acc[m] = acc[m] * jnp.concatenate([fade] * (VDIM // lanes), axis=1) + jnp.dot(
                e.astype(BF16), kbuf[o, :, 2 * HEAD :], preferred_element_type=F32
            )
            return carry

        for m in range(2):
            one(m, 0)

    def window(lo, hi, stride):
        span = 3 * WINDOW
        heads = wq // HEAD
        i_q = lax.broadcasted_iota(jnp.int32, (WINDOW, span), 0)
        i_k = lax.broadcasted_iota(jnp.int32, (WINDOW, span), 1)
        near = jnp.abs(i_k - WINDOW - i_q) <= WINDOW

        def one(i, carry):
            b = i * stride
            r = pl.ds(pl.multiple_of(b * WINDOW, WINDOW), WINDOW)
            band = pl.ds(pl.multiple_of(b * WINDOW, WINDOW), span)
            where = i_k + (me * rows + b * WINDOW - WINDOW)
            valid = near & (where >= 0) & (where < n * rows)
            for h in range(heads):
                cols = pl.ds(h * HEAD, HEAD)
                s = lax.dot_general(qw[r, cols], kw[0, band, :], contract_last, preferred_element_type=F32)
                s = jnp.where(valid, s * scale, -jnp.inf)
                sunk = jnp.full((WINDOW, lanes), sink[h], F32)
                peak = jnp.maximum(jnp.max(s, axis=1, keepdims=True), sunk)
                e = jnp.exp(s - jnp.concatenate([peak] * 3, axis=1))
                whole = jnp.sum(e, axis=1, keepdims=True) + jnp.exp(sunk - peak)
                w = (e / jnp.concatenate([whole] * 3, axis=1)).astype(BF16)
                res = jnp.dot(w, kw[1, band, :], preferred_element_type=F32).astype(BF16)
                for j in range(WINDOW // block):
                    yv[j % 2, b * (WINDOW // block // 2) + j // 2, :, cols] = res[j * block : (j + 1) * block]
            return carry

        lax.fori_loop(lo, hi, one, 0)

    width = 512

    def columns(one):
        def run(j, carry):
            one(pl.ds(pl.multiple_of(j * width, width), width))
            return carry

        lax.fori_loop(0, out.shape[1] // width, run, 0)

    def window_rows(core, cols):
        ys = yv[core].reshape(NX * block, wq)
        return jnp.dot(ys, pwb[:, cols], preferred_element_type=F32).reshape(NX, block, width)

    def to_give(cols):
        give[:, :, cols] = window_rows(1 - c, cols).astype(BF16)

    def to_sum(cols):
        take[:, :, cols] = (window_rows(c, cols) + take[:, :, cols].astype(F32)).astype(BF16)

    attend(me)

    def side_work(s, k):
        def at(when):
            return pl.when(s == when)

        if k == 0:

            @at(0)
            def _():
                ring2.land(last - 1, 0)
                ring2.start(last, 0)
                ring2.land(last - 1, 1)
                swap_late(last)

            @at(1)
            def _():
                ring2.land(last, 0)
                swap2.start(ring2.origin(0, last + 1), 1)

            @at(4)
            def _():
                for i in (1, 2):
                    twin(i, True).wait_recv()
                window(0, 2, rows // WINDOW - 1)

        if k == 1:

            @at(1)
            def _():
                late.step(1)

            @at(2)
            def _():
                swap2.several(n // 2 - 1, 0).wait_recv()
                gather(w2, None, acc2, 0, n // 2)

            @at(3)
            def _():
                twin(0, True).wait_recv()
                window(1, rows // WINDOW - 1, 1)

            @at(4)
            def _():
                columns(to_give)
                pass_on.start()

        if k == 2:

            @at(0)
            def _():
                late.step(0)

        if k == 3:

            @at(2)
            def _():
                swap2.several(n // 2, 1).wait_recv()
                gather(w2, None, acc2, n // 2, n)
                kw[c, spans[0]] = acc2[:, wq:].astype(BF16)
                qw[...] = acc2[:, :wq].astype(BF16)
                for d in (0, 1):
                    edge(d, False).start()
                twin(0, False).start()

            @at(3)
            def _():
                for d in (0, 1):
                    edge(d, True).wait_recv()
                    twin(d + 1, False).start()
                late.step(2)

            @at(4)
            def _():
                pass_on.wait_recv()
                columns(to_sum)
                for d in (0, 1):
                    relay(d, False).start()

            @at(5)
            def _():
                merge()

    def phase2(s, carry):
        for k in range(4):
            ring.land(s, k)
            ring.start(s + 1, k)
            side_work(s, k)
            if k % 2 == 1:

                @pl.when(s > 0)
                def _():
                    attend(ring.origin(k // 2, s))

        return carry

    lax.fori_loop(0, last - 1, phase2, 0)
    for k in range(4):
        ring.land(last - 1, k)
        if k < 2:
            ring.start(last, k)
        if k % 2 == 1:
            attend(ring.origin(k // 2, last - 1))
    late.finish()
    for r in (ring1, ring2, swap1, swap2, side, late):
        r.drain()
    for d in (0, 1):
        edge(d, False).wait_send()
    for i in range(3):
        twin(i, False).wait_send()
    pass_on.wait_send()

    def both(i, carry):
        attend(lax.rem(me + n - last + 2 * last * i, n))
        return carry

    lax.fori_loop(0, 2, both, 0)
    for k in (0, 1):
        ring.land(last, k)
    attend(lax.rem(me + last + 1, n))

    def close(j):
        r = pl.ds(pl.multiple_of(j * block, block), block)
        parts = [1.0 / jnp.sum(tot[m, r, :], axis=1, keepdims=True) for m in range(2)]
        d = acc[0, r, :] * parts[0] - acc[1, r, :] * (lam[0] * parts[1])
        d = d * lax.rsqrt(jnp.mean(d * d, axis=-1, keepdims=True) + EPS) * ogain[...]
        return d.astype(BF16)

    for k in (4, 5, 2, 6, 3, 7, 1):
        j = 2 * lax.rem(x + k // 2, NX) + lax.rem(c + k % 2, 2)
        y[j] = close(j)
        trade(k).start()
    yd[t] = close(t)
    wide = 2048

    def add(total, away, cols):
        first = 2 * lax.rem(x + NX - away, NX)
        for h in (0, 1):
            total = total + jnp.dot(yd[first + h], pdb[first + h, :, cols], preferred_element_type=F32)
        return total

    def begin(j, carry):
        cols = pl.ds(pl.multiple_of(j * wide, wide), wide)
        total = take[x, :, cols].astype(F32)
        for d in (0, 1):
            total = total + sums[d, :, cols].astype(F32)
        facc[:, cols] = add(total, 0, cols)
        return carry

    def finish(j, carry):
        cols = pl.ds(pl.multiple_of(j * wide, wide), wide)
        total = facc[:, cols]
        for away in (1, 3, 2):
            total = add(total, away, cols)
        out[:, cols] = total.astype(out.dtype)
        return carry

    for d in (0, 1):
        deal(d, True).wait_recv()
    traded(1, 0).wait_recv()
    lax.fori_loop(0, out.shape[1] // wide, begin, 0)
    traded(2 * NX - 2, 1).wait_recv()
    lax.fori_loop(0, out.shape[1] // wide, finish, 0)
    traded(2 * NX - 1, 0).wait_send()
    for d in (0, 1):
        relay(d, False).wait_send()
        deal(d, False).wait_send()
    ring.drain()


def body(
    n, tokens, norm_gain, query_diff, key_diff, value_diff, lam, output_norm_gain,
    query_win, keyval_win, sink, proj_diff, proj_win,
):
    block, model = tokens.shape
    rows = block * 2 * NX
    depth, wq = query_win.shape
    kvd = key_diff.shape[1] + value_diff.shape[1]
    dq = query_diff.shape[1]
    part = keyval_win.shape[2] // 2
    hops = n // 2

    def pair(*shape):
        return [DMA(shape), DMA(shape)]

    return pl.pallas_call(
        functools.partial(layer_kernel, n, sink.shape[0]),
        out_shape=jax.ShapeDtypeStruct((block, model), BF16),
        in_specs=[
            pl.BlockSpec(memory_space=m)
            for m in [ANY, VMEM] + [ANY] * 7 + [pltpu.SMEM, pltpu.SMEM, VMEM]
        ],
        out_specs=pl.BlockSpec(memory_space=VMEM),
        scratch_shapes=[
            VMEM((n, depth, kvd + dq), BF16),
            VMEM((n, depth, wq + part), BF16),
            VMEM((2 * NX, block, model), BF16),
            VMEM((n, rows, depth), BF16),
            VMEM((rows, kvd + dq), F32),
            VMEM((rows, wq + part), F32),
            VMEM((n, rows, kvd), BF16),
            VMEM((2 * NX,) + proj_diff.shape, BF16),
            VMEM(proj_win.shape, BF16),
            VMEM((rows, dq), BF16),
            VMEM((rows, wq), BF16),
            VMEM((2, rows + 2 * WINDOW, part), BF16),
            VMEM((2, rows, HEAD), F32),
            VMEM((2, rows, HEAD), F32),
            VMEM((2, rows, VDIM), F32),
            VMEM((2 * NX, block, VDIM), BF16),
            VMEM((2 * NX, block, VDIM), BF16),
            VMEM((2, NX, block, wq), BF16),
            VMEM((NX, block, model), BF16),
            VMEM((NX, block, model), BF16),
            VMEM((2, block // 2, model), BF16),
            VMEM((2, block, model), BF16),
            VMEM((block, model), F32),
            DMA((8,)),
        ]
        + [DMA((1,)), DMA((hops, 4)), DMA((1,)), DMA((n,))]
        + [DMA((1,)), DMA((hops, 2)), DMA((1,)), DMA((2,))]
        + [DMA((1,)), DMA((hops, 4))]
        + pair(2)
        + pair(3)
        + [DMA((1,)), DMA((2,))]
        + pair(5)
        + side_sems()
        + side_sems(),
        compiler_params=pltpu.CompilerParams(
            collective_id=0, has_side_effects=True, vmem_limit_bytes=67_000_000
        ),
    )(
        tokens, norm_gain.reshape(1, model), key_diff, value_diff, query_diff, query_win, keyval_win,
        proj_diff, proj_win, lam, sink, output_norm_gain.reshape(1, VDIM),
    )


def solution(mesh):
    torus = Mesh(
        mesh.devices.reshape(mesh.shape["grp"], mesh.shape["sp"], NX, 2),
        ("grp", "sp", "tp_0", "tp_1"),
    )
    return jax.shard_map(
        functools.partial(body, mesh.shape["sp"]),
        mesh=torus,
        in_specs=(
            P(GRP_SP_TP, None),
            P(),
            P("sp", TP),
            P("sp", TP),
            P("sp", TP),
            P(TP),
            P(),
            P("sp", TP),
            P(None, "sp", None),
            P(TP),
            P(TP, None),
            P(TP, None),
        ),
        out_specs=P(GRP_SP_TP, None),
        check_vma=False,
    )
```
